256 devices in a mesh: grp: 2 (over y), sp: 32 (over z, core), tp: 4 (over x).
Axes of the slice: x: 4, y: 2, z: 16, core: 2. Of those that a mesh axis runs over, the one named last changes fastest.
The devices are a block of a 4x16x16 slice.
Arguments:
- residual: bfloat16 [16384, 2048], P(('grp', 'sp', 'tp')), parts along dimension 0, may hold values from -6 to 6
- queries_wide: bfloat16 [16384, 1024], P(('grp', 'sp'), 'tp'), parts along dimension 0, may hold values from -6 to 6
- keys_wide: bfloat16 [16384, 512], P(('grp', 'sp'), 'tp'), parts along dimension 0, may hold values from -6 to 6
- values_wide: bfloat16 [16384, 512], P(('grp', 'sp'), 'tp'), parts along dimension 0, may hold values from -6 to 6
- queries_narrow: bfloat16 [16384, 512], P(('grp', 'sp'), 'tp'), parts along dimension 0, may hold values from -6 to 6
- keys_narrow: bfloat16 [16384, 256], P(('grp', 'sp'), 'tp'), parts along dimension 0, may hold values from -6 to 6
- values_narrow: bfloat16 [16384, 256], P(('grp', 'sp'), 'tp'), parts along dimension 0, may hold values from -6 to 6
- query_gain_wide: float32 [128], replicated, may hold values from 1 to 6
- key_gain_wide: float32 [128], replicated, may hold values from 1 to 6
- query_gain_narrow: float32 [64], replicated, may hold values from 1 to 6
- key_gain_narrow: float32 [64], replicated, may hold values from 1 to 6
- output_wide: bfloat16 [1024, 2048], P('tp'), may hold values from -0.3125 to 0.3125
- output_narrow: bfloat16 [512, 2048], P('tp'), may hold values from -0.3125 to 0.3125
- norm_gain: float32 [2048], replicated, may hold values from 0.1 to 1.9
- gate_weight: bfloat16 [32, 2048, 3584], P('sp', None, 'tp'), may hold values from -0.125 to 0.125
- up_weight: bfloat16 [32, 2048, 3584], P('sp', None, 'tp'), may hold values from -0.125 to 0.125
- down_weight: bfloat16 [32, 3584, 2048], P('sp', 'tp'), may hold values from -0.09375 to 0.09375
- route_ids: int32 [16384, 2], P(('grp', 'sp', 'tp')), parts along dimension 0, may hold values from 0 to 31, all different within a row; in each aligned block of 64 rows (0 to 63, 64 to 127, ...) at most 8 rows name the same one
- route_weights: float32 [16384, 2], P(('grp', 'sp', 'tp')), parts along dimension 0, may hold values from 0.1 to 0.9
Outputs:
- result: bfloat16 [16384, 2048], P(('grp', 'sp', 'tp')), parts along dimension 0
The draws below stay inside these ranges and needn't reach their ends.
There are 2 independent parts, one for each index of `grp`. The reference program is written for one: setup_inputs(seed, part) draws one part's arguments, and reference() takes and returns one part's arrays. A program takes and returns all parts, laid end to end along the dimension named above; an argument that names none is the same for every part. Nothing has to cross between parts.
Inputs may be any that keep to these rules, and one draw needn't show every extreme that they name: `route_ids`: in each aligned block of 64 rows (the rows of one device) no expert is named by more than 8 rows, a bound that some block reaches; a row names 2 different experts.
All inputs are finite; a program needn't handle non-finite values.
Results may differ from the reference program's by a relative error of at most 0.013.
The reference program's roundings to bfloat16 on the way count: a program that leaves them out, or rounds other values in their place, can miss the bound.
Values may be sent and summed in bfloat16 or wider, within the bound.
A program may use at most 128 MiB of HBM per device.

```python
import math
import jax
import jax.numpy as jnp
import numpy as np
from jax import lax

D = 2048
HW = 8
KW = 4
DW = 128
HN = 8
KN = 4
DN = 64
FF = 3584
TOPK = 2
GRID = 64
TOKENS = 8192
ROWS = 64
EXPERTS = 32
CAP = 8
N_SP = 32
N_TP = 4


def draw_field(key, tag, head_count, head_width):
    noise_key = jax.random.fold_in(key, tag)
    field = jax.random.normal(noise_key, (TOKENS, head_count, head_width), jnp.float32)
    field = jnp.clip(field, -6.0, 6.0)
    return field.reshape(TOKENS, head_count * head_width).astype(jnp.bfloat16)


def draw_gain(key, tag, head_width):
    base_key = jax.random.fold_in(key, tag)
    return jax.random.uniform(base_key, (head_width,), jnp.float32, 1.0, 2.2)


def draw_queries_wide(key, part):
    return draw_field(key, 101, HW, DW)


def draw_keys_wide(key, part):
    return draw_field(key, 102, KW, DW)


def draw_queries_narrow(key, part):
    return draw_field(key, 103, HN, DN)


def draw_keys_narrow(key, part):
    return draw_field(key, 104, KN, DN)


def draw_query_gain_wide(key, part):
    return draw_gain(key, 201, DW)


def draw_key_gain_wide(key, part):
    return draw_gain(key, 202, DW)


def draw_query_gain_narrow(key, part):
    return draw_gain(key, 203, DN)


def draw_key_gain_narrow(key, part):
    return draw_gain(key, 204, DN)


def block_scale(key, dims, split, smallest, largest):
    gain = 1.0
    for dim, shards_of in split:
        heights = jax.random.uniform(jax.random.fold_in(jax.random.fold_in(key, 6), dim), (shards_of,), jnp.float32, smallest / len(split), largest / len(split))
        gain = gain * jnp.repeat(jnp.exp(heights), dims[dim] // shards_of).reshape((-1,) + (1,) * (len(dims) - 1 - dim))
    return gain


def shared_out(stream_key, own, number, rows, count, top, limit, skew):
    sequence = jax.random.permutation(stream_key, count)
    packed, usual = shares(count, rows * top, limit, skew, True), shares(count, rows * top, limit, skew, False)
    places = jnp.arange(count)

    def named(sizes, rotation):
        used = int((sizes > 0).sum())
        fixed = max(1, used // 4)
        moved = fixed + (places - fixed + rotation * (used - fixed)) % max(1, count - fixed)
        return jnp.zeros((count,), jnp.int32).at[sequence[jnp.where(places < fixed, places, moved)]].set(jnp.asarray(sizes, jnp.int32))

    sizes = jnp.where(number % 4 == 0, named(packed, number // 4), named(usual, number - number // 4 - 1))
    mixed = jax.random.permutation(jax.random.fold_in(own, 3), count)
    source_of, receiver = mixed[0:count // 2 * 2:2], mixed[1:count // 2 * 2:2]
    margin = jnp.minimum(sizes[source_of] - 1, limit - sizes[receiver]) // 2
    margin = jnp.where((source_of == sequence[0]) | (receiver == sequence[0]) | (sizes[receiver] == 0), 0, jnp.maximum(margin, 0))
    moved = jax.random.randint(jax.random.fold_in(own, 4), (count // 2,), 0, 1 << 20) % (margin + 1)
    sizes = sizes.at[source_of].add(-moved).at[receiver].add(moved)
    items = jnp.searchsorted(jnp.cumsum(sizes), jnp.arange(rows * top), side="right").astype(jnp.int32)
    grid = items.reshape(top, rows).T
    grid = grid[jax.random.permutation(jax.random.fold_in(own, 1), rows)]
    rotation = jax.random.randint(jax.random.fold_in(own, 2), (rows, 1), 0, top)
    return jnp.take_along_axis(grid, (jnp.arange(top)[None, :] + rotation) % top, axis=1)


def shares(amount, total, bound, slope, full):
    portions = [(1 << 20) // math.isqrt(grade ** slope) + 1 for grade in range(1, amount + 1)]
    largest = bound if full else min(bound, max(-(-total // amount), total * portions[0] // sum(portions)))
    least = 1 if total - largest >= amount - 1 else 0
    counts, spare = [largest] + [least] * (amount - 1), total - largest - least * (amount - 1)
    while spare > 0:
        candidates = [i for i in range(1, amount) if counts[i] < largest] or [i for i in range(1, amount) if counts[i] < bound]
        mass, left = sum([portions[i] for i in candidates]), spare
        for i in candidates:
            more = min(bound - counts[i], max(1, left * portions[i] // mass), spare)
            counts[i] = counts[i] + more
            spare = spare - more
    return np.array(counts)


def noise(rng, shape, width, reach, split=(), kind=jnp.bfloat16):
    level = block_scale(rng, shape, split, -0.22, 0.18) if split else 1.0
    result = jax.random.normal(rng, shape, jnp.float32) * width * level
    return jnp.minimum(jnp.maximum(result, -reach), reach).astype(kind)


def setup_inputs(seed: int = 0, part: int = 0) -> dict:
    splits = jax.random.split(jax.random.key(seed), 20)
    part_splits = jax.random.split(jax.random.fold_in(splits[19], part), 20)
    residual = noise(part_splits[0], (TOKENS, D), 1.0, 6.0, ((0, 128),))
    queries_wide = draw_queries_wide(jax.random.fold_in(jax.random.fold_in(splits[19], part), 71), part)
    keys_wide = draw_keys_wide(jax.random.fold_in(jax.random.fold_in(splits[19], part), 71), part)
    values_wide = noise(part_splits[3], (TOKENS, KW * DW), 1.0, 6.0, ((0, 32), (1, 4)))
    queries_narrow = draw_queries_narrow(jax.random.fold_in(jax.random.fold_in(splits[19], part), 71), part)
    keys_narrow = draw_keys_narrow(jax.random.fold_in(jax.random.fold_in(splits[19], part), 71), part)
    values_narrow = noise(part_splits[6], (TOKENS, KN * DN), 1.0, 6.0, ((0, 32), (1, 4)))
    query_gain_wide = draw_query_gain_wide(jax.random.fold_in(splits[19], 71), part)
    key_gain_wide = draw_key_gain_wide(jax.random.fold_in(splits[19], 71), part)
    query_gain_narrow = draw_query_gain_narrow(jax.random.fold_in(splits[19], 71), part)
    key_gain_narrow = draw_key_gain_narrow(jax.random.fold_in(splits[19], 71), part)
    output_wide = noise(splits[11], (HW * DW, D), ((HW * DW + HN * DN) // 4) ** -0.5, 0.3125, ((0, 4),))
    output_narrow = noise(splits[12], (HN * DN, D), ((HW * DW + HN * DN) // 4) ** -0.5, 0.3125, ((0, 4),))
    norm_gain = jnp.clip(1.0 + 0.18 * jax.random.normal(splits[13], (D,), jnp.float32), 0.1, 1.9)
    gate_weight = noise(splits[14], (EXPERTS, D, FF), D ** -0.5, 0.125, ((0, 32), (2, 4)))
    up_weight = noise(splits[15], (EXPERTS, D, FF), D ** -0.5, 0.125, ((0, 32), (2, 4)))
    down_weight = noise(splits[16], (EXPERTS, FF, D), FF ** -0.5, 0.09375, ((0, 32), (1, 4)))
    route_ids_keys = jax.random.split(jax.random.fold_in(part_splits[17], 1), TOKENS // ROWS)
    route_ids_turns = jax.random.permutation(jax.random.fold_in(part_splits[17], 3), TOKENS // ROWS)
    route_ids = jax.vmap(lambda own, number: shared_out(jax.random.fold_in(part_splits[17], 2), own, number, ROWS, EXPERTS, TOPK, CAP, 2))(route_ids_keys, route_ids_turns).reshape((TOKENS, TOPK))
    route_weights = jnp.clip(0.1 + 0.79999997 * jax.random.uniform(part_splits[18], (TOKENS, TOPK), jnp.float32) ** block_scale(part_splits[18], (TOKENS, TOPK), ((0, 128),), -0.2, 0.2), 0.1, 0.9)
    return {"residual": residual, "queries_wide": queries_wide, "keys_wide": keys_wide, "values_wide": values_wide, "queries_narrow": queries_narrow, "keys_narrow": keys_narrow, "values_narrow": values_narrow, "query_gain_wide": query_gain_wide, "key_gain_wide": key_gain_wide, "query_gain_narrow": query_gain_narrow, "key_gain_narrow": key_gain_narrow, "output_wide": output_wide, "output_narrow": output_narrow, "norm_gain": norm_gain, "gate_weight": gate_weight, "up_weight": up_weight, "down_weight": down_weight, "route_ids": route_ids, "route_weights": route_weights}


THETA = 10000.0
EPS = 1e-06

def rotary_tables(places, head_width):
    quarter = head_width // 4
    inv_freq = THETA ** (-jnp.arange(quarter, dtype=jnp.float32) / quarter)
    grid_rows = (places // GRID).astype(jnp.float32)
    grid_cols = (places % GRID).astype(jnp.float32)
    row_angle = grid_rows[:, None] * inv_freq[None, :]
    col_angle = grid_cols[:, None] * inv_freq[None, :]
    angles = jnp.concatenate([row_angle, row_angle, col_angle, col_angle], axis=-1)
    return (jnp.cos(angles), jnp.sin(angles))

def head_norm_rotate(values, gain_vec, cos_table, sin_table):
    as_float = values.astype(jnp.float32)
    scaled = as_float * lax.rsqrt(lax.optimization_barrier(jnp.mean(as_float * as_float, axis=-1, keepdims=True)) + EPS)
    scaled = scaled * gain_vec.astype(jnp.float32)
    full_shape = scaled.shape
    quarter = full_shape[-1] // 4
    halves = scaled.reshape(full_shape[:-1] + (2, 2, quarter))
    turned = jnp.stack([-halves[..., 1, :], halves[..., 0, :]], axis=-2).reshape(full_shape)
    return (scaled * cos_table[:, None, :] + turned * sin_table[:, None, :]).astype(jnp.bfloat16)

def rounded(values):
    return lax.optimization_barrier(values.astype(jnp.bfloat16)).astype(jnp.float32)

def attend(queries, keys, values, key_heads):
    token_count = queries.shape[0]
    head_width = queries.shape[2]
    group_size = queries.shape[1] // key_heads
    block_len = math.gcd(token_count, 512)
    grouped = queries.reshape(token_count // block_len, block_len, key_heads, group_size, head_width)
    keys_float = keys.reshape(token_count, key_heads, head_width).astype(jnp.float32)
    values_float = values.reshape(token_count, key_heads, head_width).astype(jnp.float32)
    score_scale = head_width ** (-0.5)

    def one_block(query_block):
        scores = jnp.einsum('qhgd,khd->hgqk', query_block.astype(jnp.float32), keys_float) * score_scale
        row_max = lax.optimization_barrier(jnp.max(scores, axis=-1, keepdims=True))
        weights = jnp.exp(scores - row_max)
        weight_sum = lax.optimization_barrier(jnp.sum(weights, axis=-1))
        mixed_values = jnp.einsum('hgqk,khd->qhgd', rounded(weights), values_float)
        return (mixed_values / jnp.transpose(weight_sum, (2, 0, 1))[..., None]).astype(jnp.bfloat16)
    heads_out = lax.map(one_block, grouped)
    return heads_out.reshape(token_count, key_heads * group_size * head_width)

def reference(residual, queries_wide, keys_wide, values_wide, queries_narrow, keys_narrow, values_narrow, query_gain_wide, key_gain_wide, query_gain_narrow, key_gain_narrow, output_wide, output_narrow, norm_gain, gate_weight, up_weight, down_weight, route_ids, route_weights):
    places = jnp.arange(TOKENS, dtype=jnp.int32)
    cos_wide, sin_wide = rotary_tables(places, DW)
    cos_narrow, sin_narrow = rotary_tables(places, DN)
    q_wide = head_norm_rotate(queries_wide.reshape(TOKENS, HW, DW), query_gain_wide, cos_wide, sin_wide)
    k_wide = head_norm_rotate(keys_wide.reshape(TOKENS, KW, DW), key_gain_wide, cos_wide, sin_wide)
    q_narrow = head_norm_rotate(queries_narrow.reshape(TOKENS, HN, DN), query_gain_narrow, cos_narrow, sin_narrow)
    k_narrow = head_norm_rotate(keys_narrow.reshape(TOKENS, KN, DN), key_gain_narrow, cos_narrow, sin_narrow)
    heads_wide = attend(q_wide, k_wide, values_wide, KW)
    heads_narrow = attend(q_narrow, k_narrow, values_narrow, KN)
    wide_cols = HW * DW // N_TP
    narrow_cols = HN * DN // N_TP
    summed = jnp.zeros((TOKENS, D), jnp.float32)
    for shard_index in range(N_TP):
        wide_lo = shard_index * wide_cols
        narrow_lo = shard_index * narrow_cols
        shard_term = jnp.dot(heads_wide[:, wide_lo:wide_lo + wide_cols], output_wide[wide_lo:wide_lo + wide_cols], preferred_element_type=jnp.float32)
        shard_term = shard_term + jnp.dot(heads_narrow[:, narrow_lo:narrow_lo + narrow_cols], output_narrow[narrow_lo:narrow_lo + narrow_cols], preferred_element_type=jnp.float32)
        summed = summed + rounded(shard_term)
    state_float = rounded(residual.astype(jnp.float32) + summed)
    normed = (state_float * lax.rsqrt(lax.optimization_barrier(jnp.mean(state_float * state_float, axis=-1, keepdims=True)) + EPS) * norm_gain.astype(jnp.float32)).astype(jnp.bfloat16)
    flat_ids = route_ids.reshape(-1)
    flat_weights = route_weights.reshape(-1)
    room = N_SP * N_TP * CAP
    shard_cols = FF // N_TP

    def expert_step(carried, expert):
        gate_one, up_one, down_one, number = expert
        ordering = jnp.argsort((flat_ids != number).astype(jnp.int32), stable=True)[:room].astype(jnp.int32)
        live_slot = flat_ids[ordering] == number
        owner_row = ordering // TOPK
        picked = normed[owner_row]
        gate_act = jnp.dot(picked, gate_one, preferred_element_type=jnp.float32)
        up_act = jnp.dot(picked, up_one, preferred_element_type=jnp.float32)
        hidden = (jax.nn.silu(gate_act) * up_act).astype(jnp.bfloat16)
        summed_out = jnp.zeros((room, D), jnp.float32)
        for shard_index in range(N_TP):
            low = shard_index * shard_cols
            partial_value = jnp.dot(hidden[:, low:low + shard_cols], down_one[low:low + shard_cols], preferred_element_type=jnp.float32)
            summed_out = summed_out + rounded(partial_value)
        expert_out = rounded(summed_out)
        weight = jnp.where(live_slot, flat_weights[ordering], 0.0)
        return (carried.at[owner_row].add(weight[:, None] * expert_out), None)
    mixture, _ = lax.scan(expert_step, jnp.zeros((TOKENS, D), jnp.float32), (gate_weight, up_weight, down_weight, jnp.arange(EXPERTS, dtype=jnp.int32)))
    return (state_float + mixture).astype(jnp.bfloat16)
```

```python
import functools
import math

import jax
import jax.numpy as jnp
from jax import lax
from jax.experimental import pallas as pl
from jax.experimental.pallas import tpu as pltpu
from jax.sharding import PartitionSpec as P

GRID = 64
THETA = 10000.0
EPS = 1e-06
NEG_BIG = -1e30
LOG2E = math.log2(math.e)
MESH = pl.DeviceIdType.MESH
F32 = jnp.float32
BF16 = jnp.bfloat16


def in_blocks(value, dim, peers):
    lengths = value.shape
    blocks = value.reshape(*lengths[:dim], peers, lengths[dim] // peers, *lengths[dim + 1 :])
    return jnp.moveaxis(blocks, dim, 0)


def sum_at_owner(value, axis, dim):
    peers = lax.axis_size(axis)
    blocks = lax.all_to_all(in_blocks(value, dim, peers), axis, 0, 0, tiled=True)
    return jnp.sum(blocks.astype(jnp.float32), axis=0)


def items_in_groups(value, axis, split_dim, concat_dim, work, item_dim, out_dim):
    items = jax.tree.leaves(value)[0].shape[item_dim]
    count = 2 if items % 2 == 0 else 1
    finished = []
    for k in range(count):
        group = jax.tree.map(
            lambda a: lax.slice_in_dim(
                a, k * (items // count), (k + 1) * (items // count), axis=item_dim
            ),
            value,
        )
        finished.append(
            work(
                lax.all_to_all(
                    group, axis, split_axis=split_dim, concat_axis=concat_dim, tiled=True
                )
            )
        )
    return jax.tree.map(lambda *parts: jnp.concatenate(parts, axis=out_dim), *finished)


def angles_of(places, head_width):
    quarter = head_width // 4
    inv_freq = THETA ** (-jnp.arange(quarter, dtype=jnp.float32) / quarter)
    grid_rows = (places // GRID).astype(jnp.float32)
    grid_cols = (places % GRID).astype(jnp.float32)
    row_angle = grid_rows[:, None] * inv_freq[None, :]
    col_angle = grid_cols[:, None] * inv_freq[None, :]
    return jnp.concatenate([row_angle, row_angle, col_angle, col_angle], axis=-1)


def lane_ids(shape):
    return lax.broadcasted_iota(jnp.int32, shape, 1)


def turned_lanes(values, quarter):
    lanes = lane_ids(values.shape)
    width = values.shape[1]
    return jnp.where(
        lanes % (2 * quarter) < quarter,
        pltpu.roll(values, width - quarter, 1),
        pltpu.roll(values, quarter, 1),
    )


def rotate(values, cos_table, sin_table, quarter):
    return values * cos_table + turned_lanes(values, quarter) * sin_table


def norm_wide(values, gain):
    mean = jnp.mean(values * values, axis=-1, keepdims=True)
    return values * lax.rsqrt(mean + EPS) * gain


def norm_halves(values, gain):
    lanes = lane_ids(values.shape)
    half = values.shape[1] // 2
    squares = values * values
    low = jnp.sum(jnp.where(lanes < half, squares, 0.0), axis=-1, keepdims=True) / half
    high = jnp.sum(jnp.where(lanes < half, 0.0, squares), axis=-1, keepdims=True) / half
    scale = jnp.where(lanes < half, lax.rsqrt(low + EPS), lax.rsqrt(high + EPS))
    return values * scale * gain


def attend_kernel(
    chips,
    peers,
    qw_ref,
    kw_ref,
    vw_ref,
    qn_ref,
    kvn_ref,
    gains_ref,
    tables_ref,
    res_ref,
    norm_gain_ref,
    ow_hbm,
    on_hbm,
    att_ref,
    normed_ref,
    kv_buf,
    qws,
    qns,
    m_buf,
    l_buf,
    acc_buf,
    heads,
    ow_buf,
    on_buf,
    part,
    first_in,
    last_in,
    w_sem,
    zsend,
    zrecv,
    psend,
    precv,
    xsend,
    xrecv,
):
    tok = qw_ref.shape[0]
    half = tok // 2
    wide = kw_ref.shape[1]
    sp = lax.axis_index("sp")
    tp = lax.axis_index("tp")
    z, core = sp // 2, sp % 2
    far = chips // 2
    right = {"sp": ((z + 1) % chips) * 2 + core}
    left = {"sp": ((z + chips - 1) % chips) * 2 + core}
    mate = {"sp": z * 2 + (1 - core)}
    xright = {"tp": (tp + 1) % peers}
    xleft = {"tp": (tp + peers - 1) % peers}

    w_copies = [
        pltpu.make_async_copy(ow_hbm, ow_buf, w_sem.at[0]),
        pltpu.make_async_copy(on_hbm, on_buf, w_sem.at[1]),
    ]
    for copy in w_copies:
        copy.start()

    barrier = pltpu.get_barrier_semaphore()
    for other in (right, left, mate, xright, xleft):
        pl.semaphore_signal(barrier, inc=1, device_id=other, device_id_type=MESH)

    def rows_of(chip, owner, sub):
        at = pl.multiple_of((chip * 2 + owner) * tok + sub * half, half)
        return kv_buf.at[pl.ds(at, half)]

    cos_w, sin_w = tables_ref[0], tables_ref[1]
    cos_n, sin_n = tables_ref[2], tables_ref[3]
    own = pl.ds(pl.multiple_of(sp * tok, tok), tok)
    k_wide = rotate(norm_wide(kw_ref[...].astype(F32), gains_ref[1:2]), cos_w, sin_w, wide // 4)
    kvn = kvn_ref[...].astype(F32)
    k_narrow = rotate(norm_halves(kvn, gains_ref[3:4]), cos_n, sin_n, wide // 8)
    kv_buf[own, 0:wide] = k_wide.astype(BF16)
    kv_buf[own, wide : 2 * wide] = vw_ref[...]
    kv_buf[own, 2 * wide : 3 * wide] = jnp.where(
        lane_ids(kvn.shape) < wide // 2, k_narrow, kvn
    ).astype(BF16)

    pl.semaphore_wait(barrier, 5)

    def z_copy(way, step, sub):
        shift = step - 1
        chip = (z + chips - shift) % chips if way == 0 else (z + shift) % chips
        ref = rows_of(chip, core, sub)
        return pltpu.make_async_remote_copy(
            src_ref=ref,
            dst_ref=ref,
            send_sem=zsend.at[way, step - 1, sub],
            recv_sem=zrecv.at[way, step - 1, sub],
            device_id=right if way == 0 else left,
            device_id_type=MESH,
        )

    def z_arrival(way, step, sub):
        chip = (z + chips - step) % chips if way == 0 else (z + step) % chips
        ref = rows_of(chip, core, sub)
        return pltpu.make_async_remote_copy(
            src_ref=ref,
            dst_ref=ref,
            send_sem=zsend.at[way, step - 1, sub],
            recv_sem=zrecv.at[way, step - 1, sub],
            device_id=right if way == 0 else left,
            device_id_type=MESH,
        )

    def m_copy(way, step, sub, owner):
        chip = (z + chips - step) % chips if way == 0 else (z + step) % chips
        ref = rows_of(chip, owner, sub)
        return pltpu.make_async_remote_copy(
            src_ref=ref,
            dst_ref=ref,
            send_sem=psend.at[way, step, sub],
            recv_sem=precv.at[way, step, sub],
            device_id=mate,
            device_id_type=MESH,
        )

    for way, sub in ((0, 0), (1, 1), (0, 1), (1, 0)):
        z_copy(way, 1, sub).start()
    for sub in (0, 1):
        m_copy(0, 0, sub, core).start()

    qw = qw_ref[...].astype(F32)
    for head in (0, 1):
        q = norm_wide(qw[:, head * wide : (head + 1) * wide], gains_ref[0:1])
        qws[head * tok : (head + 1) * tok] = rotate(q, cos_w, sin_w, wide // 4).astype(BF16)
    qn = rotate(norm_halves(qn_ref[...].astype(F32), gains_ref[2:3]), cos_n, sin_n, wide // 8)
    low = lane_ids(qn.shape) < wide // 2
    qns[0:tok] = jnp.where(low, qn, 0.0).astype(BF16)
    qns[tok : 2 * tok] = jnp.where(low, pltpu.roll(qn, wide // 2, 1), 0.0).astype(BF16)
    m_buf[...] = jnp.full(m_buf.shape, NEG_BIG, F32)
    l_buf[...] = jnp.zeros(l_buf.shape, F32)
    acc_buf[...] = jnp.zeros(acc_buf.shape, F32)

    def attend_chip(chip):
        keys = pl.ds(pl.multiple_of(chip * 2 * tok, 2 * tok), 2 * tok)
        k_w, v_w = kv_buf[keys, 0:wide], kv_buf[keys, wide : 2 * wide]
        kv_n = kv_buf[keys, 2 * wide : 3 * wide]
        work = []
        for kind in (0, 1):
            for head in (0, 1):
                work.append((kind, head))

        def scores(kind, head):
            q = (qws if kind == 0 else qns)[head * tok : (head + 1) * tok]
            return lax.dot_general(
                q,
                k_w if kind == 0 else kv_n,
                (((1,), (1,)), ((), ())),
                preferred_element_type=F32,
            )

        upcoming = scores(*work[0])
        for at, (kind, head) in enumerate(work):
            s = upcoming
            if at + 1 < len(work):
                upcoming = scores(*work[at + 1])
            factor = LOG2E * (wide if kind == 0 else wide // 2) ** (-0.5)
            m_old = m_buf[at]
            m_new = jnp.maximum(m_old, jnp.max(s, axis=-1, keepdims=True))
            alpha = jnp.exp2((m_old - m_new) * factor)
            parts = [
                jnp.exp2((s[:, i * wide : (i + 1) * wide] - m_new) * factor)
                for i in range(s.shape[1] // wide)
            ]
            total = parts[0]
            for p in parts[1:]:
                total = total + p
            weights = jnp.concatenate([p.astype(BF16) for p in parts], axis=1)
            mixed = jnp.dot(
                weights, v_w if kind == 0 else kv_n, preferred_element_type=F32
            )
            m_buf[at] = m_new
            l_buf[at] = l_buf[at] * alpha + total
            acc_buf[at] = acc_buf[at] * alpha + mixed

    def ring_step(step, nothing):
        @pl.when(step <= far)
        def _():
            for turn in (0, 1):
                for way in (0, 1):
                    sub = turn if way == 0 else 1 - turn

                    def arrived(way=way, sub=sub, turn=turn):
                        z_arrival(way, step, sub).wait_recv()
                        if turn == 0:

                            @pl.when(step < far)
                            def _():
                                z_copy(way, step + 1, sub).start()
                        else:

                            @pl.when(step < far - 1)
                            def _():
                                z_copy(way, step + 1, sub).start()

                        m_copy(way, step, sub, core).start()

                    if turn == 0:
                        arrived()
                    else:
                        pl.when(step < far)(arrived)

        before = step - 1

        @pl.when(before == 0)
        def _():
            for sub in (0, 1):
                m_copy(0, 0, sub, 1 - core).wait_recv()

        @pl.when(before > 0)
        def _():
            m_copy(0, before, 0, 1 - core).wait_recv()
            m_copy(1, before, 1, 1 - core).wait_recv()

        @pl.when(jnp.logical_and(before > 0, before < far))
        def _():
            m_copy(0, before, 1, 1 - core).wait_recv()
            m_copy(1, before, 0, 1 - core).wait_recv()

        def one(side, nothing):
            attend_chip((z + chips + before * (2 * side - 1)) % chips)
            return nothing

        single = jnp.logical_or(before == 0, before == far)
        return lax.fori_loop(0, jnp.where(single, 1, 2), one, nothing)

    lax.fori_loop(1, far + 2, ring_step, 0)

    outs = []
    for at in range(4):
        outs.append(acc_buf[at] / jnp.sum(l_buf[at], axis=-1, keepdims=True))
    heads[:, 0:wide] = outs[0].astype(BF16)
    heads[:, wide : 2 * wide] = outs[1].astype(BF16)
    heads[:, 2 * wide : 3 * wide] = jnp.where(
        low, pltpu.roll(outs[2], wide // 2, 1), outs[3]
    ).astype(BF16)
    for copy in w_copies:
        copy.wait()

    rows = res_ref.shape[0]
    cols = res_ref.shape[1] // 2

    def x_copy(way, number):
        dest = (tp + 1) % peers if way == 0 else (tp + peers - 1) % peers
        with_far = way * cols
        alone = (1 - way) * cols
        if number == 0:
            src = part.at[(tp + 2) % peers, :, pl.ds(with_far, cols)]
            dst = first_in.at[way]
        else:
            at = pl.ds(alone if number == 1 else with_far, cols)
            src = part.at[dest, :, at]
            dst = last_in.at[way, :, at]
        return pltpu.make_async_remote_copy(
            src_ref=src,
            dst_ref=dst,
            send_sem=xsend.at[way, number],
            recv_sem=xrecv.at[way, number],
            device_id=xright if way == 0 else xleft,
            device_id_type=MESH,
        )

    def project(peer):
        h = heads[pl.ds(pl.multiple_of(peer * rows, rows), rows)]
        product = jnp.dot(h[:, 0 : 2 * wide], ow_buf[...], preferred_element_type=F32)
        product = product + jnp.dot(
            h[:, 2 * wide : 3 * wide], on_buf[...], preferred_element_type=F32
        )
        part[peer] = product.astype(BF16)

    project((tp + 2) % peers)
    x_copy(0, 0).start()
    x_copy(1, 0).start()
    project((tp + 1) % peers)
    x_copy(0, 1).start()
    project((tp + peers - 1) % peers)
    x_copy(1, 1).start()
    project(tp)
    for way in (0, 1):
        dest = (tp + 1) % peers if way == 0 else (tp + peers - 1) % peers
        x_copy(way, 0).wait_recv()
        at = slice(way * cols, (way + 1) * cols)
        part[dest, :, at] = (
            part[dest, :, at].astype(F32) + first_in[way].astype(F32)
        ).astype(BF16)
        x_copy(way, 2).start()
    for way in (0, 1):
        x_copy(way, 1).wait_recv()
        x_copy(way, 2).wait_recv()
    total = res_ref[...].astype(F32) + part[tp].astype(F32)
    total = total + last_in[0].astype(F32) + last_in[1].astype(F32)
    attended = total.astype(BF16)
    att_ref[...] = attended
    state = attended.astype(F32)
    mean = jnp.mean(state * state, axis=-1, keepdims=True)
    normed_ref[...] = (state * lax.rsqrt(mean + EPS) * norm_gain_ref[...]).astype(BF16)

    for way in (0, 1):
        for number in (0, 1, 2):
            x_copy(way, number).wait_send()
    for sub in (0, 1):
        m_copy(0, 0, sub, core).wait_send()

    def drain(step, nothing):
        for way in (0, 1):
            for sub in (0, 1):
                z_copy(way, step, sub).wait_send()
                m_copy(way, step, sub, core).wait_send()
        return nothing

    lax.fori_loop(1, far, drain, 0)
    for way in (0, 1):
        z_copy(way, far, way).wait_send()
        m_copy(way, far, way, core).wait_send()


def attend(
    residual,
    queries_wide,
    keys_wide,
    values_wide,
    queries_narrow,
    keys_narrow,
    values_narrow,
    gains,
    tables,
    norm_gain,
    output_wide,
    output_narrow,
):
    chips = lax.axis_size("sp") // 2
    peers = lax.axis_size("tp")
    tok, wide = keys_wide.shape
    rows, width = residual.shape
    far = chips // 2
    vmem = pl.BlockSpec(memory_space=pltpu.VMEM)
    hbm = pl.BlockSpec(memory_space=pl.ANY)
    dma = pltpu.SemaphoreType.DMA
    return pl.pallas_call(
        functools.partial(attend_kernel, chips, peers),
        out_shape=(
            jax.ShapeDtypeStruct((rows, width), BF16),
            jax.ShapeDtypeStruct((rows, width), BF16),
        ),
        in_specs=[vmem] * 9 + [hbm] * 2,
        out_specs=(vmem, vmem),
        scratch_shapes=[
            pltpu.VMEM((2 * chips * tok, 3 * wide), BF16),
            pltpu.VMEM((2 * tok, wide), BF16),
            pltpu.VMEM((2 * tok, wide), BF16),
            pltpu.VMEM((4, tok, wide), F32),
            pltpu.VMEM((4, tok, wide), F32),
            pltpu.VMEM((4, tok, wide), F32),
            pltpu.VMEM((tok, 3 * wide), BF16),
            pltpu.VMEM(output_wide.shape, BF16),
            pltpu.VMEM(output_narrow.shape, BF16),
            pltpu.VMEM((peers, rows, width), BF16),
            pltpu.VMEM((2, rows, width // 2), BF16),
            pltpu.VMEM((2, rows, width), BF16),
            dma((2,)),
            dma((2, far, 2)),
            dma((2, far, 2)),
            dma((2, far + 1, 2)),
            dma((2, far + 1, 2)),
            dma((2, 3)),
            dma((2, 3)),
        ],
        compiler_params=pltpu.CompilerParams(
            collective_id=0, has_side_effects=True, vmem_limit_bytes=40 * 1024 * 1024
        ),
        name="attend",
    )(
        queries_wide,
        keys_wide,
        values_wide,
        queries_narrow,
        jnp.concatenate([keys_narrow, values_narrow], axis=1),
        gains,
        tables,
        residual,
        norm_gain.reshape(1, width),
        output_wide,
        output_narrow,
    )


def slot_tables(chosen, slot_count, expert_count):
    row_count = chosen.shape[0]
    pick_count = chosen.shape[1]
    flat_pick = chosen.reshape(row_count * pick_count)
    hit_marks = (flat_pick[:, None] == jnp.arange(expert_count, dtype=jnp.int32)[None, :]).astype(
        jnp.int32
    )
    before = jnp.cumsum(hit_marks, axis=0) - hit_marks
    slot_place = jnp.sum(before * hit_marks, axis=1)
    target = flat_pick * slot_count + slot_place
    slot_table = target[:, None] == jnp.arange(expert_count * slot_count, dtype=jnp.int32)[None, :]
    return slot_table.astype(jnp.bfloat16).reshape(row_count, pick_count, expert_count * slot_count)


def body(
    residual,
    queries_wide,
    keys_wide,
    values_wide,
    queries_narrow,
    keys_narrow,
    values_narrow,
    query_gain_wide,
    key_gain_wide,
    query_gain_narrow,
    key_gain_narrow,
    output_wide,
    output_narrow,
    norm_gain,
    gate_weight,
    up_weight,
    down_weight,
    route_ids,
    route_weights,
):
    tok_count = queries_wide.shape[0]
    places = lax.axis_index("sp") * tok_count + jnp.arange(tok_count, dtype=jnp.int32)
    wide_width = query_gain_wide.shape[0]
    narrow_width = query_gain_narrow.shape[0]
    wide_angles = angles_of(places, wide_width)
    narrow_angles = angles_of(places, narrow_width)
    narrow_angles = jnp.concatenate([narrow_angles, narrow_angles], axis=1)
    lanes = jnp.arange(wide_width, dtype=jnp.int32)
    wide_sign = jnp.where(lanes % (wide_width // 2) < wide_width // 4, -1.0, 1.0)
    narrow_sign = jnp.where(lanes % (narrow_width // 2) < narrow_width // 4, -1.0, 1.0)
    tables = jnp.stack(
        [
            jnp.cos(wide_angles),
            jnp.sin(wide_angles) * wide_sign,
            jnp.cos(narrow_angles),
            jnp.sin(narrow_angles) * narrow_sign,
        ]
    )
    gains = jnp.stack(
        [
            query_gain_wide,
            key_gain_wide,
            jnp.concatenate([query_gain_narrow, query_gain_narrow]),
            jnp.concatenate([key_gain_narrow, key_gain_narrow]),
        ]
    )
    attended, normed = attend(
        residual,
        queries_wide,
        keys_wide,
        values_wide,
        queries_narrow,
        keys_narrow,
        values_narrow,
        gains,
        tables,
        norm_gain,
        output_wide,
        output_narrow,
    )
    own_rows = residual.shape[0]
    state_float = attended.astype(jnp.float32)
    pick_count = route_ids.shape[1]
    expert_count = lax.axis_size("sp")
    slot_count = 2 * pick_count * own_rows // expert_count
    model_width = residual.shape[1]
    own_tables = slot_tables(route_ids, slot_count, expert_count)

    def expert_block(arrived):
        full_shape = arrived.shape
        flat_rows = arrived.reshape(-1, model_width)
        gate_act = jnp.dot(flat_rows, gate_weight[0], preferred_element_type=jnp.float32)
        up_act = jnp.dot(flat_rows, up_weight[0], preferred_element_type=jnp.float32)
        hidden = (jax.nn.silu(gate_act) * up_act).astype(jnp.bfloat16)
        partial_value = jnp.dot(hidden, down_weight[0], preferred_element_type=jnp.float32).reshape(
            full_shape
        )
        summed = sum_at_owner(partial_value.astype(jnp.bfloat16), "tp", 0)
        return summed.reshape(full_shape[1:]).astype(jnp.bfloat16)

    send_rows = jnp.einsum(
        "rks,rd->sd", own_tables, normed, preferred_element_type=jnp.float32
    ).astype(jnp.bfloat16)
    send_rows = send_rows.reshape(expert_count, slot_count, model_width)

    def copy_then_run(arrived):
        copies = lax.all_gather(arrived, "tp", axis=0, tiled=True)
        return expert_block(copies.reshape((lax.axis_size("tp"),) + arrived.shape))

    results = items_in_groups(send_rows, "sp", 0, 0, copy_then_run, 1, 1)
    returned = lax.all_to_all(results, "sp", split_axis=0, concat_axis=0, tiled=True)
    returned_flat = returned.reshape(expert_count * slot_count, model_width)
    picked = jnp.einsum(
        "rks,sd->rkd", own_tables, returned_flat, preferred_element_type=jnp.float32
    )
    mixture = jnp.sum(route_weights[:, :, None] * picked, axis=1)
    return (state_float + mixture).astype(jnp.bfloat16)


def solution(mesh):
    return jax.shard_map(
        body,
        mesh=mesh,
        in_specs=(
            P(("grp", "sp", "tp"), None),
            P(("grp", "sp"), "tp"),
            P(("grp", "sp"), "tp"),
            P(("grp", "sp"), "tp"),
            P(("grp", "sp"), "tp"),
            P(("grp", "sp"), "tp"),
            P(("grp", "sp"), "tp"),
            P(),
            P(),
            P(),
            P(),
            P("tp", None),
            P("tp", None),
            P(),
            P("sp", None, "tp"),
            P("sp", None, "tp"),
            P("sp", "tp", None),
            P(("grp", "sp", "tp"), None),
            P(("grp", "sp", "tp"), None),
        ),
        out_specs=P(("grp", "sp", "tp"), None),
        check_vma=False,
    )
```

```python
import functools
import math

import jax
import jax.numpy as jnp
from jax import lax
from jax.experimental import pallas as pl
from jax.experimental.pallas import tpu as pltpu
from jax.sharding import PartitionSpec as P

GRID = 64
THETA = 10000.0
EPS = 1e-06
NEG_BIG = -1e30
LOG2E = math.log2(math.e)
MESH = pl.DeviceIdType.MESH
F32 = jnp.float32
BF16 = jnp.bfloat16


def angles_of(places, head_width):
    quarter = head_width // 4
    inv_freq = THETA ** (-jnp.arange(quarter, dtype=jnp.float32) / quarter)
    grid_rows = (places // GRID).astype(jnp.float32)
    grid_cols = (places % GRID).astype(jnp.float32)
    row_angle = grid_rows[:, None] * inv_freq[None, :]
    col_angle = grid_cols[:, None] * inv_freq[None, :]
    return jnp.concatenate([row_angle, row_angle, col_angle, col_angle], axis=-1)


def lane_ids(shape):
    return lax.broadcasted_iota(jnp.int32, shape, 1)


def turned_lanes(values, quarter):
    lanes = lane_ids(values.shape)
    width = values.shape[1]
    return jnp.where(
        lanes % (2 * quarter) < quarter,
        pltpu.roll(values, width - quarter, 1),
        pltpu.roll(values, quarter, 1),
    )


def rotate(values, cos_table, sin_table, quarter):
    return values * cos_table + turned_lanes(values, quarter) * sin_table


def norm_wide(values, gain):
    mean = jnp.mean(values * values, axis=-1, keepdims=True)
    return values * lax.rsqrt(mean + EPS) * gain


def norm_halves(values, gain):
    lanes = lane_ids(values.shape)
    half = values.shape[1] // 2
    squares = values * values
    low = jnp.sum(jnp.where(lanes < half, squares, 0.0), axis=-1, keepdims=True) / half
    high = jnp.sum(jnp.where(lanes < half, 0.0, squares), axis=-1, keepdims=True) / half
    scale = jnp.where(lanes < half, lax.rsqrt(low + EPS), lax.rsqrt(high + EPS))
    return values * scale * gain


def layer_kernel(
    chips,
    peers,
    qw_ref,
    kw_ref,
    vw_ref,
    qn_ref,
    kvn_ref,
    gains_ref,
    tables_ref,
    res_ref,
    norm_gain_ref,
    route_ref,
    ow_hbm,
    on_hbm,
    gate_hbm,
    up_hbm,
    down_hbm,
    out_ref,
    kv_buf,
    qws,
    qns,
    m_buf,
    l_buf,
    acc_buf,
    heads,
    ow_buf,
    on_buf,
    part,
    first_in,
    last_in,
    info,
    gate_buf,
    up_buf,
    down_buf,
    att_buf,
    rows_buf,
    x_buf,
    y_buf,
    y_first,
    y_last,
    e_buf,
    e_mate,
    ret_out,
    ret_in,
    w_sem,
    zsend,
    zrecv,
    psend,
    precv,
    isend,
    irecv,
    imsend,
    imrecv,
    xsend,
    xrecv,
    z2send,
    z2recv,
    p2send,
    p2recv,
    asend,
    arecv,
    ysend,
    yrecv,
    esend,
    erecv,
    rsend,
    rrecv,
):
    tok = qw_ref.shape[0]
    half = tok // 2
    wide = kw_ref.shape[1]
    sp = lax.axis_index("sp")
    tp = lax.axis_index("tp")
    z, core = sp // 2, sp % 2
    far = chips // 2
    right = {"sp": ((z + 1) % chips) * 2 + core}
    left = {"sp": ((z + chips - 1) % chips) * 2 + core}
    mate = {"sp": z * 2 + (1 - core)}
    xright = {"tp": (tp + 1) % peers}
    xleft = {"tp": (tp + peers - 1) % peers}

    w_copies = [
        pltpu.make_async_copy(ow_hbm, ow_buf, w_sem.at[0]),
        pltpu.make_async_copy(on_hbm, on_buf, w_sem.at[1]),
        pltpu.make_async_copy(gate_hbm.at[0], gate_buf, w_sem.at[2]),
        pltpu.make_async_copy(up_hbm.at[0], up_buf, w_sem.at[3]),
        pltpu.make_async_copy(down_hbm.at[0], down_buf, w_sem.at[4]),
    ]
    for copy in w_copies:
        copy.start()

    barrier = pltpu.get_barrier_semaphore()
    for other in (right, left, mate, xright, xleft):
        pl.semaphore_signal(barrier, inc=1, device_id=other, device_id_type=MESH)

    def rows_of(chip, owner, sub):
        at = pl.multiple_of((chip * 2 + owner) * tok + sub * half, half)
        return kv_buf.at[pl.ds(at, half)]

    cos_w, sin_w = tables_ref[0], tables_ref[1]
    cos_n, sin_n = tables_ref[2], tables_ref[3]
    own = pl.ds(pl.multiple_of(sp * tok, tok), tok)
    k_wide = rotate(norm_wide(kw_ref[...].astype(F32), gains_ref[1:2]), cos_w, sin_w, wide // 4)
    kvn = kvn_ref[...].astype(F32)
    k_narrow = rotate(norm_halves(kvn, gains_ref[3:4]), cos_n, sin_n, wide // 8)
    kv_buf[own, 0:wide] = k_wide.astype(BF16)
    kv_buf[own, wide : 2 * wide] = vw_ref[...]
    kv_buf[own, 2 * wide : 3 * wide] = jnp.where(
        lane_ids(kvn.shape) < wide // 2, k_narrow, kvn
    ).astype(BF16)

    slots = 2 * 2 * res_ref.shape[0] // (2 * chips)
    route = route_ref[...]
    lanes = route.shape[1]
    experts = lax.broadcasted_iota(jnp.int32, (2 * chips, lanes), 0).astype(F32)
    hits = [(route[k : k + 1] == experts).astype(F32) for k in (0, 1)]
    earlier = (
        lax.broadcasted_iota(jnp.int32, (lanes, lanes), 0)
        < lax.broadcasted_iota(jnp.int32, (lanes, lanes), 1)
    ).astype(BF16)
    places = jnp.dot((hits[0] + hits[1]).astype(BF16), earlier, preferred_element_type=F32)
    targets = [
        jnp.sum(hit * (places + experts * slots), axis=0, keepdims=True) for hit in hits
    ]
    row = lax.broadcasted_iota(jnp.int32, route.shape, 0)
    info[sp] = jnp.where(row == 0, targets[0], jnp.where(row == 1, targets[1], route))

    pl.semaphore_wait(barrier, 5)

    def hop(src, dst, send, recv, device):
        return pltpu.make_async_remote_copy(
            src_ref=src,
            dst_ref=dst,
            send_sem=send,
            recv_sem=recv,
            device_id=device,
            device_id_type=MESH,
        )

    def same(ref, send, recv, device):
        return hop(ref, ref, send, recv, device)

    def chip_at(way, distance):
        return (z + chips - distance) % chips if way == 0 else (z + distance) % chips

    def along(way):
        return right if way == 0 else left

    def z_copy(way, step, sub):
        ref = rows_of(chip_at(way, step - 1), core, sub)
        return same(ref, zsend.at[way, step - 1, sub], zrecv.at[way, step - 1, sub], along(way))

    def z_arrival(way, step, sub):
        ref = rows_of(chip_at(way, step), core, sub)
        return same(ref, zsend.at[way, step - 1, sub], zrecv.at[way, step - 1, sub], along(way))

    def m_copy(way, step, sub, owner):
        ref = rows_of(chip_at(way, step), owner, sub)
        return same(ref, psend.at[way, step, sub], precv.at[way, step, sub], mate)

    def i_copy(way, step):
        ref = info.at[chip_at(way, step - 1) * 2 + core]
        return same(ref, isend.at[way, step - 1], irecv.at[way, step - 1], along(way))

    def i_arrival(way, step):
        ref = info.at[chip_at(way, step) * 2 + core]
        return same(ref, isend.at[way, step - 1], irecv.at[way, step - 1], along(way))

    def im_copy(way, step, owner):
        ref = info.at[chip_at(way, step) * 2 + owner]
        return same(ref, imsend.at[way, step], imrecv.at[way, step], mate)

    for way in (0, 1):
        i_copy(way, 1).start()
    im_copy(0, 0, core).start()
    for way, sub in ((0, 0), (1, 1), (0, 1), (1, 0)):
        z_copy(way, 1, sub).start()
    for sub in (0, 1):
        m_copy(0, 0, sub, core).start()

    qw = qw_ref[...].astype(F32)
    for head in (0, 1):
        q = norm_wide(qw[:, head * wide : (head + 1) * wide], gains_ref[0:1])
        qws[head * tok : (head + 1) * tok] = rotate(q, cos_w, sin_w, wide // 4).astype(BF16)
    qn = rotate(norm_halves(qn_ref[...].astype(F32), gains_ref[2:3]), cos_n, sin_n, wide // 8)
    low = lane_ids(qn.shape) < wide // 2
    qns[0:tok] = jnp.where(low, qn, 0.0).astype(BF16)
    qns[tok : 2 * tok] = jnp.where(low, pltpu.roll(qn, wide // 2, 1), 0.0).astype(BF16)
    m_buf[...] = jnp.full(m_buf.shape, NEG_BIG, F32)
    l_buf[...] = jnp.zeros(l_buf.shape, F32)
    acc_buf[...] = jnp.zeros(acc_buf.shape, F32)

    def attend_chip(chip):
        keys = pl.ds(pl.multiple_of(chip * 2 * tok, 2 * tok), 2 * tok)
        k_w, v_w = kv_buf[keys, 0:wide], kv_buf[keys, wide : 2 * wide]
        kv_n = kv_buf[keys, 2 * wide : 3 * wide]
        work = []
        for kind in (0, 1):
            for head in (0, 1):
                work.append((kind, head))

        def scores(kind, head):
            q = (qws if kind == 0 else qns)[head * tok : (head + 1) * tok]
            return lax.dot_general(
                q,
                k_w if kind == 0 else kv_n,
                (((1,), (1,)), ((), ())),
                preferred_element_type=F32,
            )

        upcoming = scores(*work[0])
        for at, (kind, head) in enumerate(work):
            s = upcoming
            if at + 1 < len(work):
                upcoming = scores(*work[at + 1])
            factor = LOG2E * (wide if kind == 0 else wide // 2) ** (-0.5)
            m_old = m_buf[at]
            m_new = jnp.maximum(m_old, jnp.max(s, axis=-1, keepdims=True))
            alpha = jnp.exp2((m_old - m_new) * factor)
            parts = [
                jnp.exp2((s[:, i * wide : (i + 1) * wide] - m_new) * factor)
                for i in range(s.shape[1] // wide)
            ]
            total = parts[0]
            for p in parts[1:]:
                total = total + p
            weights = jnp.concatenate([p.astype(BF16) for p in parts], axis=1)
            mixed = jnp.dot(
                weights, v_w if kind == 0 else kv_n, preferred_element_type=F32
            )
            m_buf[at] = m_new
            l_buf[at] = l_buf[at] * alpha + total
            acc_buf[at] = acc_buf[at] * alpha + mixed

    def ring_step(step, nothing):
        def pass_on(way):
            i_arrival(way, step).wait_recv()
            if way == 0:
                pl.when(step < far)(lambda: i_copy(way, step + 1).start())
            else:
                pl.when(step < far - 1)(lambda: i_copy(way, step + 1).start())
            im_copy(way, step, core).start()

        @pl.when(step <= far)
        def _():
            pass_on(0)
            pl.when(step < far)(functools.partial(pass_on, 1))
            for turn in (0, 1):
                for way in (0, 1):
                    sub = turn if way == 0 else 1 - turn

                    def arrived(way=way, sub=sub, turn=turn):
                        z_arrival(way, step, sub).wait_recv()
                        if turn == 0:

                            @pl.when(step < far)
                            def _():
                                z_copy(way, step + 1, sub).start()
                        else:

                            @pl.when(step < far - 1)
                            def _():
                                z_copy(way, step + 1, sub).start()

                        m_copy(way, step, sub, core).start()

                    if turn == 0:
                        arrived()
                    else:
                        pl.when(step < far)(arrived)

        before = step - 1

        @pl.when(before == 0)
        def _():
            im_copy(0, 0, 1 - core).wait_recv()
            for sub in (0, 1):
                m_copy(0, 0, sub, 1 - core).wait_recv()

        @pl.when(before > 0)
        def _():
            im_copy(0, before, 1 - core).wait_recv()
            m_copy(0, before, 0, 1 - core).wait_recv()
            m_copy(1, before, 1, 1 - core).wait_recv()

        @pl.when(jnp.logical_and(before > 0, before < far))
        def _():
            im_copy(1, before, 1 - core).wait_recv()
            m_copy(0, before, 1, 1 - core).wait_recv()
            m_copy(1, before, 0, 1 - core).wait_recv()

        def one(side, nothing):
            attend_chip((z + chips + before * (2 * side - 1)) % chips)
            return nothing

        single = jnp.logical_or(before == 0, before == far)
        return lax.fori_loop(0, jnp.where(single, 1, 2), one, nothing)

    lax.fori_loop(1, far + 2, ring_step, 0)

    outs = []
    for at in range(4):
        outs.append(acc_buf[at] / jnp.sum(l_buf[at], axis=-1, keepdims=True))
    heads[:, 0:wide] = outs[0].astype(BF16)
    heads[:, wide : 2 * wide] = outs[1].astype(BF16)
    heads[:, 2 * wide : 3 * wide] = jnp.where(
        low, pltpu.roll(outs[2], wide // 2, 1), outs[3]
    ).astype(BF16)
    for copy in w_copies[:2]:
        copy.wait()

    rows = res_ref.shape[0]
    cols = res_ref.shape[1] // 2

    def x_copy(way, number):
        dest = (tp + 1) % peers if way == 0 else (tp + peers - 1) % peers
        with_far = way * cols
        alone = (1 - way) * cols
        if number == 0:
            src = part.at[(tp + 2) % peers, :, pl.ds(with_far, cols)]
            dst = first_in.at[way]
        else:
            at = pl.ds(alone if number == 1 else with_far, cols)
            src = part.at[dest, :, at]
            dst = last_in.at[way, :, at]
        return pltpu.make_async_remote_copy(
            src_ref=src,
            dst_ref=dst,
            send_sem=xsend.at[way, number],
            recv_sem=xrecv.at[way, number],
            device_id=xright if way == 0 else xleft,
            device_id_type=MESH,
        )

    def project(peer):
        h = heads[pl.ds(pl.multiple_of(peer * rows, rows), rows)]
        product = jnp.dot(h[:, 0 : 2 * wide], ow_buf[...], preferred_element_type=F32)
        product = product + jnp.dot(
            h[:, 2 * wide : 3 * wide], on_buf[...], preferred_element_type=F32
        )
        part[peer] = product.astype(BF16)

    project((tp + 2) % peers)
    x_copy(0, 0).start()
    x_copy(1, 0).start()
    project((tp + 1) % peers)
    x_copy(0, 1).start()
    project((tp + peers - 1) % peers)
    x_copy(1, 1).start()
    project(tp)
    for way in (0, 1):
        dest = (tp + 1) % peers if way == 0 else (tp + peers - 1) % peers
        x_copy(way, 0).wait_recv()
        at = slice(way * cols, (way + 1) * cols)
        part[dest, :, at] = (
            part[dest, :, at].astype(F32) + first_in[way].astype(F32)
        ).astype(BF16)
        x_copy(way, 2).start()
    for way in (0, 1):
        x_copy(way, 1).wait_recv()
        x_copy(way, 2).wait_recv()
    total = res_ref[...].astype(F32) + part[tp].astype(F32)
    total = total + last_in[0].astype(F32) + last_in[1].astype(F32)
    attended = total.astype(BF16)
    att_buf[...] = attended
    state = attended.astype(F32)
    mean = jnp.mean(state * state, axis=-1, keepdims=True)
    normed = (state * lax.rsqrt(mean + EPS) * norm_gain_ref[...]).astype(BF16)
    rows_buf[pl.ds(pl.multiple_of(sp * rows, rows), rows)] = normed

    def block_of(chip, owner, sub):
        at = pl.multiple_of((chip * 2 + owner) * rows + sub * (rows // 2), rows // 2)
        return rows_buf.at[pl.ds(at, rows // 2)]

    def z2_copy(way, step, sub):
        ref = block_of(chip_at(way, step - 1), core, sub)
        return same(ref, z2send.at[way, step - 1, sub], z2recv.at[way, step - 1, sub], along(way))

    def z2_arrival(way, step, sub):
        ref = block_of(chip_at(way, step), core, sub)
        return same(ref, z2send.at[way, step - 1, sub], z2recv.at[way, step - 1, sub], along(way))

    def m2_copy(way, step, sub, owner):
        ref = block_of(chip_at(way, step), owner, sub)
        return same(ref, p2send.at[way, step, sub], p2recv.at[way, step, sub], mate)

    for way, sub in ((0, 0), (1, 1), (0, 1), (1, 0)):
        z2_copy(way, 1, sub).start()
    for sub in (0, 1):
        m2_copy(0, 0, sub, core).start()
    for copy in w_copies[2:]:
        copy.wait()

    def beside(way):
        return xright if way == 0 else xleft

    def peer_at(way):
        return (tp + 1) % peers if way == 0 else (tp + peers - 1) % peers

    opposite = (tp + 2) % peers

    def a_near(way, pair, owner):
        return same(x_buf.at[pair, owner], asend.at[way, pair, 0], arecv.at[way, pair, 0], beside(way))

    def a_far(way, pair, owner):
        ref = x_buf.at[pair, owner, :, pl.ds(way * cols, cols)]
        return same(ref, asend.at[way, pair, 1], arecv.at[way, pair, 1], beside(way))

    def y_copy(way, pair, number):
        with_far = way * cols
        alone = (1 - way) * cols
        if number == 0:
            src = y_buf.at[pair, opposite, :, pl.ds(with_far, cols)]
            dst = y_first.at[pair, way]
        else:
            at = pl.ds(alone if number == 1 else with_far, cols)
            src = y_buf.at[pair, peer_at(way), :, at]
            dst = y_last.at[pair, way, :, at]
        return hop(src, dst, ysend.at[way, pair, number], yrecv.at[way, pair, number], beside(way))

    def e_copy(pair):
        return hop(
            e_buf.at[pair, 1 - core], e_mate.at[pair], esend.at[pair], erecv.at[pair], mate
        )

    def ring_arrivals(step):
        for turn in (0, 1):
            for way in (0, 1):
                sub = turn if way == 0 else 1 - turn

                def arrived(way=way, sub=sub, turn=turn):
                    z2_arrival(way, step, sub).wait_recv()
                    last = far if turn == 0 else far - 1
                    pl.when(step < last)(lambda: z2_copy(way, step + 1, sub).start())
                    m2_copy(way, step, sub, core).start()

                if turn == 0:
                    arrived()
                else:
                    pl.when(step < far)(arrived)

    def select(step):
        pair = step % far
        m2_copy(0, step, 0, 1 - core).wait_recv()
        m2_copy(1, step, 1, 1 - core).wait_recv()

        @pl.when(step < far)
        def _():
            m2_copy(0, step, 1, 1 - core).wait_recv()
            m2_copy(1, step, 0, 1 - core).wait_recv()

        @pl.when(step == far)
        def _():
            for sub in (0, 1):
                m2_copy(0, 0, sub, 1 - core).wait_recv()

        near = jnp.where(step == far, z, chip_at(0, step))
        total = None
        for number, (chip, owner) in enumerate(
            ((near, 0), (chip_at(1, step), 0), (near, 1), (chip_at(1, step), 1))
        ):
            device = chip * 2 + owner
            table = info[device]
            slot = lax.broadcasted_iota(jnp.int32, (4 * slots, rows), 0)
            want = jnp.where(slot // slots == number, sp * slots + slot % slots, -2).astype(F32)
            hit = jnp.logical_or(table[0:1, 0:rows] == want, table[1:2, 0:rows] == want)
            block = rows_buf[pl.ds(pl.multiple_of(device * rows, rows), rows)]
            picked = jnp.dot(
                jnp.where(hit, 1.0, 0.0).astype(BF16), block, preferred_element_type=F32
            )
            total = picked if total is None else total + picked
        x_buf[pair, tp] = total.astype(BF16)
        for way in (0, 1):
            a_near(way, pair, tp).start()

    def forward(step):
        pair = step % far
        for way in (0, 1):
            source = peer_at(1 - way)
            a_near(way, pair, source).wait_recv()
            a_far(way, pair, source).start()

    def run_expert(step):
        pair = step % far
        for way in (0, 1):
            a_far(way, pair, opposite).wait_recv()
        x = x_buf[pair].reshape(peers * 4 * slots, 2 * cols)
        gate = jnp.dot(x, gate_buf[...], preferred_element_type=F32)
        up = jnp.dot(x, up_buf[...], preferred_element_type=F32)
        hidden = (gate / (1.0 + jnp.exp(-gate)) * up).astype(BF16)
        y = jnp.dot(hidden, down_buf[...], preferred_element_type=F32)
        y_buf[pair] = y.astype(BF16).reshape(peers, 4 * slots, 2 * cols)
        for number in (0, 1):
            for way in (0, 1):
                y_copy(way, pair, number).start()

    def add_far(step):
        pair = step % far
        for way in (0, 1):
            y_copy(way, pair, 0).wait_recv()
            at = slice(way * cols, (way + 1) * cols)
            y_buf[pair, peer_at(way), :, at] = (
                y_buf[pair, peer_at(way), :, at].astype(F32) + y_first[pair, way].astype(F32)
            ).astype(BF16)
            y_copy(way, pair, 2).start()

    def finish(step):
        pair = step % far
        for way in (0, 1):
            y_copy(way, pair, 1).wait_recv()
            y_copy(way, pair, 2).wait_recv()
        total = y_buf[pair, tp].astype(F32)
        total = total + y_last[pair, 0].astype(F32) + y_last[pair, 1].astype(F32)
        e_buf[pair] = total.astype(BF16).reshape(2, 2 * slots, 2 * cols)
        e_copy(pair).start()

    stages = (ring_arrivals, select, forward, run_expert, add_far, finish)

    def tick(at, nothing):
        for lag, stage in enumerate(stages):
            step = at - lag
            pl.when(jnp.logical_and(step >= 1, step <= far))(functools.partial(stage, step))
        return nothing

    lax.fori_loop(1, far + len(stages), tick, 0)

    def contribution(chip, pair, which, sub):
        table = info[chip * 2 + core]
        slot = lax.broadcasted_iota(jnp.int32, (4 * slots, rows), 0)
        expert = jnp.where(slot < 2 * slots, sp, z * 2 + (1 - core))
        ours = (slot % (2 * slots)) // slots == which
        want = jnp.where(ours, expert * slots + slot % slots, -2).astype(F32)
        weight = jnp.where(table[0:1, 0:rows] == want, table[2:3, 0:rows], 0.0)
        weight = weight + jnp.where(table[1:2, 0:rows] == want, table[3:4, 0:rows], 0.0)
        coarse = weight.astype(BF16)
        fine = (weight - coarse.astype(F32)).astype(BF16)
        at = slice(sub * cols, (sub + 1) * cols)
        mine, other = e_buf[pair, core, :, at], e_mate[pair, :, at]
        return lax.dot_general(
            jnp.concatenate([coarse, fine], axis=0),
            jnp.concatenate([mine, other, mine, other], axis=0),
            (((0,), (0,)), ((), ())),
            preferred_element_type=F32,
        )

    def r_copy(way, step, sub):
        at = pl.ds(sub * cols, cols)
        return hop(
            ret_out.at[way, step, :, at],
            ret_in.at[way, step, :, at],
            rsend.at[way, step, sub],
            rrecv.at[way, step, sub],
            along(way),
        )

    e_copy(0).wait_recv()
    for way in (0, 1):
        at = slice(way * cols, (way + 1) * cols)
        ret_out[way, 0, :, at] = contribution((z + far) % chips, 0, 1, way).astype(BF16)
        r_copy(way, 0, way).start()
        rest = slice((1 - way) * cols, (2 - way) * cols)
        ret_in[way, 0, :, rest] = jnp.zeros((rows, cols), BF16)

    def back_step(step, nothing):
        distance = far - step
        e_copy(distance).wait_recv()
        for turn in (0, 1):
            for way in (0, 1):
                sub = turn if way == 0 else 1 - turn
                added = contribution(chip_at(1 - way, distance), distance, 1 - way, sub)
                if turn == 0:
                    r_copy(way, step - 1, sub).wait_recv()
                else:
                    pl.when(step > 1)(lambda: r_copy(way, step - 1, sub).wait_recv())
                at = slice(sub * cols, (sub + 1) * cols)
                ret_out[way, step, :, at] = (
                    added + ret_in[way, step - 1, :, at].astype(F32)
                ).astype(BF16)
                r_copy(way, step, sub).start()
        return nothing

    lax.fori_loop(1, far, back_step, 0)
    for sub in (0, 1):
        at = slice(sub * cols, (sub + 1) * cols)
        total = att_buf[:, at].astype(F32) + contribution(z, 0, 0, sub)
        for way in (0, 1):
            r_copy(way, far - 1, sub).wait_recv()
            total = total + ret_in[way, far - 1, :, at].astype(F32)
        out_ref[:, at] = total.astype(BF16)

    for way in (0, 1):
        for number in (0, 1, 2):
            x_copy(way, number).wait_send()
    for sub in (0, 1):
        m_copy(0, 0, sub, core).wait_send()
        m2_copy(0, 0, sub, core).wait_send()
    im_copy(0, 0, core).wait_send()

    def drain(step, nothing):
        for way in (0, 1):
            i_copy(way, step).wait_send()
            im_copy(way, step, core).wait_send()
            for sub in (0, 1):
                z_copy(way, step, sub).wait_send()
                m_copy(way, step, sub, core).wait_send()
                z2_copy(way, step, sub).wait_send()
                m2_copy(way, step, sub, core).wait_send()
                r_copy(way, step, sub).wait_send()
        return nothing

    lax.fori_loop(1, far, drain, 0)
    i_copy(0, far).wait_send()
    im_copy(0, far, core).wait_send()
    for way in (0, 1):
        z_copy(way, far, way).wait_send()
        m_copy(way, far, way, core).wait_send()
        z2_copy(way, far, way).wait_send()
        m2_copy(way, far, way, core).wait_send()
        r_copy(way, 0, way).wait_send()

    def drain_pairs(pair, nothing):
        e_copy(pair).wait_send()
        for way in (0, 1):
            a_near(way, pair, tp).wait_send()
            a_far(way, pair, peer_at(1 - way)).wait_send()
            for number in (0, 1, 2):
                y_copy(way, pair, number).wait_send()
        return nothing

    lax.fori_loop(0, far, drain_pairs, 0)


def layer(
    residual,
    queries_wide,
    keys_wide,
    values_wide,
    queries_narrow,
    keys_narrow,
    values_narrow,
    gains,
    tables,
    norm_gain,
    route,
    output_wide,
    output_narrow,
    gate_weight,
    up_weight,
    down_weight,
):
    chips = lax.axis_size("sp") // 2
    peers = lax.axis_size("tp")
    tok, wide = keys_wide.shape
    rows, width = residual.shape
    far = chips // 2
    picked = 4 * (2 * 2 * rows // (2 * chips))
    vmem = pl.BlockSpec(memory_space=pltpu.VMEM)
    hbm = pl.BlockSpec(memory_space=pl.ANY)
    dma = pltpu.SemaphoreType.DMA
    return pl.pallas_call(
        functools.partial(layer_kernel, chips, peers),
        out_shape=jax.ShapeDtypeStruct((rows, width), BF16),
        in_specs=[vmem] * 10 + [hbm] * 5,
        out_specs=vmem,
        scratch_shapes=[
            pltpu.VMEM((2 * chips * tok, 3 * wide), BF16),
            pltpu.VMEM((2 * tok, wide), BF16),
            pltpu.VMEM((2 * tok, wide), BF16),
            pltpu.VMEM((4, tok, wide), F32),
            pltpu.VMEM((4, tok, wide), F32),
            pltpu.VMEM((4, tok, wide), F32),
            pltpu.VMEM((tok, 3 * wide), BF16),
            pltpu.VMEM(output_wide.shape, BF16),
            pltpu.VMEM(output_narrow.shape, BF16),
            pltpu.VMEM((peers, rows, width), BF16),
            pltpu.VMEM((2, rows, width // 2), BF16),
            pltpu.VMEM((2, rows, width), BF16),
            pltpu.VMEM((2 * chips,) + route.shape, F32),
            pltpu.VMEM(gate_weight.shape[1:], BF16),
            pltpu.VMEM(up_weight.shape[1:], BF16),
            pltpu.VMEM(down_weight.shape[1:], BF16),
            pltpu.VMEM((rows, width), BF16),
            pltpu.VMEM((2 * chips * rows, width), BF16),
            pltpu.VMEM((far, peers, picked, width), BF16),
            pltpu.VMEM((far, peers, picked, width), BF16),
            pltpu.VMEM((far, 2, picked, width // 2), BF16),
            pltpu.VMEM((far, 2, picked, width), BF16),
            pltpu.VMEM((far, 2, picked // 2, width), BF16),
            pltpu.VMEM((far, picked // 2, width), BF16),
            pltpu.VMEM((2, far, rows, width), BF16),
            pltpu.VMEM((2, far, rows, width), BF16),
            dma((5,)),
            dma((2, far, 2)),
            dma((2, far, 2)),
            dma((2, far + 1, 2)),
            dma((2, far + 1, 2)),
            dma((2, far)),
            dma((2, far)),
            dma((2, far + 1)),
            dma((2, far + 1)),
            dma((2, 3)),
            dma((2, 3)),
            dma((2, far, 2)),
            dma((2, far, 2)),
            dma((2, far + 1, 2)),
            dma((2, far + 1, 2)),
            dma((2, far, 2)),
            dma((2, far, 2)),
            dma((2, far, 3)),
            dma((2, far, 3)),
            dma((far,)),
            dma((far,)),
            dma((2, far, 2)),
            dma((2, far, 2)),
        ],
        compiler_params=pltpu.CompilerParams(
            collective_id=0, has_side_effects=True, vmem_limit_bytes=64 * 1024 * 1024 - 65536
        ),
        name="layer",
    )(
        queries_wide,
        keys_wide,
        values_wide,
        queries_narrow,
        jnp.concatenate([keys_narrow, values_narrow], axis=1),
        gains,
        tables,
        residual,
        norm_gain.reshape(1, width),
        route,
        output_wide,
        output_narrow,
        gate_weight,
        up_weight,
        down_weight,
    )


def body(
    residual,
    queries_wide,
    keys_wide,
    values_wide,
    queries_narrow,
    keys_narrow,
    values_narrow,
    query_gain_wide,
    key_gain_wide,
    query_gain_narrow,
    key_gain_narrow,
    output_wide,
    output_narrow,
    norm_gain,
    gate_weight,
    up_weight,
    down_weight,
    route_ids,
    route_weights,
):
    tok_count = queries_wide.shape[0]
    places = lax.axis_index("sp") * tok_count + jnp.arange(tok_count, dtype=jnp.int32)
    wide_width = query_gain_wide.shape[0]
    narrow_width = query_gain_narrow.shape[0]
    wide_angles = angles_of(places, wide_width)
    narrow_angles = angles_of(places, narrow_width)
    narrow_angles = jnp.concatenate([narrow_angles, narrow_angles], axis=1)
    lanes = jnp.arange(wide_width, dtype=jnp.int32)
    wide_sign = jnp.where(lanes % (wide_width // 2) < wide_width // 4, -1.0, 1.0)
    narrow_sign = jnp.where(lanes % (narrow_width // 2) < narrow_width // 4, -1.0, 1.0)
    tables = jnp.stack(
        [
            jnp.cos(wide_angles),
            jnp.sin(wide_angles) * wide_sign,
            jnp.cos(narrow_angles),
            jnp.sin(narrow_angles) * narrow_sign,
        ]
    )
    gains = jnp.stack(
        [
            query_gain_wide,
            key_gain_wide,
            jnp.concatenate([query_gain_narrow, query_gain_narrow]),
            jnp.concatenate([key_gain_narrow, key_gain_narrow]),
        ]
    )
    own_rows = residual.shape[0]
    route = jnp.concatenate([route_ids.astype(F32), route_weights], axis=1).T
    route = jnp.pad(route, ((0, 4), (0, 128 - own_rows)), constant_values=-1.0)
    return layer(
        residual,
        queries_wide,
        keys_wide,
        values_wide,
        queries_narrow,
        keys_narrow,
        values_narrow,
        gains,
        tables,
        norm_gain,
        route,
        output_wide,
        output_narrow,
        gate_weight,
        up_weight,
        down_weight,
    )


def solution(mesh):
    return jax.shard_map(
        body,
        mesh=mesh,
        in_specs=(
            P(("grp", "sp", "tp"), None),
            P(("grp", "sp"), "tp"),
            P(("grp", "sp"), "tp"),
            P(("grp", "sp"), "tp"),
            P(("grp", "sp"), "tp"),
            P(("grp", "sp"), "tp"),
            P(("grp", "sp"), "tp"),
            P(),
            P(),
            P(),
            P(),
            P("tp", None),
            P("tp", None),
            P(),
            P("sp", None, "tp"),
            P("sp", None, "tp"),
            P("sp", "tp", None),
            P(("grp", "sp", "tp"), None),
            P(("grp", "sp", "tp"), None),
        ),
        out_specs=P(("grp", "sp", "tp"), None),
        check_vma=False,
    )
```

```python
import functools
import math

import jax
import jax.numpy as jnp
from jax import lax
from jax.experimental import pallas as pl
from jax.experimental.pallas import tpu as pltpu
from jax.sharding import PartitionSpec as P

GRID = 64
THETA = 10000.0
EPS = 1e-06
NEG_BIG = -1e30
LOG2E = math.log2(math.e)
MESH = pl.DeviceIdType.MESH
F32 = jnp.float32
BF16 = jnp.bfloat16


def angles_of(places, head_width):
    quarter = head_width // 4
    inv_freq = THETA ** (-jnp.arange(quarter, dtype=jnp.float32) / quarter)
    grid_rows = (places // GRID).astype(jnp.float32)
    grid_cols = (places % GRID).astype(jnp.float32)
    row_angle = grid_rows[:, None] * inv_freq[None, :]
    col_angle = grid_cols[:, None] * inv_freq[None, :]
    return jnp.concatenate([row_angle, row_angle, col_angle, col_angle], axis=-1)


def lane_ids(shape):
    return lax.broadcasted_iota(jnp.int32, shape, 1)


def turned_lanes(values, quarter):
    lanes = lane_ids(values.shape)
    width = values.shape[1]
    return jnp.where(
        lanes % (2 * quarter) < quarter,
        pltpu.roll(values, width - quarter, 1),
        pltpu.roll(values, quarter, 1),
    )


def rotate(values, cos_table, sin_table, quarter):
    return values * cos_table + turned_lanes(values, quarter) * sin_table


def norm_wide(values, gain):
    mean = jnp.mean(values * values, axis=-1, keepdims=True)
    return values * lax.rsqrt(mean + EPS) * gain


def norm_halves(values, gain):
    lanes = lane_ids(values.shape)
    half = values.shape[1] // 2
    squares = values * values
    low = jnp.sum(jnp.where(lanes < half, squares, 0.0), axis=-1, keepdims=True) / half
    high = jnp.sum(jnp.where(lanes < half, 0.0, squares), axis=-1, keepdims=True) / half
    scale = jnp.where(lanes < half, lax.rsqrt(low + EPS), lax.rsqrt(high + EPS))
    return values * scale * gain


def layer_kernel(
    chips,
    peers,
    qw_ref,
    kw_ref,
    vw_ref,
    qn_ref,
    kvn_ref,
    gains_ref,
    tables_ref,
    res_ref,
    norm_gain_ref,
    route_ref,
    ow_hbm,
    on_hbm,
    gate_hbm,
    up_hbm,
    down_hbm,
    out_ref,
    kv_buf,
    qws,
    qns,
    m_buf,
    l_buf,
    acc_buf,
    heads,
    ow_buf,
    on_buf,
    part,
    first_in,
    last_in,
    info,
    gate_buf,
    up_buf,
    down_buf,
    att_buf,
    rows_buf,
    x_buf,
    y_buf,
    y_first,
    y_last,
    e_buf,
    e_mate,
    ret_out,
    ret_in,
    w_sem,
    zsend,
    zrecv,
    psend,
    precv,
    isend,
    irecv,
    imsend,
    imrecv,
    xsend,
    xrecv,
    z2send,
    z2recv,
    p2send,
    p2recv,
    asend,
    arecv,
    ysend,
    yrecv,
    esend,
    erecv,
    rsend,
    rrecv,
):
    tok = qw_ref.shape[0]
    half = tok // 2
    wide = kw_ref.shape[1]
    sp = lax.axis_index("sp")
    tp = lax.axis_index("tp")
    z, core = sp // 2, sp % 2
    far = chips // 2
    right = {"sp": ((z + 1) % chips) * 2 + core}
    left = {"sp": ((z + chips - 1) % chips) * 2 + core}
    mate = {"sp": z * 2 + (1 - core)}
    xright = {"tp": (tp + 1) % peers}
    xleft = {"tp": (tp + peers - 1) % peers}

    w_copies = [
        pltpu.make_async_copy(ow_hbm, ow_buf, w_sem.at[0]),
        pltpu.make_async_copy(on_hbm, on_buf, w_sem.at[1]),
        pltpu.make_async_copy(gate_hbm.at[0], gate_buf, w_sem.at[2]),
        pltpu.make_async_copy(up_hbm.at[0], up_buf, w_sem.at[3]),
        pltpu.make_async_copy(down_hbm.at[0], down_buf, w_sem.at[4]),
    ]
    for copy in w_copies:
        copy.start()

    barrier = pltpu.get_barrier_semaphore()
    for other in (right, left, mate, xright, xleft):
        pl.semaphore_signal(barrier, inc=1, device_id=other, device_id_type=MESH)

    def rows_of(chip, owner, sub):
        at = pl.multiple_of((chip * 2 + owner) * tok + sub * half, half)
        return kv_buf.at[pl.ds(at, half)]

    cos_w, sin_w = tables_ref[0], tables_ref[1]
    cos_n, sin_n = tables_ref[2], tables_ref[3]
    own = pl.ds(pl.multiple_of(sp * tok, tok), tok)
    k_wide = rotate(norm_wide(kw_ref[...].astype(F32), gains_ref[1:2]), cos_w, sin_w, wide // 4)
    kvn = kvn_ref[...].astype(F32)
    k_narrow = rotate(norm_halves(kvn, gains_ref[3:4]), cos_n, sin_n, wide // 8)
    kv_buf[own, 0:wide] = k_wide.astype(BF16)
    kv_buf[own, wide : 2 * wide] = vw_ref[...]
    kv_buf[own, 2 * wide : 3 * wide] = jnp.where(
        lane_ids(kvn.shape) < wide // 2, k_narrow, kvn
    ).astype(BF16)

    slots = 2 * 2 * res_ref.shape[0] // (2 * chips)
    route = route_ref[...]
    lanes = route.shape[1]
    experts = lax.broadcasted_iota(jnp.int32, (2 * chips, lanes), 0).astype(F32)
    hits = [(route[k : k + 1] == experts).astype(F32) for k in (0, 1)]
    earlier = (
        lax.broadcasted_iota(jnp.int32, (lanes, lanes), 0)
        < lax.broadcasted_iota(jnp.int32, (lanes, lanes), 1)
    ).astype(BF16)
    places = jnp.dot((hits[0] + hits[1]).astype(BF16), earlier, preferred_element_type=F32)
    targets = [
        jnp.sum(hit * (places + experts * slots), axis=0, keepdims=True) for hit in hits
    ]
    row = lax.broadcasted_iota(jnp.int32, route.shape, 0)
    info[sp] = jnp.where(row == 0, targets[0], jnp.where(row == 1, targets[1], route))

    pl.semaphore_wait(barrier, 5)

    def hop(src, dst, send, recv, device):
        return pltpu.make_async_remote_copy(
            src_ref=src,
            dst_ref=dst,
            send_sem=send,
            recv_sem=recv,
            device_id=device,
            device_id_type=MESH,
        )

    def same(ref, send, recv, device):
        return hop(ref, ref, send, recv, device)

    def chip_at(way, distance):
        return (z + chips - distance) % chips if way == 0 else (z + distance) % chips

    def along(way):
        return right if way == 0 else left

    def z_copy(way, step, sub):
        ref = rows_of(chip_at(way, step - 1), core, sub)
        return same(ref, zsend.at[way, step - 1, sub], zrecv.at[way, step - 1, sub], along(way))

    def z_arrival(way, step, sub):
        ref = rows_of(chip_at(way, step), core, sub)
        return same(ref, zsend.at[way, step - 1, sub], zrecv.at[way, step - 1, sub], along(way))

    def m_copy(way, step, sub, owner):
        ref = rows_of(chip_at(way, step), owner, sub)
        return same(ref, psend.at[way, step, sub], precv.at[way, step, sub], mate)

    def i_copy(way, step):
        ref = info.at[chip_at(way, step - 1) * 2 + core]
        return same(ref, isend.at[way, step - 1], irecv.at[way, step - 1], along(way))

    def i_arrival(way, step):
        ref = info.at[chip_at(way, step) * 2 + core]
        return same(ref, isend.at[way, step - 1], irecv.at[way, step - 1], along(way))

    def im_copy(way, step, owner):
        ref = info.at[chip_at(way, step) * 2 + owner]
        return same(ref, imsend.at[way, step], imrecv.at[way, step], mate)

    for way in (0, 1):
        i_copy(way, 1).start()
    im_copy(0, 0, core).start()
    for way, sub in ((0, 0), (1, 1), (0, 1), (1, 0)):
        z_copy(way, 1, sub).start()
    for sub in (0, 1):
        m_copy(0, 0, sub, core).start()

    qw = qw_ref[...].astype(F32)
    for head in (0, 1):
        q = norm_wide(qw[:, head * wide : (head + 1) * wide], gains_ref[0:1])
        qws[head * tok : (head + 1) * tok] = rotate(q, cos_w, sin_w, wide // 4).astype(BF16)
    qn = rotate(norm_halves(qn_ref[...].astype(F32), gains_ref[2:3]), cos_n, sin_n, wide // 8)
    low = lane_ids(qn.shape) < wide // 2
    qns[0:tok] = jnp.where(low, qn, 0.0).astype(BF16)
    qns[tok : 2 * tok] = jnp.where(low, pltpu.roll(qn, wide // 2, 1), 0.0).astype(BF16)
    m_buf[...] = jnp.full(m_buf.shape, NEG_BIG, F32)
    l_buf[...] = jnp.zeros(l_buf.shape, F32)
    acc_buf[...] = jnp.zeros(acc_buf.shape, F32)

    def attend_chip(chip):
        keys = pl.ds(pl.multiple_of(chip * 2 * tok, 2 * tok), 2 * tok)
        k_w, v_w = kv_buf[keys, 0:wide], kv_buf[keys, wide : 2 * wide]
        kv_n = kv_buf[keys, 2 * wide : 3 * wide]
        work = []
        for kind in (0, 1):
            for head in (0, 1):
                work.append((kind, head))

        def scores(kind, head):
            q = (qws if kind == 0 else qns)[head * tok : (head + 1) * tok]
            return lax.dot_general(
                q,
                k_w if kind == 0 else kv_n,
                (((1,), (1,)), ((), ())),
                preferred_element_type=F32,
            )

        upcoming = scores(*work[0])
        for at, (kind, head) in enumerate(work):
            s = upcoming
            if at + 1 < len(work):
                upcoming = scores(*work[at + 1])
            factor = LOG2E * (wide if kind == 0 else wide // 2) ** (-0.5)
            m_old = m_buf[at]
            m_new = jnp.maximum(m_old, jnp.max(s, axis=-1, keepdims=True))
            alpha = jnp.exp2((m_old - m_new) * factor)
            parts = [
                jnp.exp2((s[:, i * wide : (i + 1) * wide] - m_new) * factor)
                for i in range(s.shape[1] // wide)
            ]
            total = parts[0]
            for p in parts[1:]:
                total = total + p
            weights = jnp.concatenate([p.astype(BF16) for p in parts], axis=1)
            mixed = jnp.dot(
                weights, v_w if kind == 0 else kv_n, preferred_element_type=F32
            )
            m_buf[at] = m_new
            l_buf[at] = l_buf[at] * alpha + total
            acc_buf[at] = acc_buf[at] * alpha + mixed

    def ring_step(step, nothing):
        def pass_on(way):
            i_arrival(way, step).wait_recv()
            if way == 0:
                pl.when(step < far)(lambda: i_copy(way, step + 1).start())
            else:
                pl.when(step < far - 1)(lambda: i_copy(way, step + 1).start())
            im_copy(way, step, core).start()

        @pl.when(step <= far)
        def _():
            pass_on(0)
            pl.when(step < far)(functools.partial(pass_on, 1))
            for turn in (0, 1):
                for way in (0, 1):
                    sub = turn if way == 0 else 1 - turn

                    def arrived(way=way, sub=sub, turn=turn):
                        z_arrival(way, step, sub).wait_recv()
                        if turn == 0:

                            @pl.when(step < far)
                            def _():
                                z_copy(way, step + 1, sub).start()
                        else:

                            @pl.when(step < far - 1)
                            def _():
                                z_copy(way, step + 1, sub).start()

                        m_copy(way, step, sub, core).start()

                    if turn == 0:
                        arrived()
                    else:
                        pl.when(step < far)(arrived)

        before = step - 1

        @pl.when(before == 0)
        def _():
            im_copy(0, 0, 1 - core).wait_recv()
            for sub in (0, 1):
                m_copy(0, 0, sub, 1 - core).wait_recv()

        @pl.when(before > 0)
        def _():
            im_copy(0, before, 1 - core).wait_recv()
            m_copy(0, before, 0, 1 - core).wait_recv()
            m_copy(1, before, 1, 1 - core).wait_recv()

        @pl.when(jnp.logical_and(before > 0, before < far))
        def _():
            im_copy(1, before, 1 - core).wait_recv()
            m_copy(0, before, 1, 1 - core).wait_recv()
            m_copy(1, before, 0, 1 - core).wait_recv()

        def one(side, nothing):
            attend_chip((z + chips + before * (2 * side - 1)) % chips)
            return nothing

        single = jnp.logical_or(before == 0, before == far)
        return lax.fori_loop(0, jnp.where(single, 1, 2), one, nothing)

    lax.fori_loop(1, far + 2, ring_step, 0)

    outs = []
    for at in range(4):
        outs.append(acc_buf[at] / jnp.sum(l_buf[at], axis=-1, keepdims=True))
    heads[:, 0:wide] = outs[0].astype(BF16)
    heads[:, wide : 2 * wide] = outs[1].astype(BF16)
    heads[:, 2 * wide : 3 * wide] = jnp.where(
        low, pltpu.roll(outs[2], wide // 2, 1), outs[3]
    ).astype(BF16)
    for copy in w_copies[:2]:
        copy.wait()

    rows = res_ref.shape[0]
    cols = res_ref.shape[1] // 2

    def x_copy(way, number):
        dest = (tp + 1) % peers if way == 0 else (tp + peers - 1) % peers
        with_far = way * cols
        alone = (1 - way) * cols
        if number == 0:
            src = part.at[(tp + 2) % peers, :, pl.ds(with_far, cols)]
            dst = first_in.at[way]
        else:
            at = pl.ds(alone if number == 1 else with_far, cols)
            src = part.at[dest, :, at]
            dst = last_in.at[way, :, at]
        return pltpu.make_async_remote_copy(
            src_ref=src,
            dst_ref=dst,
            send_sem=xsend.at[way, number],
            recv_sem=xrecv.at[way, number],
            device_id=xright if way == 0 else xleft,
            device_id_type=MESH,
        )

    def project(peer):
        h = heads[pl.ds(pl.multiple_of(peer * rows, rows), rows)]
        product = jnp.dot(h[:, 0 : 2 * wide], ow_buf[...], preferred_element_type=F32)
        product = product + jnp.dot(
            h[:, 2 * wide : 3 * wide], on_buf[...], preferred_element_type=F32
        )
        part[peer] = product.astype(BF16)

    project((tp + 2) % peers)
    x_copy(0, 0).start()
    x_copy(1, 0).start()
    project((tp + 1) % peers)
    x_copy(0, 1).start()
    project((tp + peers - 1) % peers)
    x_copy(1, 1).start()
    project(tp)
    for way in (0, 1):
        dest = (tp + 1) % peers if way == 0 else (tp + peers - 1) % peers
        x_copy(way, 0).wait_recv()
        at = slice(way * cols, (way + 1) * cols)
        part[dest, :, at] = (
            part[dest, :, at].astype(F32) + first_in[way].astype(F32)
        ).astype(BF16)
        x_copy(way, 2).start()
    for way in (0, 1):
        x_copy(way, 1).wait_recv()
        x_copy(way, 2).wait_recv()
    total = res_ref[...].astype(F32) + part[tp].astype(F32)
    total = total + last_in[0].astype(F32) + last_in[1].astype(F32)
    attended = total.astype(BF16)
    att_buf[...] = attended
    state = attended.astype(F32)
    mean = jnp.mean(state * state, axis=-1, keepdims=True)
    normed = (state * lax.rsqrt(mean + EPS) * norm_gain_ref[...]).astype(BF16)
    rows_buf[pl.ds(pl.multiple_of(sp * rows, rows), rows)] = normed

    def block_of(chip, owner, sub):
        at = pl.multiple_of((chip * 2 + owner) * rows + sub * (rows // 2), rows // 2)
        return rows_buf.at[pl.ds(at, rows // 2)]

    def z2_copy(way, step, sub):
        ref = block_of(chip_at(way, step - 1), core, sub)
        return same(ref, z2send.at[way, step - 1, sub], z2recv.at[way, step - 1, sub], along(way))

    def z2_arrival(way, step, sub):
        ref = block_of(chip_at(way, step), core, sub)
        return same(ref, z2send.at[way, step - 1, sub], z2recv.at[way, step - 1, sub], along(way))

    def m2_copy(way, step, sub, owner):
        ref = block_of(chip_at(way, step), owner, sub)
        return same(ref, p2send.at[way, step, sub], p2recv.at[way, step, sub], mate)

    for way, sub in ((0, 0), (1, 1), (0, 1), (1, 0)):
        z2_copy(way, 1, sub).start()
    for sub in (0, 1):
        m2_copy(0, 0, sub, core).start()
    for copy in w_copies[2:]:
        copy.wait()

    def beside(way):
        return xright if way == 0 else xleft

    def peer_at(way):
        return (tp + 1) % peers if way == 0 else (tp + peers - 1) % peers

    opposite = (tp + 2) % peers

    def a_near(way, pair, owner):
        return same(x_buf.at[pair, owner], asend.at[way, pair, 0], arecv.at[way, pair, 0], beside(way))

    def a_far(way, pair, owner):
        ref = x_buf.at[pair, owner, :, pl.ds(way * cols, cols)]
        return same(ref, asend.at[way, pair, 1], arecv.at[way, pair, 1], beside(way))

    def y_copy(way, pair, number):
        with_far = way * cols
        alone = (1 - way) * cols
        if number == 0:
            src = y_buf.at[pair, opposite, :, pl.ds(with_far, cols)]
            dst = y_first.at[pair, way]
        else:
            at = pl.ds(alone if number == 1 else with_far, cols)
            src = y_buf.at[pair, peer_at(way), :, at]
            dst = y_last.at[pair, way, :, at]
        return hop(src, dst, ysend.at[way, pair, number], yrecv.at[way, pair, number], beside(way))

    def e_copy(pair):
        return hop(
            e_buf.at[pair, 1 - core], e_mate.at[pair], esend.at[pair], erecv.at[pair], mate
        )

    def ring_arrivals(step):
        for turn in (0, 1):
            for way in (0, 1):
                sub = turn if way == 0 else 1 - turn

                def arrived(way=way, sub=sub, turn=turn):
                    z2_arrival(way, step, sub).wait_recv()
                    last = far if turn == 0 else far - 1
                    pl.when(step < last)(lambda: z2_copy(way, step + 1, sub).start())
                    m2_copy(way, step, sub, core).start()

                if turn == 0:
                    arrived()
                else:
                    pl.when(step < far)(arrived)

    def select(step):
        pair = step % far
        m2_copy(0, step, 0, 1 - core).wait_recv()
        m2_copy(1, step, 1, 1 - core).wait_recv()

        @pl.when(step < far)
        def _():
            m2_copy(0, step, 1, 1 - core).wait_recv()
            m2_copy(1, step, 0, 1 - core).wait_recv()

        @pl.when(step == far)
        def _():
            for sub in (0, 1):
                m2_copy(0, 0, sub, 1 - core).wait_recv()

        near = jnp.where(step == far, z, chip_at(0, step))
        total = None
        for number, (chip, owner) in enumerate(
            ((near, 0), (chip_at(1, step), 0), (near, 1), (chip_at(1, step), 1))
        ):
            device = chip * 2 + owner
            table = info[device]
            slot = lax.broadcasted_iota(jnp.int32, (4 * slots, rows), 0)
            want = jnp.where(slot // slots == number, sp * slots + slot % slots, -2).astype(F32)
            hit = jnp.logical_or(table[0:1, 0:rows] == want, table[1:2, 0:rows] == want)
            block = rows_buf[pl.ds(pl.multiple_of(device * rows, rows), rows)]
            picked = jnp.dot(
                jnp.where(hit, 1.0, 0.0).astype(BF16), block, preferred_element_type=F32
            )
            total = picked if total is None else total + picked
        x_buf[pair, tp] = total.astype(BF16)
        for way in (0, 1):
            a_near(way, pair, tp).start()

    def forward(step):
        pair = step % far
        for way in (0, 1):
            source = peer_at(1 - way)
            a_near(way, pair, source).wait_recv()
            a_far(way, pair, source).start()

    def run_expert(step):
        pair = step % far
        for way in (0, 1):
            a_far(way, pair, opposite).wait_recv()
        x = x_buf[pair].reshape(peers * 4 * slots, 2 * cols)
        gate = jnp.dot(x, gate_buf[...], preferred_element_type=F32)
        up = jnp.dot(x, up_buf[...], preferred_element_type=F32)
        hidden = (gate / (1.0 + jnp.exp(-gate)) * up).astype(BF16)
        y = jnp.dot(hidden, down_buf[...], preferred_element_type=F32)
        y_buf[pair] = y.astype(BF16).reshape(peers, 4 * slots, 2 * cols)
        pl.when(step >= far - 1)(lambda: begin_sum(step))

    def begin_sum(step):
        pair = step % far
        for number in (0, 1):
            for way in (0, 1):
                y_copy(way, pair, number).start()

    def add_far(step):
        pair = step % far
        for way in (0, 1):
            y_copy(way, pair, 0).wait_recv()
            at = slice(way * cols, (way + 1) * cols)
            y_buf[pair, peer_at(way), :, at] = (
                y_buf[pair, peer_at(way), :, at].astype(F32) + y_first[pair, way].astype(F32)
            ).astype(BF16)
            y_copy(way, pair, 2).start()

    def finish(step):
        pair = step % far
        for way in (0, 1):
            y_copy(way, pair, 1).wait_recv()
            y_copy(way, pair, 2).wait_recv()
        total = y_buf[pair, tp].astype(F32)
        total = total + y_last[pair, 0].astype(F32) + y_last[pair, 1].astype(F32)
        e_buf[pair] = total.astype(BF16).reshape(2, 2 * slots, 2 * cols)
        e_copy(pair).start()

    stages = (ring_arrivals, select, forward, run_expert)

    def tick(at, nothing):
        for lag, stage in enumerate(stages):
            step = at - lag
            pl.when(jnp.logical_and(step >= 1, step <= far))(functools.partial(stage, step))
        return nothing

    lax.fori_loop(1, far + len(stages), tick, 0)

    def contribution(chip, pair, which, sub):
        table = info[chip * 2 + core]
        slot = lax.broadcasted_iota(jnp.int32, (4 * slots, rows), 0)
        expert = jnp.where(slot < 2 * slots, sp, z * 2 + (1 - core))
        ours = (slot % (2 * slots)) // slots == which
        want = jnp.where(ours, expert * slots + slot % slots, -2).astype(F32)
        weight = jnp.where(table[0:1, 0:rows] == want, table[2:3, 0:rows], 0.0)
        weight = weight + jnp.where(table[1:2, 0:rows] == want, table[3:4, 0:rows], 0.0)
        coarse = weight.astype(BF16)
        fine = (weight - coarse.astype(F32)).astype(BF16)
        at = slice(sub * cols, (sub + 1) * cols)
        mine, other = e_buf[pair, core, :, at], e_mate[pair, :, at]
        return lax.dot_general(
            jnp.concatenate([coarse, fine], axis=0),
            jnp.concatenate([mine, other, mine, other], axis=0),
            (((0,), (0,)), ((), ())),
            preferred_element_type=F32,
        )

    def r_copy(way, step, sub):
        at = pl.ds(sub * cols, cols)
        return hop(
            ret_out.at[way, step, :, at],
            ret_in.at[way, step, :, at],
            rsend.at[way, step, sub],
            rrecv.at[way, step, sub],
            along(way),
        )

    for way in (0, 1):
        rest = slice((1 - way) * cols, (2 - way) * cols)
        ret_in[way, 0, :, rest] = jnp.zeros((rows, cols), BF16)

    def start_back():
        for way in (0, 1):
            at = slice(way * cols, (way + 1) * cols)
            ret_out[way, 0, :, at] = contribution((z + far) % chips, 0, 1, way).astype(BF16)
            r_copy(way, 0, way).start()

    def go_back(distance):
        step = far - distance
        for turn in (0, 1):
            for way in (0, 1):
                sub = turn if way == 0 else 1 - turn
                added = contribution(chip_at(1 - way, distance), distance, 1 - way, sub)
                if turn == 0:
                    r_copy(way, step - 1, sub).wait_recv()
                else:
                    pl.when(step > 1)(lambda: r_copy(way, step - 1, sub).wait_recv())
                at = slice(sub * cols, (sub + 1) * cols)
                ret_out[way, step, :, at] = (
                    added + ret_in[way, step - 1, :, at].astype(F32)
                ).astype(BF16)
                r_copy(way, step, sub).start()

    def back(distance):
        e_copy(distance % far).wait_recv()
        pl.when(distance == far)(start_back)
        pl.when(distance < far)(functools.partial(go_back, distance))

    back_stages = ((2, back), (1, finish), (0, add_far), (-2, begin_sum))

    def back_tick(at, nothing):
        for lag, stage in back_stages:
            step = far - at + lag
            last = far - 2 if stage is begin_sum else far
            pl.when(jnp.logical_and(step >= 1, step <= last))(functools.partial(stage, step))
        return nothing

    lax.fori_loop(0, far + 2, back_tick, 0)
    for sub in (0, 1):
        at = slice(sub * cols, (sub + 1) * cols)
        total = att_buf[:, at].astype(F32) + contribution(z, 0, 0, sub)
        for way in (0, 1):
            r_copy(way, far - 1, sub).wait_recv()
            total = total + ret_in[way, far - 1, :, at].astype(F32)
        out_ref[:, at] = total.astype(BF16)

    for way in (0, 1):
        for number in (0, 1, 2):
            x_copy(way, number).wait_send()
    for sub in (0, 1):
        m_copy(0, 0, sub, core).wait_send()
        m2_copy(0, 0, sub, core).wait_send()
    im_copy(0, 0, core).wait_send()

    def drain(step, nothing):
        for way in (0, 1):
            i_copy(way, step).wait_send()
            im_copy(way, step, core).wait_send()
            for sub in (0, 1):
                z_copy(way, step, sub).wait_send()
                m_copy(way, step, sub, core).wait_send()
                z2_copy(way, step, sub).wait_send()
                m2_copy(way, step, sub, core).wait_send()
                r_copy(way, step, sub).wait_send()
        return nothing

    lax.fori_loop(1, far, drain, 0)
    i_copy(0, far).wait_send()
    im_copy(0, far, core).wait_send()
    for way in (0, 1):
        z_copy(way, far, way).wait_send()
        m_copy(way, far, way, core).wait_send()
        z2_copy(way, far, way).wait_send()
        m2_copy(way, far, way, core).wait_send()
        r_copy(way, 0, way).wait_send()

    def drain_pairs(pair, nothing):
        e_copy(pair).wait_send()
        for way in (0, 1):
            a_near(way, pair, tp).wait_send()
            a_far(way, pair, peer_at(1 - way)).wait_send()
            for number in (0, 1, 2):
                y_copy(way, pair, number).wait_send()
        return nothing

    lax.fori_loop(0, far, drain_pairs, 0)


def layer(
    residual,
    queries_wide,
    keys_wide,
    values_wide,
    queries_narrow,
    keys_narrow,
    values_narrow,
    gains,
    tables,
    norm_gain,
    route,
    output_wide,
    output_narrow,
    gate_weight,
    up_weight,
    down_weight,
):
    chips = lax.axis_size("sp") // 2
    peers = lax.axis_size("tp")
    tok, wide = keys_wide.shape
    rows, width = residual.shape
    far = chips // 2
    picked = 4 * (2 * 2 * rows // (2 * chips))
    vmem = pl.BlockSpec(memory_space=pltpu.VMEM)
    hbm = pl.BlockSpec(memory_space=pl.ANY)
    dma = pltpu.SemaphoreType.DMA
    return pl.pallas_call(
        functools.partial(layer_kernel, chips, peers),
        out_shape=jax.ShapeDtypeStruct((rows, width), BF16),
        in_specs=[vmem] * 10 + [hbm] * 5,
        out_specs=vmem,
        scratch_shapes=[
            pltpu.VMEM((2 * chips * tok, 3 * wide), BF16),
            pltpu.VMEM((2 * tok, wide), BF16),
            pltpu.VMEM((2 * tok, wide), BF16),
            pltpu.VMEM((4, tok, wide), F32),
            pltpu.VMEM((4, tok, wide), F32),
            pltpu.VMEM((4, tok, wide), F32),
            pltpu.VMEM((tok, 3 * wide), BF16),
            pltpu.VMEM(output_wide.shape, BF16),
            pltpu.VMEM(output_narrow.shape, BF16),
            pltpu.VMEM((peers, rows, width), BF16),
            pltpu.VMEM((2, rows, width // 2), BF16),
            pltpu.VMEM((2, rows, width), BF16),
            pltpu.VMEM((2 * chips,) + route.shape, F32),
            pltpu.VMEM(gate_weight.shape[1:], BF16),
            pltpu.VMEM(up_weight.shape[1:], BF16),
            pltpu.VMEM(down_weight.shape[1:], BF16),
            pltpu.VMEM((rows, width), BF16),
            pltpu.VMEM((2 * chips * rows, width), BF16),
            pltpu.VMEM((far, peers, picked, width), BF16),
            pltpu.VMEM((far, peers, picked, width), BF16),
            pltpu.VMEM((far, 2, picked, width // 2), BF16),
            pltpu.VMEM((far, 2, picked, width), BF16),
            pltpu.VMEM((far, 2, picked // 2, width), BF16),
            pltpu.VMEM((far, picked // 2, width), BF16),
            pltpu.VMEM((2, far, rows, width), BF16),
            pltpu.VMEM((2, far, rows, width), BF16),
            dma((5,)),
            dma((2, far, 2)),
            dma((2, far, 2)),
            dma((2, far + 1, 2)),
            dma((2, far + 1, 2)),
            dma((2, far)),
            dma((2, far)),
            dma((2, far + 1)),
            dma((2, far + 1)),
            dma((2, 3)),
            dma((2, 3)),
            dma((2, far, 2)),
            dma((2, far, 2)),
            dma((2, far + 1, 2)),
            dma((2, far + 1, 2)),
            dma((2, far, 2)),
            dma((2, far, 2)),
            dma((2, far, 3)),
            dma((2, far, 3)),
            dma((far,)),
            dma((far,)),
            dma((2, far, 2)),
            dma((2, far, 2)),
        ],
        compiler_params=pltpu.CompilerParams(
            collective_id=0, has_side_effects=True, vmem_limit_bytes=64 * 1024 * 1024 - 65536
        ),
        name="layer",
    )(
        queries_wide,
        keys_wide,
        values_wide,
        queries_narrow,
        jnp.concatenate([keys_narrow, values_narrow], axis=1),
        gains,
        tables,
        residual,
        norm_gain.reshape(1, width),
        route,
        output_wide,
        output_narrow,
        gate_weight,
        up_weight,
        down_weight,
    )


def body(
    residual,
    queries_wide,
    keys_wide,
    values_wide,
    queries_narrow,
    keys_narrow,
    values_narrow,
    query_gain_wide,
    key_gain_wide,
    query_gain_narrow,
    key_gain_narrow,
    output_wide,
    output_narrow,
    norm_gain,
    gate_weight,
    up_weight,
    down_weight,
    route_ids,
    route_weights,
):
    tok_count = queries_wide.shape[0]
    places = lax.axis_index("sp") * tok_count + jnp.arange(tok_count, dtype=jnp.int32)
    wide_width = query_gain_wide.shape[0]
    narrow_width = query_gain_narrow.shape[0]
    wide_angles = angles_of(places, wide_width)
    narrow_angles = angles_of(places, narrow_width)
    narrow_angles = jnp.concatenate([narrow_angles, narrow_angles], axis=1)
    lanes = jnp.arange(wide_width, dtype=jnp.int32)
    wide_sign = jnp.where(lanes % (wide_width // 2) < wide_width // 4, -1.0, 1.0)
    narrow_sign = jnp.where(lanes % (narrow_width // 2) < narrow_width // 4, -1.0, 1.0)
    tables = jnp.stack(
        [
            jnp.cos(wide_angles),
            jnp.sin(wide_angles) * wide_sign,
            jnp.cos(narrow_angles),
            jnp.sin(narrow_angles) * narrow_sign,
        ]
    )
    gains = jnp.stack(
        [
            query_gain_wide,
            key_gain_wide,
            jnp.concatenate([query_gain_narrow, query_gain_narrow]),
            jnp.concatenate([key_gain_narrow, key_gain_narrow]),
        ]
    )
    own_rows = residual.shape[0]
    route = jnp.concatenate([route_ids.astype(F32), route_weights], axis=1).T
    route = jnp.pad(route, ((0, 4), (0, 128 - own_rows)), constant_values=-1.0)
    return layer(
        residual,
        queries_wide,
        keys_wide,
        values_wide,
        queries_narrow,
        keys_narrow,
        values_narrow,
        gains,
        tables,
        norm_gain,
        route,
        output_wide,
        output_narrow,
        gate_weight,
        up_weight,
        down_weight,
    )


def solution(mesh):
    return jax.shard_map(
        body,
        mesh=mesh,
        in_specs=(
            P(("grp", "sp", "tp"), None),
            P(("grp", "sp"), "tp"),
            P(("grp", "sp"), "tp"),
            P(("grp", "sp"), "tp"),
            P(("grp", "sp"), "tp"),
            P(("grp", "sp"), "tp"),
            P(("grp", "sp"), "tp"),
            P(),
            P(),
            P(),
            P(),
            P("tp", None),
            P("tp", None),
            P(),
            P("sp", None, "tp"),
            P("sp", None, "tp"),
            P("sp", "tp", None),
            P(("grp", "sp", "tp"), None),
            P(("grp", "sp", "tp"), None),
        ),
        out_specs=P(("grp", "sp", "tp"), None),
        check_vma=False,
    )
```

```python
import functools
import math

import jax
import jax.numpy as jnp
from jax import lax
from jax.experimental import pallas as pl
from jax.experimental.pallas import tpu as pltpu
from jax.sharding import PartitionSpec as P

GRID = 64
FAR_STEPS = 3
THETA = 10000.0
EPS = 1e-06
NEG_BIG = -1e30
LOG2E = math.log2(math.e)
MESH = pl.DeviceIdType.MESH
F32 = jnp.float32
BF16 = jnp.bfloat16


def angles_of(places, head_width):
    quarter = head_width // 4
    inv_freq = THETA ** (-jnp.arange(quarter, dtype=jnp.float32) / quarter)
    grid_rows = (places // GRID).astype(jnp.float32)
    grid_cols = (places % GRID).astype(jnp.float32)
    row_angle = grid_rows[:, None] * inv_freq[None, :]
    col_angle = grid_cols[:, None] * inv_freq[None, :]
    return jnp.concatenate([row_angle, row_angle, col_angle, col_angle], axis=-1)


def lane_ids(shape):
    return lax.broadcasted_iota(jnp.int32, shape, 1)


def turned_lanes(values, quarter):
    lanes = lane_ids(values.shape)
    width = values.shape[1]
    return jnp.where(
        lanes % (2 * quarter) < quarter,
        pltpu.roll(values, width - quarter, 1),
        pltpu.roll(values, quarter, 1),
    )


def rotate(values, cos_table, sin_table, quarter):
    return values * cos_table + turned_lanes(values, quarter) * sin_table


def norm_wide(values, gain):
    mean = jnp.mean(values * values, axis=-1, keepdims=True)
    return values * lax.rsqrt(mean + EPS) * gain


def norm_halves(values, gain):
    lanes = lane_ids(values.shape)
    half = values.shape[1] // 2
    squares = values * values
    low = jnp.sum(jnp.where(lanes < half, squares, 0.0), axis=-1, keepdims=True) / half
    high = jnp.sum(jnp.where(lanes < half, 0.0, squares), axis=-1, keepdims=True) / half
    scale = jnp.where(lanes < half, lax.rsqrt(low + EPS), lax.rsqrt(high + EPS))
    return values * scale * gain


def layer_kernel(
    chips,
    peers,
    qw_ref,
    kw_ref,
    vw_ref,
    qn_ref,
    kvn_ref,
    gains_ref,
    tables_ref,
    res_ref,
    norm_gain_ref,
    route_ref,
    ow_hbm,
    on_hbm,
    gate_hbm,
    up_hbm,
    down_hbm,
    out_ref,
    kv_buf,
    qws,
    qns,
    m_buf,
    l_buf,
    acc_buf,
    heads,
    ow_buf,
    on_buf,
    part,
    first_in,
    last_in,
    info,
    gate_buf,
    up_buf,
    down_buf,
    att_buf,
    rows_buf,
    x_buf,
    y_buf,
    y_first,
    y_last,
    e_buf,
    e_mate,
    ret_out,
    ret_in,
    c_out,
    c_in,
    c_mate,
    own_rows,
    g_out,
    g_in,
    w_sem,
    zsend,
    zrecv,
    psend,
    precv,
    isend,
    irecv,
    imsend,
    imrecv,
    xsend,
    xrecv,
    z2send,
    z2recv,
    p2send,
    p2recv,
    asend,
    arecv,
    ysend,
    yrecv,
    esend,
    erecv,
    rsend,
    rrecv,
    csend,
    crecv,
    cmsend,
    cmrecv,
    gsend,
    grecv,
):
    tok = qw_ref.shape[0]
    half = tok // 2
    wide = kw_ref.shape[1]
    sp = lax.axis_index("sp")
    tp = lax.axis_index("tp")
    z, core = sp // 2, sp % 2
    far = chips // 2
    right = {"sp": ((z + 1) % chips) * 2 + core}
    left = {"sp": ((z + chips - 1) % chips) * 2 + core}
    mate = {"sp": z * 2 + (1 - core)}
    xright = {"tp": (tp + 1) % peers}
    xleft = {"tp": (tp + peers - 1) % peers}

    w_copies = [
        pltpu.make_async_copy(ow_hbm, ow_buf, w_sem.at[0]),
        pltpu.make_async_copy(on_hbm, on_buf, w_sem.at[1]),
        pltpu.make_async_copy(gate_hbm.at[0], gate_buf, w_sem.at[2]),
        pltpu.make_async_copy(up_hbm.at[0], up_buf, w_sem.at[3]),
        pltpu.make_async_copy(down_hbm.at[0], down_buf, w_sem.at[4]),
    ]
    for copy in w_copies:
        copy.start()

    barrier = pltpu.get_barrier_semaphore()
    for other in (right, left, mate, xright, xleft):
        pl.semaphore_signal(barrier, inc=1, device_id=other, device_id_type=MESH)

    def rows_of(chip, owner, sub):
        at = pl.multiple_of((chip * 2 + owner) * tok + sub * half, half)
        return kv_buf.at[pl.ds(at, half)]

    cos_w, sin_w = tables_ref[0], tables_ref[1]
    cos_n, sin_n = tables_ref[2], tables_ref[3]
    own = pl.ds(pl.multiple_of(sp * tok, tok), tok)
    k_wide = rotate(norm_wide(kw_ref[...].astype(F32), gains_ref[1:2]), cos_w, sin_w, wide // 4)
    kvn = kvn_ref[...].astype(F32)
    k_narrow = rotate(norm_halves(kvn, gains_ref[3:4]), cos_n, sin_n, wide // 8)
    kv_buf[own, 0:wide] = k_wide.astype(BF16)
    kv_buf[own, wide : 2 * wide] = vw_ref[...]
    kv_buf[own, 2 * wide : 3 * wide] = jnp.where(
        lane_ids(kvn.shape) < wide // 2, k_narrow, kvn
    ).astype(BF16)

    slots = 2 * 2 * res_ref.shape[0] // (2 * chips)
    route = route_ref[...]
    lanes = route.shape[1]
    experts = lax.broadcasted_iota(jnp.int32, (2 * chips, lanes), 0).astype(F32)
    hits = [(route[k : k + 1] == experts).astype(F32) for k in (0, 1)]
    earlier = (
        lax.broadcasted_iota(jnp.int32, (lanes, lanes), 0)
        < lax.broadcasted_iota(jnp.int32, (lanes, lanes), 1)
    ).astype(BF16)
    places = jnp.dot((hits[0] + hits[1]).astype(BF16), earlier, preferred_element_type=F32)
    targets = [
        jnp.sum(hit * (places + experts * slots), axis=0, keepdims=True) for hit in hits
    ]
    row = lax.broadcasted_iota(jnp.int32, route.shape, 0)
    info[sp] = jnp.where(row == 0, targets[0], jnp.where(row == 1, targets[1], route))

    pl.semaphore_wait(barrier, 5)

    def hop(src, dst, send, recv, device):
        return pltpu.make_async_remote_copy(
            src_ref=src,
            dst_ref=dst,
            send_sem=send,
            recv_sem=recv,
            device_id=device,
            device_id_type=MESH,
        )

    def same(ref, send, recv, device):
        return hop(ref, ref, send, recv, device)

    def chip_at(way, distance):
        return (z + chips - distance) % chips if way == 0 else (z + distance) % chips

    def along(way):
        return right if way == 0 else left

    def z_copy(way, step, sub):
        ref = rows_of(chip_at(way, step - 1), core, sub)
        return same(ref, zsend.at[way, step - 1, sub], zrecv.at[way, step - 1, sub], along(way))

    def z_arrival(way, step, sub):
        ref = rows_of(chip_at(way, step), core, sub)
        return same(ref, zsend.at[way, step - 1, sub], zrecv.at[way, step - 1, sub], along(way))

    def m_copy(way, step, sub, owner):
        ref = rows_of(chip_at(way, step), owner, sub)
        return same(ref, psend.at[way, step, sub], precv.at[way, step, sub], mate)

    def i_copy(way, step):
        ref = info.at[chip_at(way, step - 1) * 2 + core]
        return same(ref, isend.at[way, step - 1], irecv.at[way, step - 1], along(way))

    def i_arrival(way, step):
        ref = info.at[chip_at(way, step) * 2 + core]
        return same(ref, isend.at[way, step - 1], irecv.at[way, step - 1], along(way))

    def im_copy(way, step, owner):
        ref = info.at[chip_at(way, step) * 2 + owner]
        return same(ref, imsend.at[way, step], imrecv.at[way, step], mate)

    for way in (0, 1):
        i_copy(way, 1).start()
    im_copy(0, 0, core).start()
    for way, sub in ((0, 0), (1, 1), (0, 1), (1, 0)):
        z_copy(way, 1, sub).start()
    for sub in (0, 1):
        m_copy(0, 0, sub, core).start()

    qw = qw_ref[...].astype(F32)
    for head in (0, 1):
        q = norm_wide(qw[:, head * wide : (head + 1) * wide], gains_ref[0:1])
        qws[head * tok : (head + 1) * tok] = rotate(q, cos_w, sin_w, wide // 4).astype(BF16)
    qn = rotate(norm_halves(qn_ref[...].astype(F32), gains_ref[2:3]), cos_n, sin_n, wide // 8)
    low = lane_ids(qn.shape) < wide // 2
    qns[0:tok] = jnp.where(low, qn, 0.0).astype(BF16)
    qns[tok : 2 * tok] = jnp.where(low, pltpu.roll(qn, wide // 2, 1), 0.0).astype(BF16)
    m_buf[...] = jnp.full(m_buf.shape, NEG_BIG, F32)
    l_buf[...] = jnp.zeros(l_buf.shape, F32)
    acc_buf[...] = jnp.zeros(acc_buf.shape, F32)

    def attend_chip(chip):
        keys = pl.ds(pl.multiple_of(chip * 2 * tok, 2 * tok), 2 * tok)
        k_w, v_w = kv_buf[keys, 0:wide], kv_buf[keys, wide : 2 * wide]
        kv_n = kv_buf[keys, 2 * wide : 3 * wide]
        work = []
        for kind in (0, 1):
            for head in (0, 1):
                work.append((kind, head))

        def scores(kind, head):
            q = (qws if kind == 0 else qns)[head * tok : (head + 1) * tok]
            return lax.dot_general(
                q,
                k_w if kind == 0 else kv_n,
                (((1,), (1,)), ((), ())),
                preferred_element_type=F32,
            )

        upcoming = scores(*work[0])
        for at, (kind, head) in enumerate(work):
            s = upcoming
            if at + 1 < len(work):
                upcoming = scores(*work[at + 1])
            factor = LOG2E * (wide if kind == 0 else wide // 2) ** (-0.5)
            m_old = m_buf[at]
            m_new = jnp.maximum(m_old, jnp.max(s, axis=-1, keepdims=True))
            alpha = jnp.exp2((m_old - m_new) * factor)
            parts = [
                jnp.exp2((s[:, i * wide : (i + 1) * wide] - m_new) * factor)
                for i in range(s.shape[1] // wide)
            ]
            total = parts[0]
            for p in parts[1:]:
                total = total + p
            weights = jnp.concatenate([p.astype(BF16) for p in parts], axis=1)
            mixed = jnp.dot(
                weights, v_w if kind == 0 else kv_n, preferred_element_type=F32
            )
            m_buf[at] = m_new
            l_buf[at] = l_buf[at] * alpha + total
            acc_buf[at] = acc_buf[at] * alpha + mixed

    def ring_step(step, nothing):
        def pass_on(way):
            i_arrival(way, step).wait_recv()
            if way == 0:
                pl.when(step < far)(lambda: i_copy(way, step + 1).start())
            else:
                pl.when(step < far - 1)(lambda: i_copy(way, step + 1).start())
            im_copy(way, step, core).start()

        @pl.when(step <= far)
        def _():
            pass_on(0)
            pl.when(step < far)(functools.partial(pass_on, 1))
            for turn in (0, 1):
                for way in (0, 1):
                    sub = turn if way == 0 else 1 - turn

                    def arrived(way=way, sub=sub, turn=turn):
                        z_arrival(way, step, sub).wait_recv()
                        if turn == 0:

                            @pl.when(step < far)
                            def _():
                                z_copy(way, step + 1, sub).start()
                        else:

                            @pl.when(step < far - 1)
                            def _():
                                z_copy(way, step + 1, sub).start()

                        m_copy(way, step, sub, core).start()

                    if turn == 0:
                        arrived()
                    else:
                        pl.when(step < far)(arrived)

        before = step - 1

        @pl.when(before == 0)
        def _():
            im_copy(0, 0, 1 - core).wait_recv()
            for sub in (0, 1):
                m_copy(0, 0, sub, 1 - core).wait_recv()

        @pl.when(before > 0)
        def _():
            im_copy(0, before, 1 - core).wait_recv()
            m_copy(0, before, 0, 1 - core).wait_recv()
            m_copy(1, before, 1, 1 - core).wait_recv()

        @pl.when(jnp.logical_and(before > 0, before < far))
        def _():
            im_copy(1, before, 1 - core).wait_recv()
            m_copy(0, before, 1, 1 - core).wait_recv()
            m_copy(1, before, 0, 1 - core).wait_recv()

        def one(side, nothing):
            attend_chip((z + chips + before * (2 * side - 1)) % chips)
            return nothing

        single = jnp.logical_or(before == 0, before == far)
        return lax.fori_loop(0, jnp.where(single, 1, 2), one, nothing)

    lax.fori_loop(1, far + 2, ring_step, 0)

    outs = []
    for at in range(4):
        outs.append(acc_buf[at] / jnp.sum(l_buf[at], axis=-1, keepdims=True))
    heads[:, 0:wide] = outs[0].astype(BF16)
    heads[:, wide : 2 * wide] = outs[1].astype(BF16)
    heads[:, 2 * wide : 3 * wide] = jnp.where(
        low, pltpu.roll(outs[2], wide // 2, 1), outs[3]
    ).astype(BF16)
    for copy in w_copies[:2]:
        copy.wait()

    rows = res_ref.shape[0]
    cols = res_ref.shape[1] // 2

    def x_copy(way, number):
        dest = (tp + 1) % peers if way == 0 else (tp + peers - 1) % peers
        with_far = way * cols
        alone = (1 - way) * cols
        if number == 0:
            src = part.at[(tp + 2) % peers, :, pl.ds(with_far, cols)]
            dst = first_in.at[way]
        else:
            at = pl.ds(alone if number == 1 else with_far, cols)
            src = part.at[dest, :, at]
            dst = last_in.at[way, :, at]
        return pltpu.make_async_remote_copy(
            src_ref=src,
            dst_ref=dst,
            send_sem=xsend.at[way, number],
            recv_sem=xrecv.at[way, number],
            device_id=xright if way == 0 else xleft,
            device_id_type=MESH,
        )

    def project(peer):
        h = heads[pl.ds(pl.multiple_of(peer * rows, rows), rows)]
        product = jnp.dot(h[:, 0 : 2 * wide], ow_buf[...], preferred_element_type=F32)
        product = product + jnp.dot(
            h[:, 2 * wide : 3 * wide], on_buf[...], preferred_element_type=F32
        )
        part[peer] = product.astype(BF16)

    project((tp + 2) % peers)
    x_copy(0, 0).start()
    x_copy(1, 0).start()
    project((tp + 1) % peers)
    x_copy(0, 1).start()
    project((tp + peers - 1) % peers)
    x_copy(1, 1).start()
    project(tp)
    for way in (0, 1):
        dest = (tp + 1) % peers if way == 0 else (tp + peers - 1) % peers
        x_copy(way, 0).wait_recv()
        at = slice(way * cols, (way + 1) * cols)
        part[dest, :, at] = (
            part[dest, :, at].astype(F32) + first_in[way].astype(F32)
        ).astype(BF16)
        x_copy(way, 2).start()
    for way in (0, 1):
        x_copy(way, 1).wait_recv()
        x_copy(way, 2).wait_recv()
    total = res_ref[...].astype(F32) + part[tp].astype(F32)
    total = total + last_in[0].astype(F32) + last_in[1].astype(F32)
    attended = total.astype(BF16)
    att_buf[...] = attended
    state = attended.astype(F32)
    mean = jnp.mean(state * state, axis=-1, keepdims=True)
    normed = (state * lax.rsqrt(mean + EPS) * norm_gain_ref[...]).astype(BF16)
    rows_buf[pl.ds(pl.multiple_of(sp * rows, rows), rows)] = normed

    def block_of(chip, owner, sub):
        at = pl.multiple_of((chip * 2 + owner) * rows + sub * (rows // 2), rows // 2)
        return rows_buf.at[pl.ds(at, rows // 2)]

    def z2_copy(way, step, sub):
        ref = block_of(chip_at(way, step - 1), core, sub)
        return same(ref, z2send.at[way, step - 1, sub], z2recv.at[way, step - 1, sub], along(way))

    def z2_arrival(way, step, sub):
        ref = block_of(chip_at(way, step), core, sub)
        return same(ref, z2send.at[way, step - 1, sub], z2recv.at[way, step - 1, sub], along(way))

    def m2_copy(way, step, sub, owner):
        ref = block_of(chip_at(way, step), owner, sub)
        return same(ref, p2send.at[way, step, sub], p2recv.at[way, step, sub], mate)

    for way, sub in ((0, 0), (1, 1), (0, 1), (1, 0)):
        z2_copy(way, 1, sub).start()
    for sub in (0, 1):
        m2_copy(0, 0, sub, core).start()
    for copy in w_copies[2:]:
        copy.wait()

    def beside(way):
        return xright if way == 0 else xleft

    def peer_at(way):
        return (tp + 1) % peers if way == 0 else (tp + peers - 1) % peers

    opposite = (tp + 2) % peers

    def a_near(way, pair, owner):
        return same(x_buf.at[pair, owner], asend.at[way, pair, 0], arecv.at[way, pair, 0], beside(way))

    def a_far(way, pair, owner):
        ref = x_buf.at[pair, owner, :, pl.ds(way * cols, cols)]
        return same(ref, asend.at[way, pair, 1], arecv.at[way, pair, 1], beside(way))

    def y_copy(way, pair, number):
        with_far = way * cols
        alone = (1 - way) * cols
        if number == 0:
            src = y_buf.at[pair, opposite, :, pl.ds(with_far, cols)]
            dst = y_first.at[pair, way]
        else:
            at = pl.ds(alone if number == 1 else with_far, cols)
            src = y_buf.at[pair, peer_at(way), :, at]
            dst = y_last.at[pair, way, :, at]
        return hop(src, dst, ysend.at[way, pair, number], yrecv.at[way, pair, number], beside(way))

    def e_copy(pair):
        return hop(
            e_buf.at[pair, 1 - core], e_mate.at[pair], esend.at[pair], erecv.at[pair], mate
        )

    tile = 2 * slots
    near = far - FAR_STEPS

    def c_copy(way, number, piece):
        last = FAR_STEPS - 1
        if piece == 0:
            at = (pl.ds(number * tile, (last - number) * tile),)
        else:
            at = (pl.ds(last * tile, tile), pl.ds(way * cols, cols))
        src = c_out.at[way] if number == 0 else c_in.at[way, number - 1]
        return hop(
            src.at[at],
            c_in.at[(way, number) + at],
            csend.at[way, number, piece],
            crecv.at[way, number, piece],
            along(way),
        )

    def cm_copy(way, number):
        at = (pl.ds(number * tile, tile),)
        to = ()
        if number == FAR_STEPS - 1:
            at = at + (pl.ds(way * cols, cols),)
            to = (slice(None), pl.ds(way * cols, cols))
        return hop(
            c_in.at[(way, number) + at],
            c_mate.at[(way, number) + to],
            cmsend.at[way, number],
            cmrecv.at[way, number],
            mate,
        )

    def pieces_of(number):
        return (0, 1) if number < FAR_STEPS - 1 else (1,)

    def picks(table, want):
        hit = jnp.logical_or(table[0:1, 0:rows] == want, table[1:2, 0:rows] == want)
        return jnp.where(hit, 1.0, 0.0).astype(BF16)

    def rows_at(device):
        return rows_buf[pl.ds(pl.multiple_of(device * rows, rows), rows)]

    def near_arrivals(step):
        for turn in (0, 1):
            for way in (0, 1):
                sub = turn if way == 0 else 1 - turn
                z2_arrival(way, step, sub).wait_recv()
                pl.when(step < near)(lambda: z2_copy(way, step + 1, sub).start())
                m2_copy(way, step, sub, core).start()

        @pl.when(step == near)
        def _():
            for way in (0, 1):
                device = chip_at(way, near) * 2 + core
                slot = lax.broadcasted_iota(jnp.int32, (FAR_STEPS * tile, rows), 0)
                onward = slot // tile + 1
                chip = (z + onward) % chips if way == 0 else (z + chips - onward) % chips
                want = ((chip * 2 + slot % tile // slots) * slots + slot % slots).astype(F32)
                c_out[way] = jnp.dot(
                    picks(info[device], want), rows_at(device), preferred_element_type=F32
                ).astype(BF16)
                for piece in (0, 1):
                    c_copy(way, 0, piece).start()

    def far_arrivals(number):
        for way in (0, 1):
            for piece in pieces_of(number):
                c_copy(way, number, piece).wait_recv()
            if number + 1 < FAR_STEPS:
                for piece in pieces_of(number + 1):
                    c_copy(way, number + 1, piece).start()
            cm_copy(way, number).start()

    def arrive(step):
        pl.when(step <= near)(functools.partial(near_arrivals, step))
        for number in range(FAR_STEPS):
            pl.when(step == near + 1 + number)(functools.partial(far_arrivals, number))

    def select_near(step):
        for way in (0, 1):
            for sub in (0, 1):
                m2_copy(way, step, sub, 1 - core).wait_recv()
        total = None
        for number, (way, owner) in enumerate(((0, 0), (1, 0), (0, 1), (1, 1))):
            device = chip_at(way, step) * 2 + owner
            slot = lax.broadcasted_iota(jnp.int32, (2 * tile, rows), 0)
            want = jnp.where(slot // slots == number, sp * slots + slot % slots, -2).astype(F32)
            picked = jnp.dot(
                picks(info[device], want), rows_at(device), preferred_element_type=F32
            )
            total = picked if total is None else total + picked
        x_buf[step, tp] = total.astype(BF16)
        for way in (0, 1):
            a_near(way, step, tp).start()

    def my_half(ref, at):
        both = ref[at].astype(F32)
        return jnp.where(core == 0, both[0:slots], both[slots:tile])

    def select_far(step):
        pair = step % far
        for number in range(FAR_STEPS):

            @pl.when(step == near + 1 + number)
            def _(number=number):
                for way in (0, 1):
                    cm_copy(way, number).wait_recv()
                for owner in (0, 1):
                    if owner == 0:
                        at_row = core * tile
                        source, at = c_in, slice(number * tile, (number + 1) * tile)
                    else:
                        at_row = (1 - core) * tile
                        source, at = c_mate, slice(None)
                    if number < FAR_STEPS - 1:
                        low = my_half(source, (0, number, at))
                        high = my_half(source, (1, number, at))
                    else:
                        low = own_rows[owner]
                        high = jnp.concatenate(
                            [
                                my_half(source, (0, number, at, slice(0, cols))),
                                my_half(source, (1, number, at, slice(cols, 2 * cols))),
                            ],
                            axis=1,
                        )
                    x_buf[pair, tp, pl.ds(pl.multiple_of(at_row, tile), tile)] = jnp.concatenate(
                        [low, high], axis=0
                    ).astype(BF16)

        for way in (0, 1):
            a_near(way, pair, tp).start()

    slot8 = lax.broadcasted_iota(jnp.int32, (slots, rows), 0)
    own_want = (sp * slots + slot8).astype(F32)
    own_rows[0] = jnp.dot(picks(info[sp], own_want), normed, preferred_element_type=F32)
    for sub in (0, 1):
        m2_copy(0, 0, sub, 1 - core).wait_recv()
    other = z * 2 + (1 - core)
    own_rows[1] = jnp.dot(picks(info[other], own_want), rows_at(other), preferred_element_type=F32)

    def forward(step):
        pair = step % far
        for way in (0, 1):
            source = peer_at(1 - way)
            a_near(way, pair, source).wait_recv()
            a_far(way, pair, source).start()

    def run_expert(step):
        pair = step % far
        for way in (0, 1):
            a_far(way, pair, opposite).wait_recv()
        x = x_buf[pair].reshape(peers * 4 * slots, 2 * cols)
        gate = jnp.dot(x, gate_buf[...], preferred_element_type=F32)
        up = jnp.dot(x, up_buf[...], preferred_element_type=F32)
        hidden = (gate / (1.0 + jnp.exp(-gate)) * up).astype(BF16)
        y = jnp.dot(hidden, down_buf[...], preferred_element_type=F32)
        y_buf[pair] = y.astype(BF16).reshape(peers, 4 * slots, 2 * cols)
        pl.when(step >= far - 1)(lambda: begin_sum(step))

    def begin_sum(step):
        pair = step % far
        for number in (0, 1):
            for way in (0, 1):
                y_copy(way, pair, number).start()

    def add_far(step):
        pair = step % far
        for way in (0, 1):
            y_copy(way, pair, 0).wait_recv()
            at = slice(way * cols, (way + 1) * cols)
            y_buf[pair, peer_at(way), :, at] = (
                y_buf[pair, peer_at(way), :, at].astype(F32) + y_first[pair, way].astype(F32)
            ).astype(BF16)
            y_copy(way, pair, 2).start()

    def finish(step):
        pair = step % far
        for way in (0, 1):
            y_copy(way, pair, 1).wait_recv()
            y_copy(way, pair, 2).wait_recv()
        total = y_buf[pair, tp].astype(F32)
        total = total + y_last[pair, 0].astype(F32) + y_last[pair, 1].astype(F32)
        e_buf[pair] = total.astype(BF16).reshape(2, 2 * slots, 2 * cols)
        e_copy(pair).start()

    stages = (
        (0, arrive, 1, far),
        (1, forward, 1, far),
        (0, select_far, near + 1, far),
        (2, run_expert, 1, far),
        (0, select_near, 1, near),
    )

    def tick(at, nothing):
        for lag, stage, first, last in stages:
            step = at - lag
            pl.when(jnp.logical_and(step >= first, step <= last))(functools.partial(stage, step))
        return nothing

    lax.fori_loop(1, far + 3, tick, 0)

    def weighted(chip, want, stack):
        table = info[chip * 2 + core]
        weight = jnp.where(table[0:1, 0:rows] == want, table[2:3, 0:rows], 0.0)
        weight = weight + jnp.where(table[1:2, 0:rows] == want, table[3:4, 0:rows], 0.0)
        coarse = weight.astype(BF16)
        fine = (weight - coarse.astype(F32)).astype(BF16)
        return lax.dot_general(
            jnp.concatenate([coarse, fine], axis=0),
            jnp.concatenate([stack, stack], axis=0),
            (((0,), (0,)), ((), ())),
            preferred_element_type=F32,
        )

    def contribution(chip, pair, which, sub):
        slot = lax.broadcasted_iota(jnp.int32, (2 * tile, rows), 0)
        expert = jnp.where(slot < tile, sp, z * 2 + (1 - core))
        ours = (slot % tile) // slots == which
        want = jnp.where(ours, expert * slots + slot % slots, -2).astype(F32)
        at = slice(sub * cols, (sub + 1) * cols)
        return weighted(
            chip, want, jnp.concatenate([e_buf[pair, core, :, at], e_mate[pair, :, at]], axis=0)
        )

    def passed_on(way, sub):
        chip = chip_at(1 - way, near)
        slot = lax.broadcasted_iota(jnp.int32, (FAR_STEPS * tile, rows), 0)
        giver = chip_at(way, FAR_STEPS - slot // tile)
        want = ((giver * 2 + slot % tile // slots) * slots + slot % slots).astype(F32)
        at = slice(sub * cols, (sub + 1) * cols)
        return weighted(chip, want, g_in[way, FAR_STEPS - 1, :, at])

    def g_copy(way, number, piece):
        at = (pl.ds(piece * tile, tile),)
        to = ()
        if piece == 0:
            at = at + (pl.ds(way * cols, cols),)
            to = (slice(None), pl.ds(way * cols, cols))
        if piece == number:
            src = g_out.at[(way, number) + to]
        else:
            src = g_in.at[(way, number - 1) + at]
        return hop(
            src,
            g_in.at[(way, number) + at],
            gsend.at[way, number, piece],
            grecv.at[way, number, piece],
            along(way),
        )

    def r_copy(way, step, sub):
        at = pl.ds(sub * cols, cols)
        return hop(
            ret_out.at[way, step, :, at],
            ret_in.at[way, step, :, at],
            rsend.at[way, step, sub],
            rrecv.at[way, step, sub],
            along(way),
        )

    for way in (0, 1):
        rest = slice((1 - way) * cols, (2 - way) * cols)
        g_in[way, FAR_STEPS - 1, 0:tile, rest] = jnp.zeros((tile, cols), BF16)

    def far_back(number):
        pair = (far - number) % far
        for way in (0, 1):
            for piece in range(number):
                g_copy(way, number - 1, piece).wait_recv()
                g_copy(way, number, piece).start()
        e_copy(pair).wait_recv()
        for way in (0, 1):
            which = 1 if number == 0 else 1 - way
            at = slice(which * slots, (which + 1) * slots)
            mine = e_buf[pair, core].astype(F32)[at]
            other = e_mate[pair].astype(F32)[at]
            g_out[way, number] = jnp.concatenate(
                [jnp.where(core == 0, mine, other), jnp.where(core == 0, other, mine)], axis=0
            ).astype(BF16)
            g_copy(way, number, number).start()

    def near_back(distance):
        step = far - distance
        e_copy(distance).wait_recv()

        @pl.when(distance == near)
        def _():
            for way in (0, 1):
                for piece in range(FAR_STEPS):
                    g_copy(way, FAR_STEPS - 1, piece).wait_recv()
                for sub in (0, 1):
                    at = slice(sub * cols, (sub + 1) * cols)
                    ret_in[way, FAR_STEPS - 1, :, at] = passed_on(way, sub).astype(BF16)

        for turn in (0, 1):
            for way in (0, 1):
                sub = turn if way == 0 else 1 - turn
                added = contribution(chip_at(1 - way, distance), distance, 1 - way, sub)
                pl.when(distance < near)(lambda: r_copy(way, step - 1, sub).wait_recv())
                at = slice(sub * cols, (sub + 1) * cols)
                ret_out[way, step, :, at] = (
                    added + ret_in[way, step - 1, :, at].astype(F32)
                ).astype(BF16)
                r_copy(way, step, sub).start()

    def back(distance):
        for number in range(FAR_STEPS):
            pl.when(distance == far - number)(functools.partial(far_back, number))
        pl.when(distance <= near)(functools.partial(near_back, distance))

    back_stages = ((2, back), (1, finish), (0, add_far), (-2, begin_sum))

    def back_tick(at, nothing):
        for lag, stage in back_stages:
            step = far - at + lag
            last = far - 2 if stage is begin_sum else far
            pl.when(jnp.logical_and(step >= 1, step <= last))(functools.partial(stage, step))
        return nothing

    lax.fori_loop(0, far + 2, back_tick, 0)
    for sub in (0, 1):
        at = slice(sub * cols, (sub + 1) * cols)
        total = att_buf[:, at].astype(F32) + contribution(z, 0, 0, sub)
        for way in (0, 1):
            r_copy(way, far - 1, sub).wait_recv()
            total = total + ret_in[way, far - 1, :, at].astype(F32)
        out_ref[:, at] = total.astype(BF16)

    for way in (0, 1):
        for number in (0, 1, 2):
            x_copy(way, number).wait_send()
    for sub in (0, 1):
        m_copy(0, 0, sub, core).wait_send()
        m2_copy(0, 0, sub, core).wait_send()
    im_copy(0, 0, core).wait_send()

    def drain(step, nothing):
        for way in (0, 1):
            i_copy(way, step).wait_send()
            im_copy(way, step, core).wait_send()
            for sub in (0, 1):
                z_copy(way, step, sub).wait_send()
                m_copy(way, step, sub, core).wait_send()
        return nothing

    def drain_near(step, nothing):
        for way in (0, 1):
            for sub in (0, 1):
                z2_copy(way, step, sub).wait_send()
                m2_copy(way, step, sub, core).wait_send()
                r_copy(way, far - step, sub).wait_send()
        return nothing

    lax.fori_loop(1, far, drain, 0)
    lax.fori_loop(1, near + 1, drain_near, 0)
    i_copy(0, far).wait_send()
    im_copy(0, far, core).wait_send()
    for way in (0, 1):
        z_copy(way, far, way).wait_send()
        m_copy(way, far, way, core).wait_send()
        for number in range(FAR_STEPS):
            for piece in pieces_of(number):
                c_copy(way, number, piece).wait_send()
            cm_copy(way, number).wait_send()
            for piece in range(number + 1):
                g_copy(way, number, piece).wait_send()

    def drain_pairs(pair, nothing):
        e_copy(pair).wait_send()
        for way in (0, 1):
            a_near(way, pair, tp).wait_send()
            a_far(way, pair, peer_at(1 - way)).wait_send()
            for number in (0, 1, 2):
                y_copy(way, pair, number).wait_send()
        return nothing

    lax.fori_loop(0, far, drain_pairs, 0)


def layer(
    residual,
    queries_wide,
    keys_wide,
    values_wide,
    queries_narrow,
    keys_narrow,
    values_narrow,
    gains,
    tables,
    norm_gain,
    route,
    output_wide,
    output_narrow,
    gate_weight,
    up_weight,
    down_weight,
):
    chips = lax.axis_size("sp") // 2
    peers = lax.axis_size("tp")
    tok, wide = keys_wide.shape
    rows, width = residual.shape
    far = chips // 2
    picked = 4 * (2 * 2 * rows // (2 * chips))
    vmem = pl.BlockSpec(memory_space=pltpu.VMEM)
    hbm = pl.BlockSpec(memory_space=pl.ANY)
    dma = pltpu.SemaphoreType.DMA
    return pl.pallas_call(
        functools.partial(layer_kernel, chips, peers),
        out_shape=jax.ShapeDtypeStruct((rows, width), BF16),
        in_specs=[vmem] * 10 + [hbm] * 5,
        out_specs=vmem,
        scratch_shapes=[
            pltpu.VMEM((2 * chips * tok, 3 * wide), BF16),
            pltpu.VMEM((2 * tok, wide), BF16),
            pltpu.VMEM((2 * tok, wide), BF16),
            pltpu.VMEM((4, tok, wide), F32),
            pltpu.VMEM((4, tok, wide), F32),
            pltpu.VMEM((4, tok, wide), F32),
            pltpu.VMEM((tok, 3 * wide), BF16),
            pltpu.VMEM(output_wide.shape, BF16),
            pltpu.VMEM(output_narrow.shape, BF16),
            pltpu.VMEM((peers, rows, width), BF16),
            pltpu.VMEM((2, rows, width // 2), BF16),
            pltpu.VMEM((2, rows, width), BF16),
            pltpu.VMEM((2 * chips,) + route.shape, F32),
            pltpu.VMEM(gate_weight.shape[1:], BF16),
            pltpu.VMEM(up_weight.shape[1:], BF16),
            pltpu.VMEM(down_weight.shape[1:], BF16),
            pltpu.VMEM((rows, width), BF16),
            pltpu.VMEM((2 * chips * rows, width), BF16),
            pltpu.VMEM((far, peers, picked, width), BF16),
            pltpu.VMEM((far, peers, picked, width), BF16),
            pltpu.VMEM((far, 2, picked, width // 2), BF16),
            pltpu.VMEM((far, 2, picked, width), BF16),
            pltpu.VMEM((far, 2, picked // 2, width), BF16),
            pltpu.VMEM((far, picked // 2, width), BF16),
            pltpu.VMEM((2, far, rows, width), BF16),
            pltpu.VMEM((2, far, rows, width), BF16),
            pltpu.VMEM((2, FAR_STEPS * picked // 2, width), BF16),
            pltpu.VMEM((2, FAR_STEPS, FAR_STEPS * picked // 2, width), BF16),
            pltpu.VMEM((2, FAR_STEPS, picked // 2, width), BF16),
            pltpu.VMEM((2, picked // 4, width), F32),
            pltpu.VMEM((2, FAR_STEPS, picked // 2, width), BF16),
            pltpu.VMEM((2, FAR_STEPS, FAR_STEPS * picked // 2, width), BF16),
            dma((5,)),
            dma((2, far, 2)),
            dma((2, far, 2)),
            dma((2, far + 1, 2)),
            dma((2, far + 1, 2)),
            dma((2, far)),
            dma((2, far)),
            dma((2, far + 1)),
            dma((2, far + 1)),
            dma((2, 3)),
            dma((2, 3)),
            dma((2, far, 2)),
            dma((2, far, 2)),
            dma((2, far + 1, 2)),
            dma((2, far + 1, 2)),
            dma((2, far, 2)),
            dma((2, far, 2)),
            dma((2, far, 3)),
            dma((2, far, 3)),
            dma((far,)),
            dma((far,)),
            dma((2, far, 2)),
            dma((2, far, 2)),
            dma((2, FAR_STEPS, 2)),
            dma((2, FAR_STEPS, 2)),
            dma((2, FAR_STEPS)),
            dma((2, FAR_STEPS)),
            dma((2, FAR_STEPS, FAR_STEPS)),
            dma((2, FAR_STEPS, FAR_STEPS)),
        ],
        compiler_params=pltpu.CompilerParams(
            collective_id=0, has_side_effects=True, vmem_limit_bytes=64 * 1024 * 1024 - 65536
        ),
        name="layer",
    )(
        queries_wide,
        keys_wide,
        values_wide,
        queries_narrow,
        jnp.concatenate([keys_narrow, values_narrow], axis=1),
        gains,
        tables,
        residual,
        norm_gain.reshape(1, width),
        route,
        output_wide,
        output_narrow,
        gate_weight,
        up_weight,
        down_weight,
    )


def body(
    residual,
    queries_wide,
    keys_wide,
    values_wide,
    queries_narrow,
    keys_narrow,
    values_narrow,
    query_gain_wide,
    key_gain_wide,
    query_gain_narrow,
    key_gain_narrow,
    output_wide,
    output_narrow,
    norm_gain,
    gate_weight,
    up_weight,
    down_weight,
    route_ids,
    route_weights,
):
    tok_count = queries_wide.shape[0]
    places = lax.axis_index("sp") * tok_count + jnp.arange(tok_count, dtype=jnp.int32)
    wide_width = query_gain_wide.shape[0]
    narrow_width = query_gain_narrow.shape[0]
    wide_angles = angles_of(places, wide_width)
    narrow_angles = angles_of(places, narrow_width)
    narrow_angles = jnp.concatenate([narrow_angles, narrow_angles], axis=1)
    lanes = jnp.arange(wide_width, dtype=jnp.int32)
    wide_sign = jnp.where(lanes % (wide_width // 2) < wide_width // 4, -1.0, 1.0)
    narrow_sign = jnp.where(lanes % (narrow_width // 2) < narrow_width // 4, -1.0, 1.0)
    tables = jnp.stack(
        [
            jnp.cos(wide_angles),
            jnp.sin(wide_angles) * wide_sign,
            jnp.cos(narrow_angles),
            jnp.sin(narrow_angles) * narrow_sign,
        ]
    )
    gains = jnp.stack(
        [
            query_gain_wide,
            key_gain_wide,
            jnp.concatenate([query_gain_narrow, query_gain_narrow]),
            jnp.concatenate([key_gain_narrow, key_gain_narrow]),
        ]
    )
    own_rows = residual.shape[0]
    route = jnp.concatenate([route_ids.astype(F32), route_weights], axis=1).T
    route = jnp.pad(route, ((0, 4), (0, 128 - own_rows)), constant_values=-1.0)
    return layer(
        residual,
        queries_wide,
        keys_wide,
        values_wide,
        queries_narrow,
        keys_narrow,
        values_narrow,
        gains,
        tables,
        norm_gain,
        route,
        output_wide,
        output_narrow,
        gate_weight,
        up_weight,
        down_weight,
    )


def solution(mesh):
    return jax.shard_map(
        body,
        mesh=mesh,
        in_specs=(
            P(("grp", "sp", "tp"), None),
            P(("grp", "sp"), "tp"),
            P(("grp", "sp"), "tp"),
            P(("grp", "sp"), "tp"),
            P(("grp", "sp"), "tp"),
            P(("grp", "sp"), "tp"),
            P(("grp", "sp"), "tp"),
            P(),
            P(),
            P(),
            P(),
            P("tp", None),
            P("tp", None),
            P(),
            P("sp", None, "tp"),
            P("sp", None, "tp"),
            P("sp", "tp", None),
            P(("grp", "sp", "tp"), None),
            P(("grp", "sp", "tp"), None),
        ),
        out_specs=P(("grp", "sp", "tp"), None),
        check_vma=False,
    )
```

```python
import functools
import math

import jax
import jax.numpy as jnp
from jax import lax
from jax.experimental import pallas as pl
from jax.experimental.pallas import tpu as pltpu
from jax.sharding import PartitionSpec as P

GRID = 64
FAR_STEPS = 3
THETA = 10000.0
EPS = 1e-06
NEG_BIG = -1e30
LOG2E = math.log2(math.e)
MESH = pl.DeviceIdType.MESH
F32 = jnp.float32
BF16 = jnp.bfloat16


def angles_of(places, head_width):
    quarter = head_width // 4
    inv_freq = THETA ** (-jnp.arange(quarter, dtype=jnp.float32) / quarter)
    grid_rows = (places // GRID).astype(jnp.float32)
    grid_cols = (places % GRID).astype(jnp.float32)
    row_angle = grid_rows[:, None] * inv_freq[None, :]
    col_angle = grid_cols[:, None] * inv_freq[None, :]
    return jnp.concatenate([row_angle, row_angle, col_angle, col_angle], axis=-1)


def lane_ids(shape):
    return lax.broadcasted_iota(jnp.int32, shape, 1)


def turned_lanes(values, quarter):
    lanes = lane_ids(values.shape)
    width = values.shape[1]
    return jnp.where(
        lanes % (2 * quarter) < quarter,
        pltpu.roll(values, width - quarter, 1),
        pltpu.roll(values, quarter, 1),
    )


def rotate(values, cos_table, sin_table, quarter):
    return values * cos_table + turned_lanes(values, quarter) * sin_table


def norm_wide(values, gain):
    mean = jnp.mean(values * values, axis=-1, keepdims=True)
    return values * lax.rsqrt(mean + EPS) * gain


def norm_halves(values, gain):
    lanes = lane_ids(values.shape)
    half = values.shape[1] // 2
    squares = values * values
    low = jnp.sum(jnp.where(lanes < half, squares, 0.0), axis=-1, keepdims=True) / half
    high = jnp.sum(jnp.where(lanes < half, 0.0, squares), axis=-1, keepdims=True) / half
    scale = jnp.where(lanes < half, lax.rsqrt(low + EPS), lax.rsqrt(high + EPS))
    return values * scale * gain


def layer_kernel(
    chips,
    peers,
    qw_ref,
    kw_ref,
    vw_ref,
    qn_ref,
    kvn_ref,
    gains_ref,
    tables_ref,
    res_ref,
    norm_gain_ref,
    route_ref,
    ow_hbm,
    on_hbm,
    gate_hbm,
    up_hbm,
    down_hbm,
    out_ref,
    kv_buf,
    qws,
    qns,
    m_buf,
    l_buf,
    acc_buf,
    heads,
    ow_buf,
    on_buf,
    part,
    first_in,
    last_in,
    info,
    gate_buf,
    up_buf,
    down_buf,
    att_buf,
    rows_buf,
    x_buf,
    y_buf,
    y_first,
    y_last,
    e_buf,
    e_mate,
    ret_out,
    ret_in,
    c_out,
    c_in,
    c_mate,
    own_rows,
    g_out,
    g_in,
    w_sem,
    zsend,
    zrecv,
    psend,
    precv,
    isend,
    irecv,
    imsend,
    imrecv,
    xsend,
    xrecv,
    z2send,
    z2recv,
    p2send,
    p2recv,
    asend,
    arecv,
    ysend,
    yrecv,
    esend,
    erecv,
    rsend,
    rrecv,
    csend,
    crecv,
    cmsend,
    cmrecv,
    gsend,
    grecv,
):
    tok = qw_ref.shape[0]
    half = tok // 2
    wide = kw_ref.shape[1]
    sp = lax.axis_index("sp")
    tp = lax.axis_index("tp")
    z, core = sp // 2, sp % 2
    far = chips // 2
    right = {"sp": ((z + 1) % chips) * 2 + core}
    left = {"sp": ((z + chips - 1) % chips) * 2 + core}
    mate = {"sp": z * 2 + (1 - core)}
    xright = {"tp": (tp + 1) % peers}
    xleft = {"tp": (tp + peers - 1) % peers}

    w_copies = [
        pltpu.make_async_copy(ow_hbm, ow_buf, w_sem.at[0]),
        pltpu.make_async_copy(on_hbm, on_buf, w_sem.at[1]),
        pltpu.make_async_copy(gate_hbm.at[0], gate_buf, w_sem.at[2]),
        pltpu.make_async_copy(up_hbm.at[0], up_buf, w_sem.at[3]),
        pltpu.make_async_copy(down_hbm.at[0], down_buf, w_sem.at[4]),
    ]
    for copy in w_copies:
        copy.start()

    barrier = pltpu.get_barrier_semaphore()
    for other in (right, left, mate, xright, xleft):
        pl.semaphore_signal(barrier, inc=1, device_id=other, device_id_type=MESH)

    def rows_of(chip, owner, sub):
        at = pl.multiple_of((chip * 2 + owner) * tok + sub * half, half)
        return kv_buf.at[pl.ds(at, half)]

    cos_w, sin_w = tables_ref[0], tables_ref[1]
    cos_n, sin_n = tables_ref[2], tables_ref[3]
    own = pl.ds(pl.multiple_of(sp * tok, tok), tok)
    k_wide = rotate(norm_wide(kw_ref[...].astype(F32), gains_ref[1:2]), cos_w, sin_w, wide // 4)
    kvn = kvn_ref[...].astype(F32)
    k_narrow = rotate(norm_halves(kvn, gains_ref[3:4]), cos_n, sin_n, wide // 8)
    kv_buf[own, 0:wide] = k_wide.astype(BF16)
    kv_buf[own, wide : 2 * wide] = vw_ref[...]
    kv_buf[own, 2 * wide : 3 * wide] = jnp.where(
        lane_ids(kvn.shape) < wide // 2, k_narrow, kvn
    ).astype(BF16)

    slots = 2 * 2 * res_ref.shape[0] // (2 * chips)
    route = route_ref[...]
    lanes = route.shape[1]
    experts = lax.broadcasted_iota(jnp.int32, (2 * chips, lanes), 0).astype(F32)
    hits = [(route[k : k + 1] == experts).astype(F32) for k in (0, 1)]
    earlier = (
        lax.broadcasted_iota(jnp.int32, (lanes, lanes), 0)
        < lax.broadcasted_iota(jnp.int32, (lanes, lanes), 1)
    ).astype(BF16)
    places = jnp.dot((hits[0] + hits[1]).astype(BF16), earlier, preferred_element_type=F32)
    targets = [
        jnp.sum(hit * (places + experts * slots), axis=0, keepdims=True) for hit in hits
    ]
    row = lax.broadcasted_iota(jnp.int32, route.shape, 0)
    info[sp] = jnp.where(row == 0, targets[0], jnp.where(row == 1, targets[1], route))

    pl.semaphore_wait(barrier, 5)

    def hop(src, dst, send, recv, device):
        return pltpu.make_async_remote_copy(
            src_ref=src,
            dst_ref=dst,
            send_sem=send,
            recv_sem=recv,
            device_id=device,
            device_id_type=MESH,
        )

    def same(ref, send, recv, device):
        return hop(ref, ref, send, recv, device)

    def chip_at(way, distance):
        return (z + chips - distance) % chips if way == 0 else (z + distance) % chips

    def along(way):
        return right if way == 0 else left

    def z_copy(way, step, sub):
        ref = rows_of(chip_at(way, step - 1), core, sub)
        return same(ref, zsend.at[way, step - 1, sub], zrecv.at[way, step - 1, sub], along(way))

    def z_arrival(way, step, sub):
        ref = rows_of(chip_at(way, step), core, sub)
        return same(ref, zsend.at[way, step - 1, sub], zrecv.at[way, step - 1, sub], along(way))

    def m_copy(way, step, sub, owner):
        ref = rows_of(chip_at(way, step), owner, sub)
        return same(ref, psend.at[way, step, sub], precv.at[way, step, sub], mate)

    def i_copy(way, step):
        ref = info.at[chip_at(way, step - 1) * 2 + core]
        return same(ref, isend.at[way, step - 1], irecv.at[way, step - 1], along(way))

    def i_arrival(way, step):
        ref = info.at[chip_at(way, step) * 2 + core]
        return same(ref, isend.at[way, step - 1], irecv.at[way, step - 1], along(way))

    def im_copy(way, step, owner):
        ref = info.at[chip_at(way, step) * 2 + owner]
        return same(ref, imsend.at[way, step], imrecv.at[way, step], mate)

    for way in (0, 1):
        i_copy(way, 1).start()
    im_copy(0, 0, core).start()
    for way, sub in ((0, 0), (1, 1), (0, 1), (1, 0)):
        z_copy(way, 1, sub).start()
    for sub in (0, 1):
        m_copy(0, 0, sub, core).start()

    qw = qw_ref[...].astype(F32)
    for head in (0, 1):
        q = norm_wide(qw[:, head * wide : (head + 1) * wide], gains_ref[0:1])
        qws[head * tok : (head + 1) * tok] = rotate(q, cos_w, sin_w, wide // 4).astype(BF16)
    qn = rotate(norm_halves(qn_ref[...].astype(F32), gains_ref[2:3]), cos_n, sin_n, wide // 8)
    low = lane_ids(qn.shape) < wide // 2
    qns[0:tok] = jnp.where(low, qn, 0.0).astype(BF16)
    qns[tok : 2 * tok] = jnp.where(low, pltpu.roll(qn, wide // 2, 1), 0.0).astype(BF16)
    m_buf[...] = jnp.full(m_buf.shape, NEG_BIG, F32)
    l_buf[...] = jnp.zeros(l_buf.shape, F32)
    acc_buf[...] = jnp.zeros(acc_buf.shape, F32)

    def attend_chip(chip):
        keys = pl.ds(pl.multiple_of(chip * 2 * tok, 2 * tok), 2 * tok)
        k_w, v_w = kv_buf[keys, 0:wide], kv_buf[keys, wide : 2 * wide]
        kv_n = kv_buf[keys, 2 * wide : 3 * wide]
        work = []
        for kind in (0, 1):
            for head in (0, 1):
                work.append((kind, head))

        def scores(kind, head):
            q = (qws if kind == 0 else qns)[head * tok : (head + 1) * tok]
            return lax.dot_general(
                q,
                k_w if kind == 0 else kv_n,
                (((1,), (1,)), ((), ())),
                preferred_element_type=F32,
            )

        upcoming = scores(*work[0])
        for at, (kind, head) in enumerate(work):
            s = upcoming
            if at + 1 < len(work):
                upcoming = scores(*work[at + 1])
            factor = LOG2E * (wide if kind == 0 else wide // 2) ** (-0.5)
            m_old = m_buf[at]
            m_new = jnp.maximum(m_old, jnp.max(s, axis=-1, keepdims=True))
            alpha = jnp.exp2((m_old - m_new) * factor)
            parts = [
                jnp.exp2((s[:, i * wide : (i + 1) * wide] - m_new) * factor)
                for i in range(s.shape[1] // wide)
            ]
            total = parts[0]
            for p in parts[1:]:
                total = total + p
            weights = jnp.concatenate([p.astype(BF16) for p in parts], axis=1)
            mixed = jnp.dot(
                weights, v_w if kind == 0 else kv_n, preferred_element_type=F32
            )
            m_buf[at] = m_new
            l_buf[at] = l_buf[at] * alpha + total
            acc_buf[at] = acc_buf[at] * alpha + mixed

    def ring_step(step, nothing):
        def pass_on(way):
            i_arrival(way, step).wait_recv()
            if way == 0:
                pl.when(step < far)(lambda: i_copy(way, step + 1).start())
            else:
                pl.when(step < far - 1)(lambda: i_copy(way, step + 1).start())
            im_copy(way, step, core).start()

        @pl.when(step <= far)
        def _():
            pass_on(0)
            pl.when(step < far)(functools.partial(pass_on, 1))
            for turn in (0, 1):
                for way in (0, 1):
                    sub = turn if way == 0 else 1 - turn

                    def arrived(way=way, sub=sub, turn=turn):
                        z_arrival(way, step, sub).wait_recv()
                        if turn == 0:

                            @pl.when(step < far)
                            def _():
                                z_copy(way, step + 1, sub).start()
                        else:

                            @pl.when(step < far - 1)
                            def _():
                                z_copy(way, step + 1, sub).start()

                        m_copy(way, step, sub, core).start()

                    if turn == 0:
                        arrived()
                    else:
                        pl.when(step < far)(arrived)

        before = step - 1

        @pl.when(before == 0)
        def _():
            im_copy(0, 0, 1 - core).wait_recv()
            for sub in (0, 1):
                m_copy(0, 0, sub, 1 - core).wait_recv()

        @pl.when(before > 0)
        def _():
            im_copy(0, before, 1 - core).wait_recv()
            m_copy(0, before, 0, 1 - core).wait_recv()
            m_copy(1, before, 1, 1 - core).wait_recv()

        @pl.when(jnp.logical_and(before > 0, before < far))
        def _():
            im_copy(1, before, 1 - core).wait_recv()
            m_copy(0, before, 1, 1 - core).wait_recv()
            m_copy(1, before, 0, 1 - core).wait_recv()

        def one(side, nothing):
            attend_chip((z + chips + before * (2 * side - 1)) % chips)
            return nothing

        single = jnp.logical_or(before == 0, before == far)
        return lax.fori_loop(0, jnp.where(single, 1, 2), one, nothing)

    lax.fori_loop(1, far + 2, ring_step, 0)

    outs = []
    for at in range(4):
        outs.append(acc_buf[at] / jnp.sum(l_buf[at], axis=-1, keepdims=True))
    heads[:, 0:wide] = outs[0].astype(BF16)
    heads[:, wide : 2 * wide] = outs[1].astype(BF16)
    heads[:, 2 * wide : 3 * wide] = jnp.where(
        low, pltpu.roll(outs[2], wide // 2, 1), outs[3]
    ).astype(BF16)
    for copy in w_copies[:2]:
        copy.wait()

    rows = res_ref.shape[0]
    cols = res_ref.shape[1] // 2

    def x_copy(way, number):
        dest = (tp + 1) % peers if way == 0 else (tp + peers - 1) % peers
        with_far = way * cols
        alone = (1 - way) * cols
        if number == 0:
            src = part.at[(tp + 2) % peers, :, pl.ds(with_far, cols)]
            dst = first_in.at[way]
        else:
            at = pl.ds(alone if number == 1 else with_far, cols)
            src = part.at[dest, :, at]
            dst = last_in.at[way, :, at]
        return pltpu.make_async_remote_copy(
            src_ref=src,
            dst_ref=dst,
            send_sem=xsend.at[way, number],
            recv_sem=xrecv.at[way, number],
            device_id=xright if way == 0 else xleft,
            device_id_type=MESH,
        )

    def project(peer):
        h = heads[pl.ds(pl.multiple_of(peer * rows, rows), rows)]
        product = jnp.dot(h[:, 0 : 2 * wide], ow_buf[...], preferred_element_type=F32)
        product = product + jnp.dot(
            h[:, 2 * wide : 3 * wide], on_buf[...], preferred_element_type=F32
        )
        part[peer] = product.astype(BF16)

    project((tp + 2) % peers)
    x_copy(0, 0).start()
    x_copy(1, 0).start()
    project((tp + 1) % peers)
    x_copy(0, 1).start()
    project((tp + peers - 1) % peers)
    x_copy(1, 1).start()
    project(tp)
    for way in (0, 1):
        dest = (tp + 1) % peers if way == 0 else (tp + peers - 1) % peers
        x_copy(way, 0).wait_recv()
        at = slice(way * cols, (way + 1) * cols)
        part[dest, :, at] = (
            part[dest, :, at].astype(F32) + first_in[way].astype(F32)
        ).astype(BF16)
        x_copy(way, 2).start()
    for way in (0, 1):
        x_copy(way, 1).wait_recv()
        x_copy(way, 2).wait_recv()
    total = res_ref[...].astype(F32) + part[tp].astype(F32)
    total = total + last_in[0].astype(F32) + last_in[1].astype(F32)
    attended = total.astype(BF16)
    att_buf[...] = attended
    state = attended.astype(F32)
    mean = jnp.mean(state * state, axis=-1, keepdims=True)
    normed = (state * lax.rsqrt(mean + EPS) * norm_gain_ref[...]).astype(BF16)
    rows_buf[pl.ds(pl.multiple_of(sp * rows, rows), rows)] = normed

    def block_of(chip, owner, sub):
        at = pl.multiple_of((chip * 2 + owner) * rows + sub * (rows // 2), rows // 2)
        return rows_buf.at[pl.ds(at, rows // 2)]

    def z2_copy(way, step, sub):
        ref = block_of(chip_at(way, step - 1), core, sub)
        return same(ref, z2send.at[way, step - 1, sub], z2recv.at[way, step - 1, sub], along(way))

    def z2_arrival(way, step, sub):
        ref = block_of(chip_at(way, step), core, sub)
        return same(ref, z2send.at[way, step - 1, sub], z2recv.at[way, step - 1, sub], along(way))

    def m2_copy(way, step, sub, owner):
        ref = block_of(chip_at(way, step), owner, sub)
        return same(ref, p2send.at[way, step, sub], p2recv.at[way, step, sub], mate)

    for way, sub in ((0, 0), (1, 1), (0, 1), (1, 0)):
        z2_copy(way, 1, sub).start()
    for sub in (0, 1):
        m2_copy(0, 0, sub, core).start()
    for copy in w_copies[2:]:
        copy.wait()

    def beside(way):
        return xright if way == 0 else xleft

    def peer_at(way):
        return (tp + 1) % peers if way == 0 else (tp + peers - 1) % peers

    opposite = (tp + 2) % peers

    def a_near(way, pair, owner):
        return same(x_buf.at[pair, owner], asend.at[way, pair, 0], arecv.at[way, pair, 0], beside(way))

    def a_far(way, pair, owner):
        ref = x_buf.at[pair, owner, :, pl.ds(way * cols, cols)]
        return same(ref, asend.at[way, pair, 1], arecv.at[way, pair, 1], beside(way))

    def y_copy(way, pair, number):
        with_far = way * cols
        alone = (1 - way) * cols
        if number == 0:
            src = y_buf.at[pair, opposite, :, pl.ds(with_far, cols)]
            dst = y_first.at[pair, way]
        else:
            at = pl.ds(alone if number == 1 else with_far, cols)
            src = y_buf.at[pair, peer_at(way), :, at]
            dst = y_last.at[pair, way, :, at]
        return hop(src, dst, ysend.at[way, pair, number], yrecv.at[way, pair, number], beside(way))

    def e_copy(pair):
        return hop(
            e_buf.at[pair, 1 - core], e_mate.at[pair], esend.at[pair], erecv.at[pair], mate
        )

    tile = 2 * slots
    near = far - FAR_STEPS

    def c_copy(way, number, piece):
        last = FAR_STEPS - 1
        if piece == 0:
            at = (pl.ds(number * tile, (last - number) * tile),)
        else:
            at = (pl.ds(last * tile, tile), pl.ds(way * cols, cols))
        src = c_out.at[way] if number == 0 else c_in.at[way, number - 1]
        return hop(
            src.at[at],
            c_in.at[(way, number) + at],
            csend.at[way, number, piece],
            crecv.at[way, number, piece],
            along(way),
        )

    def cm_copy(way, number):
        at = (pl.ds(number * tile, tile),)
        to = ()
        if number == FAR_STEPS - 1:
            at = at + (pl.ds(way * cols, cols),)
            to = (slice(None), pl.ds(way * cols, cols))
        return hop(
            c_in.at[(way, number) + at],
            c_mate.at[(way, number) + to],
            cmsend.at[way, number],
            cmrecv.at[way, number],
            mate,
        )

    def pieces_of(number):
        return (0, 1) if number < FAR_STEPS - 1 else (1,)

    def picks(table, want):
        hit = jnp.logical_or(table[0:1, 0:rows] == want, table[1:2, 0:rows] == want)
        return jnp.where(hit, 1.0, 0.0).astype(BF16)

    def rows_at(device):
        return rows_buf[pl.ds(pl.multiple_of(device * rows, rows), rows)]

    def near_arrivals(step):
        for turn in (0, 1):
            for way in (0, 1):
                sub = turn if way == 0 else 1 - turn
                z2_arrival(way, step, sub).wait_recv()
                pl.when(step < near)(lambda: z2_copy(way, step + 1, sub).start())
                m2_copy(way, step, sub, core).start()

        @pl.when(step == near)
        def _():
            for way in (0, 1):
                device = chip_at(way, near) * 2 + core
                slot = lax.broadcasted_iota(jnp.int32, (FAR_STEPS * tile, rows), 0)
                onward = slot // tile + 1
                chip = (z + onward) % chips if way == 0 else (z + chips - onward) % chips
                want = ((chip * 2 + slot % tile // slots) * slots + slot % slots).astype(F32)
                c_out[way] = jnp.dot(
                    picks(info[device], want), rows_at(device), preferred_element_type=F32
                ).astype(BF16)
                for piece in (0, 1):
                    c_copy(way, 0, piece).start()

    def far_arrivals(number):
        for way in (0, 1):
            for piece in pieces_of(number):
                c_copy(way, number, piece).wait_recv()
            if number + 1 < FAR_STEPS:
                for piece in pieces_of(number + 1):
                    c_copy(way, number + 1, piece).start()
            cm_copy(way, number).start()

    def arrive(step):
        pl.when(step <= near)(functools.partial(near_arrivals, step))
        for number in range(FAR_STEPS):
            pl.when(step == near + 1 + number)(functools.partial(far_arrivals, number))

    def select_near(step):
        for way in (0, 1):
            for sub in (0, 1):
                m2_copy(way, step, sub, 1 - core).wait_recv()
        total = None
        for number, (way, owner) in enumerate(((0, 0), (1, 0), (0, 1), (1, 1))):
            device = chip_at(way, step) * 2 + owner
            slot = lax.broadcasted_iota(jnp.int32, (2 * tile, rows), 0)
            want = jnp.where(slot // slots == number, sp * slots + slot % slots, -2).astype(F32)
            picked = jnp.dot(
                picks(info[device], want), rows_at(device), preferred_element_type=F32
            )
            total = picked if total is None else total + picked
        x_buf[step, tp] = total.astype(BF16)
        for way in (0, 1):
            a_near(way, step, tp).start()

    def my_half(ref, at):
        both = ref[at].astype(F32)
        return jnp.where(core == 0, both[0:slots], both[slots:tile])

    def select_far(step):
        pair = step % far
        for number in range(FAR_STEPS):

            @pl.when(step == near + 1 + number)
            def _(number=number):
                for way in (0, 1):
                    cm_copy(way, number).wait_recv()
                for owner in (0, 1):
                    if owner == 0:
                        at_row = core * tile
                        source, at = c_in, slice(number * tile, (number + 1) * tile)
                    else:
                        at_row = (1 - core) * tile
                        source, at = c_mate, slice(None)
                    if number < FAR_STEPS - 1:
                        low = my_half(source, (0, number, at))
                        high = my_half(source, (1, number, at))
                    else:
                        low = own_rows[owner]
                        high = jnp.concatenate(
                            [
                                my_half(source, (0, number, at, slice(0, cols))),
                                my_half(source, (1, number, at, slice(cols, 2 * cols))),
                            ],
                            axis=1,
                        )
                    x_buf[pair, tp, pl.ds(pl.multiple_of(at_row, tile), tile)] = jnp.concatenate(
                        [low, high], axis=0
                    ).astype(BF16)

        for way in (0, 1):
            a_near(way, pair, tp).start()

    slot8 = lax.broadcasted_iota(jnp.int32, (slots, rows), 0)
    own_want = (sp * slots + slot8).astype(F32)
    own_rows[0] = jnp.dot(picks(info[sp], own_want), normed, preferred_element_type=F32)
    for sub in (0, 1):
        m2_copy(0, 0, sub, 1 - core).wait_recv()
    other = z * 2 + (1 - core)
    own_rows[1] = jnp.dot(picks(info[other], own_want), rows_at(other), preferred_element_type=F32)

    def forward(step):
        pair = step % far
        for way in (0, 1):
            source = peer_at(1 - way)
            a_near(way, pair, source).wait_recv()
            a_far(way, pair, source).start()

    def run_expert(step):
        pair = step % far
        for way in (0, 1):
            a_far(way, pair, opposite).wait_recv()
        x = x_buf[pair].reshape(peers * 4 * slots, 2 * cols)
        gate = jnp.dot(x, gate_buf[...], preferred_element_type=F32)
        up = jnp.dot(x, up_buf[...], preferred_element_type=F32)
        hidden = (gate / (1.0 + jnp.exp(-gate)) * up).astype(BF16)
        y = jnp.dot(hidden, down_buf[...], preferred_element_type=F32)
        y_buf[pair] = y.astype(BF16).reshape(peers, 4 * slots, 2 * cols)
        pl.when(step >= far - 1)(lambda: begin_sum(step))

    def begin_sum(step):
        pair = step % far
        for number in (0, 1):
            for way in (0, 1):
                y_copy(way, pair, number).start()

    def add_far(step):
        pair = step % far
        for way in (0, 1):
            y_copy(way, pair, 0).wait_recv()
            at = slice(way * cols, (way + 1) * cols)
            y_buf[pair, peer_at(way), :, at] = (
                y_buf[pair, peer_at(way), :, at].astype(F32) + y_first[pair, way].astype(F32)
            ).astype(BF16)
            y_copy(way, pair, 2).start()

    def finish(step):
        pair = step % far
        for way in (0, 1):
            y_copy(way, pair, 1).wait_recv()
            y_copy(way, pair, 2).wait_recv()
        total = y_buf[pair, tp].astype(F32)
        total = total + y_last[pair, 0].astype(F32) + y_last[pair, 1].astype(F32)
        e_buf[pair] = total.astype(BF16).reshape(2, 2 * slots, 2 * cols)
        e_copy(pair).start()

    stages = (
        (0, arrive, 1, far),
        (1, select_near, 1, near),
        (1, select_far, near + 1, far - 1),
        (0, select_far, far, far),
        (2, forward, 1, far),
        (3, run_expert, 1, far),
    )

    def tick(at, nothing):
        for lag, stage, first, last in stages:
            step = at - lag
            pl.when(jnp.logical_and(step >= first, step <= last))(functools.partial(stage, step))
        return nothing

    lax.fori_loop(1, far + 4, tick, 0)

    def weighted(chip, want, stack):
        table = info[chip * 2 + core]
        weight = jnp.where(table[0:1, 0:rows] == want, table[2:3, 0:rows], 0.0)
        weight = weight + jnp.where(table[1:2, 0:rows] == want, table[3:4, 0:rows], 0.0)
        coarse = weight.astype(BF16)
        fine = (weight - coarse.astype(F32)).astype(BF16)
        return lax.dot_general(
            jnp.concatenate([coarse, fine], axis=0),
            jnp.concatenate([stack, stack], axis=0),
            (((0,), (0,)), ((), ())),
            preferred_element_type=F32,
        )

    def contribution(chip, pair, which, sub):
        slot = lax.broadcasted_iota(jnp.int32, (2 * tile, rows), 0)
        expert = jnp.where(slot < tile, sp, z * 2 + (1 - core))
        ours = (slot % tile) // slots == which
        want = jnp.where(ours, expert * slots + slot % slots, -2).astype(F32)
        at = slice(sub * cols, (sub + 1) * cols)
        return weighted(
            chip, want, jnp.concatenate([e_buf[pair, core, :, at], e_mate[pair, :, at]], axis=0)
        )

    def passed_on(way, sub):
        chip = chip_at(1 - way, near)
        slot = lax.broadcasted_iota(jnp.int32, (FAR_STEPS * tile, rows), 0)
        giver = chip_at(way, FAR_STEPS - slot // tile)
        want = ((giver * 2 + slot % tile // slots) * slots + slot % slots).astype(F32)
        at = slice(sub * cols, (sub + 1) * cols)
        return weighted(chip, want, g_in[way, FAR_STEPS - 1, :, at])

    def g_copy(way, number, piece):
        at = (pl.ds(piece * tile, tile),)
        to = ()
        if piece == 0:
            at = at + (pl.ds(way * cols, cols),)
            to = (slice(None), pl.ds(way * cols, cols))
        if piece == number:
            src = g_out.at[(way, number) + to]
        else:
            src = g_in.at[(way, number - 1) + at]
        return hop(
            src,
            g_in.at[(way, number) + at],
            gsend.at[way, number, piece],
            grecv.at[way, number, piece],
            along(way),
        )

    def r_copy(way, step, sub):
        at = pl.ds(sub * cols, cols)
        return hop(
            ret_out.at[way, step, :, at],
            ret_in.at[way, step, :, at],
            rsend.at[way, step, sub],
            rrecv.at[way, step, sub],
            along(way),
        )

    for way in (0, 1):
        rest = slice((1 - way) * cols, (2 - way) * cols)
        g_in[way, FAR_STEPS - 1, 0:tile, rest] = jnp.zeros((tile, cols), BF16)

    def far_back(number):
        pair = (far - number) % far
        for way in (0, 1):
            for piece in range(number):
                g_copy(way, number - 1, piece).wait_recv()
                g_copy(way, number, piece).start()
        e_copy(pair).wait_recv()
        for way in (0, 1):
            which = 1 if number == 0 else 1 - way
            at = slice(which * slots, (which + 1) * slots)
            mine = e_buf[pair, core].astype(F32)[at]
            other = e_mate[pair].astype(F32)[at]
            g_out[way, number] = jnp.concatenate(
                [jnp.where(core == 0, mine, other), jnp.where(core == 0, other, mine)], axis=0
            ).astype(BF16)
            g_copy(way, number, number).start()

    def near_back(distance):
        step = far - distance
        e_copy(distance).wait_recv()

        @pl.when(distance == near)
        def _():
            for way in (0, 1):
                for piece in range(FAR_STEPS):
                    g_copy(way, FAR_STEPS - 1, piece).wait_recv()
                for sub in (0, 1):
                    at = slice(sub * cols, (sub + 1) * cols)
                    ret_in[way, FAR_STEPS - 1, :, at] = passed_on(way, sub).astype(BF16)

        for turn in (0, 1):
            for way in (0, 1):
                sub = turn if way == 0 else 1 - turn
                added = contribution(chip_at(1 - way, distance), distance, 1 - way, sub)
                pl.when(distance < near)(lambda: r_copy(way, step - 1, sub).wait_recv())
                at = slice(sub * cols, (sub + 1) * cols)
                ret_out[way, step, :, at] = (
                    added + ret_in[way, step - 1, :, at].astype(F32)
                ).astype(BF16)
                r_copy(way, step, sub).start()

    def back(distance):
        for number in range(FAR_STEPS):
            pl.when(distance == far - number)(functools.partial(far_back, number))
        pl.when(distance <= near)(functools.partial(near_back, distance))

    back_stages = ((3, back), (2, finish), (0, add_far), (-2, begin_sum))

    def back_tick(at, nothing):
        for lag, stage in back_stages:
            step = far - at + lag
            last = far - 2 if stage is begin_sum else far
            pl.when(jnp.logical_and(step >= 1, step <= last))(functools.partial(stage, step))
        return nothing

    lax.fori_loop(0, far + 3, back_tick, 0)
    for sub in (0, 1):
        at = slice(sub * cols, (sub + 1) * cols)
        total = att_buf[:, at].astype(F32) + contribution(z, 0, 0, sub)
        for way in (0, 1):
            r_copy(way, far - 1, sub).wait_recv()
            total = total + ret_in[way, far - 1, :, at].astype(F32)
        out_ref[:, at] = total.astype(BF16)

    for way in (0, 1):
        for number in (0, 1, 2):
            x_copy(way, number).wait_send()
    for sub in (0, 1):
        m_copy(0, 0, sub, core).wait_send()
        m2_copy(0, 0, sub, core).wait_send()
    im_copy(0, 0, core).wait_send()

    def drain(step, nothing):
        for way in (0, 1):
            i_copy(way, step).wait_send()
            im_copy(way, step, core).wait_send()
            for sub in (0, 1):
                z_copy(way, step, sub).wait_send()
                m_copy(way, step, sub, core).wait_send()
        return nothing

    def drain_near(step, nothing):
        for way in (0, 1):
            for sub in (0, 1):
                z2_copy(way, step, sub).wait_send()
                m2_copy(way, step, sub, core).wait_send()
                r_copy(way, far - step, sub).wait_send()
        return nothing

    lax.fori_loop(1, far, drain, 0)
    lax.fori_loop(1, near + 1, drain_near, 0)
    i_copy(0, far).wait_send()
    im_copy(0, far, core).wait_send()
    for way in (0, 1):
        z_copy(way, far, way).wait_send()
        m_copy(way, far, way, core).wait_send()
        for number in range(FAR_STEPS):
            for piece in pieces_of(number):
                c_copy(way, number, piece).wait_send()
            cm_copy(way, number).wait_send()
            for piece in range(number + 1):
                g_copy(way, number, piece).wait_send()

    def drain_pairs(pair, nothing):
        e_copy(pair).wait_send()
        for way in (0, 1):
            a_near(way, pair, tp).wait_send()
            a_far(way, pair, peer_at(1 - way)).wait_send()
            for number in (0, 1, 2):
                y_copy(way, pair, number).wait_send()
        return nothing

    lax.fori_loop(0, far, drain_pairs, 0)


def layer(
    residual,
    queries_wide,
    keys_wide,
    values_wide,
    queries_narrow,
    keys_narrow,
    values_narrow,
    gains,
    tables,
    norm_gain,
    route,
    output_wide,
    output_narrow,
    gate_weight,
    up_weight,
    down_weight,
):
    chips = lax.axis_size("sp") // 2
    peers = lax.axis_size("tp")
    tok, wide = keys_wide.shape
    rows, width = residual.shape
    far = chips // 2
    picked = 4 * (2 * 2 * rows // (2 * chips))
    vmem = pl.BlockSpec(memory_space=pltpu.VMEM)
    hbm = pl.BlockSpec(memory_space=pl.ANY)
    dma = pltpu.SemaphoreType.DMA
    return pl.pallas_call(
        functools.partial(layer_kernel, chips, peers),
        out_shape=jax.ShapeDtypeStruct((rows, width), BF16),
        in_specs=[vmem] * 10 + [hbm] * 5,
        out_specs=vmem,
        scratch_shapes=[
            pltpu.VMEM((2 * chips * tok, 3 * wide), BF16),
            pltpu.VMEM((2 * tok, wide), BF16),
            pltpu.VMEM((2 * tok, wide), BF16),
            pltpu.VMEM((4, tok, wide), F32),
            pltpu.VMEM((4, tok, wide), F32),
            pltpu.VMEM((4, tok, wide), F32),
            pltpu.VMEM((tok, 3 * wide), BF16),
            pltpu.VMEM(output_wide.shape, BF16),
            pltpu.VMEM(output_narrow.shape, BF16),
            pltpu.VMEM((peers, rows, width), BF16),
            pltpu.VMEM((2, rows, width // 2), BF16),
            pltpu.VMEM((2, rows, width), BF16),
            pltpu.VMEM((2 * chips,) + route.shape, F32),
            pltpu.VMEM(gate_weight.shape[1:], BF16),
            pltpu.VMEM(up_weight.shape[1:], BF16),
            pltpu.VMEM(down_weight.shape[1:], BF16),
            pltpu.VMEM((rows, width), BF16),
            pltpu.VMEM((2 * chips * rows, width), BF16),
            pltpu.VMEM((far, peers, picked, width), BF16),
            pltpu.VMEM((far, peers, picked, width), BF16),
            pltpu.VMEM((far, 2, picked, width // 2), BF16),
            pltpu.VMEM((far, 2, picked, width), BF16),
            pltpu.VMEM((far, 2, picked // 2, width), BF16),
            pltpu.VMEM((far, picked // 2, width), BF16),
            pltpu.VMEM((2, far, rows, width), BF16),
            pltpu.VMEM((2, far, rows, width), BF16),
            pltpu.VMEM((2, FAR_STEPS * picked // 2, width), BF16),
            pltpu.VMEM((2, FAR_STEPS, FAR_STEPS * picked // 2, width), BF16),
            pltpu.VMEM((2, FAR_STEPS, picked // 2, width), BF16),
            pltpu.VMEM((2, picked // 4, width), F32),
            pltpu.VMEM((2, FAR_STEPS, picked // 2, width), BF16),
            pltpu.VMEM((2, FAR_STEPS, FAR_STEPS * picked // 2, width), BF16),
            dma((5,)),
            dma((2, far, 2)),
            dma((2, far, 2)),
            dma((2, far + 1, 2)),
            dma((2, far + 1, 2)),
            dma((2, far)),
            dma((2, far)),
            dma((2, far + 1)),
            dma((2, far + 1)),
            dma((2, 3)),
            dma((2, 3)),
            dma((2, far, 2)),
            dma((2, far, 2)),
            dma((2, far + 1, 2)),
            dma((2, far + 1, 2)),
            dma((2, far, 2)),
            dma((2, far, 2)),
            dma((2, far, 3)),
            dma((2, far, 3)),
            dma((far,)),
            dma((far,)),
            dma((2, far, 2)),
            dma((2, far, 2)),
            dma((2, FAR_STEPS, 2)),
            dma((2, FAR_STEPS, 2)),
            dma((2, FAR_STEPS)),
            dma((2, FAR_STEPS)),
            dma((2, FAR_STEPS, FAR_STEPS)),
            dma((2, FAR_STEPS, FAR_STEPS)),
        ],
        compiler_params=pltpu.CompilerParams(
            collective_id=0, has_side_effects=True, vmem_limit_bytes=64 * 1024 * 1024 - 65536
        ),
        name="layer",
    )(
        queries_wide,
        keys_wide,
        values_wide,
        queries_narrow,
        jnp.concatenate([keys_narrow, values_narrow], axis=1),
        gains,
        tables,
        residual,
        norm_gain.reshape(1, width),
        route,
        output_wide,
        output_narrow,
        gate_weight,
        up_weight,
        down_weight,
    )


def body(
    residual,
    queries_wide,
    keys_wide,
    values_wide,
    queries_narrow,
    keys_narrow,
    values_narrow,
    query_gain_wide,
    key_gain_wide,
    query_gain_narrow,
    key_gain_narrow,
    output_wide,
    output_narrow,
    norm_gain,
    gate_weight,
    up_weight,
    down_weight,
    route_ids,
    route_weights,
):
    tok_count = queries_wide.shape[0]
    places = lax.axis_index("sp") * tok_count + jnp.arange(tok_count, dtype=jnp.int32)
    wide_width = query_gain_wide.shape[0]
    narrow_width = query_gain_narrow.shape[0]
    wide_angles = angles_of(places, wide_width)
    narrow_angles = angles_of(places, narrow_width)
    narrow_angles = jnp.concatenate([narrow_angles, narrow_angles], axis=1)
    lanes = jnp.arange(wide_width, dtype=jnp.int32)
    wide_sign = jnp.where(lanes % (wide_width // 2) < wide_width // 4, -1.0, 1.0)
    narrow_sign = jnp.where(lanes % (narrow_width // 2) < narrow_width // 4, -1.0, 1.0)
    tables = jnp.stack(
        [
            jnp.cos(wide_angles),
            jnp.sin(wide_angles) * wide_sign,
            jnp.cos(narrow_angles),
            jnp.sin(narrow_angles) * narrow_sign,
        ]
    )
    gains = jnp.stack(
        [
            query_gain_wide,
            key_gain_wide,
            jnp.concatenate([query_gain_narrow, query_gain_narrow]),
            jnp.concatenate([key_gain_narrow, key_gain_narrow]),
        ]
    )
    own_rows = residual.shape[0]
    route = jnp.concatenate([route_ids.astype(F32), route_weights], axis=1).T
    route = jnp.pad(route, ((0, 4), (0, 128 - own_rows)), constant_values=-1.0)
    return layer(
        residual,
        queries_wide,
        keys_wide,
        values_wide,
        queries_narrow,
        keys_narrow,
        values_narrow,
        gains,
        tables,
        norm_gain,
        route,
        output_wide,
        output_narrow,
        gate_weight,
        up_weight,
        down_weight,
    )


def solution(mesh):
    return jax.shard_map(
        body,
        mesh=mesh,
        in_specs=(
            P(("grp", "sp", "tp"), None),
            P(("grp", "sp"), "tp"),
            P(("grp", "sp"), "tp"),
            P(("grp", "sp"), "tp"),
            P(("grp", "sp"), "tp"),
            P(("grp", "sp"), "tp"),
            P(("grp", "sp"), "tp"),
            P(),
            P(),
            P(),
            P(),
            P("tp", None),
            P("tp", None),
            P(),
            P("sp", None, "tp"),
            P("sp", None, "tp"),
            P("sp", "tp", None),
            P(("grp", "sp", "tp"), None),
            P(("grp", "sp", "tp"), None),
        ),
        out_specs=P(("grp", "sp", "tp"), None),
        check_vma=False,
    )
```

```python
import functools
import math

import jax
import jax.numpy as jnp
from jax import lax
from jax.experimental import pallas as pl
from jax.experimental.pallas import tpu as pltpu
from jax.sharding import PartitionSpec as P

GRID = 64
FAR_STEPS = 3
THETA = 10000.0
EPS = 1e-06
NEG_BIG = -1e30
LOG2E = math.log2(math.e)
MESH = pl.DeviceIdType.MESH
F32 = jnp.float32
BF16 = jnp.bfloat16


def angles_of(places, head_width):
    quarter = head_width // 4
    inv_freq = THETA ** (-jnp.arange(quarter, dtype=jnp.float32) / quarter)
    grid_rows = (places // GRID).astype(jnp.float32)
    grid_cols = (places % GRID).astype(jnp.float32)
    row_angle = grid_rows[:, None] * inv_freq[None, :]
    col_angle = grid_cols[:, None] * inv_freq[None, :]
    return jnp.concatenate([row_angle, row_angle, col_angle, col_angle], axis=-1)


def lane_ids(shape):
    return lax.broadcasted_iota(jnp.int32, shape, 1)


def turned_lanes(values, quarter):
    lanes = lane_ids(values.shape)
    width = values.shape[1]
    return jnp.where(
        lanes % (2 * quarter) < quarter,
        pltpu.roll(values, width - quarter, 1),
        pltpu.roll(values, quarter, 1),
    )


def rotate(values, cos_table, sin_table, quarter):
    return values * cos_table + turned_lanes(values, quarter) * sin_table


def norm_wide(values, gain):
    mean = jnp.mean(values * values, axis=-1, keepdims=True)
    return values * lax.rsqrt(mean + EPS) * gain


def norm_halves(values, gain):
    lanes = lane_ids(values.shape)
    half = values.shape[1] // 2
    squares = values * values
    low = jnp.sum(jnp.where(lanes < half, squares, 0.0), axis=-1, keepdims=True) / half
    high = jnp.sum(jnp.where(lanes < half, 0.0, squares), axis=-1, keepdims=True) / half
    scale = jnp.where(lanes < half, lax.rsqrt(low + EPS), lax.rsqrt(high + EPS))
    return values * scale * gain


def layer_kernel(
    chips,
    peers,
    qw_ref,
    kw_ref,
    vw_ref,
    qn_ref,
    kn_ref,
    vn_ref,
    gain_qw,
    gain_kw,
    gain_qn,
    gain_kn,
    cos_w_ref,
    sin_w_ref,
    cos_n_ref,
    sin_n_ref,
    res_ref,
    norm_gain_ref,
    route_ref,
    ow_hbm,
    on_hbm,
    gate_hbm,
    up_hbm,
    down_hbm,
    out_ref,
    kv_buf,
    qws,
    qns,
    m_buf,
    l_buf,
    acc_buf,
    heads,
    ow_buf,
    on_buf,
    part,
    first_in,
    last_in,
    info,
    gate_buf,
    up_buf,
    down_buf,
    att_buf,
    rows_buf,
    x_buf,
    y_buf,
    y_first,
    y_last,
    e_buf,
    e_mate,
    ret_out,
    ret_in,
    c_out,
    c_in,
    c_mate,
    own_rows,
    g_out,
    g_in,
    w_sem,
    zsend,
    zrecv,
    psend,
    precv,
    isend,
    irecv,
    imsend,
    imrecv,
    xsend,
    xrecv,
    z2send,
    z2recv,
    p2send,
    p2recv,
    asend,
    arecv,
    ysend,
    yrecv,
    esend,
    erecv,
    rsend,
    rrecv,
    csend,
    crecv,
    cmsend,
    cmrecv,
    gsend,
    grecv,
):
    tok = qw_ref.shape[0]
    half = tok // 2
    wide = kw_ref.shape[1]
    sp = lax.axis_index("sp")
    tp = lax.axis_index("tp")
    z, core = sp // 2, sp % 2
    far = chips // 2
    right = {"sp": ((z + 1) % chips) * 2 + core}
    left = {"sp": ((z + chips - 1) % chips) * 2 + core}
    mate = {"sp": z * 2 + (1 - core)}
    xright = {"tp": (tp + 1) % peers}
    xleft = {"tp": (tp + peers - 1) % peers}

    w_copies = [
        pltpu.make_async_copy(ow_hbm, ow_buf, w_sem.at[0]),
        pltpu.make_async_copy(on_hbm, on_buf, w_sem.at[1]),
        pltpu.make_async_copy(gate_hbm.at[0], gate_buf, w_sem.at[2]),
        pltpu.make_async_copy(up_hbm.at[0], up_buf, w_sem.at[3]),
        pltpu.make_async_copy(down_hbm.at[0], down_buf, w_sem.at[4]),
    ]
    for copy in w_copies:
        copy.start()

    barrier = pltpu.get_barrier_semaphore()
    for other in (right, left, mate, xright, xleft):
        pl.semaphore_signal(barrier, inc=1, device_id=other, device_id_type=MESH)

    def rows_of(chip, owner, sub):
        at = pl.multiple_of((chip * 2 + owner) * tok + sub * half, half)
        return kv_buf.at[pl.ds(at, half)]

    cos_w, sin_w = cos_w_ref[...], sin_w_ref[...]
    cos_n, sin_n = cos_n_ref[...], sin_n_ref[...]

    def beside_itself(ref):
        return jnp.concatenate([ref[...], ref[...]], axis=1)

    own = pl.ds(pl.multiple_of(sp * tok, tok), tok)
    k_wide = rotate(norm_wide(kw_ref[...].astype(F32), gain_kw[...]), cos_w, sin_w, wide // 4)
    kvn = jnp.concatenate([kn_ref[...].astype(F32), vn_ref[...].astype(F32)], axis=1)
    k_narrow = rotate(norm_halves(kvn, beside_itself(gain_kn)), cos_n, sin_n, wide // 8)
    kv_buf[own, 0:wide] = k_wide.astype(BF16)
    kv_buf[own, wide : 2 * wide] = vw_ref[...]
    kv_buf[own, 2 * wide : 3 * wide] = jnp.where(
        lane_ids(kvn.shape) < wide // 2, k_narrow, kvn
    ).astype(BF16)

    slots = 2 * 2 * res_ref.shape[0] // (2 * chips)
    route = route_ref[...]
    lanes = route.shape[1]
    experts = lax.broadcasted_iota(jnp.int32, (2 * chips, lanes), 0).astype(F32)
    hits = [(route[k : k + 1] == experts).astype(F32) for k in (0, 1)]
    earlier = (
        lax.broadcasted_iota(jnp.int32, (lanes, lanes), 0)
        < lax.broadcasted_iota(jnp.int32, (lanes, lanes), 1)
    ).astype(BF16)
    places = jnp.dot((hits[0] + hits[1]).astype(BF16), earlier, preferred_element_type=F32)
    targets = [
        jnp.sum(hit * (places + experts * slots), axis=0, keepdims=True) for hit in hits
    ]
    row = lax.broadcasted_iota(jnp.int32, route.shape, 0)
    info[sp] = jnp.where(row == 0, targets[0], jnp.where(row == 1, targets[1], route))

    pl.semaphore_wait(barrier, 5)

    def hop(src, dst, send, recv, device):
        return pltpu.make_async_remote_copy(
            src_ref=src,
            dst_ref=dst,
            send_sem=send,
            recv_sem=recv,
            device_id=device,
            device_id_type=MESH,
        )

    def same(ref, send, recv, device):
        return hop(ref, ref, send, recv, device)

    def chip_at(way, distance):
        return (z + chips - distance) % chips if way == 0 else (z + distance) % chips

    def along(way):
        return right if way == 0 else left

    def z_copy(way, step, sub):
        ref = rows_of(chip_at(way, step - 1), core, sub)
        return same(ref, zsend.at[way, step - 1, sub], zrecv.at[way, step - 1, sub], along(way))

    def z_arrival(way, step, sub):
        ref = rows_of(chip_at(way, step), core, sub)
        return same(ref, zsend.at[way, step - 1, sub], zrecv.at[way, step - 1, sub], along(way))

    def m_copy(way, step, sub, owner):
        ref = rows_of(chip_at(way, step), owner, sub)
        return same(ref, psend.at[way, step, sub], precv.at[way, step, sub], mate)

    def i_copy(way, step):
        ref = info.at[chip_at(way, step - 1) * 2 + core]
        return same(ref, isend.at[way, step - 1], irecv.at[way, step - 1], along(way))

    def i_arrival(way, step):
        ref = info.at[chip_at(way, step) * 2 + core]
        return same(ref, isend.at[way, step - 1], irecv.at[way, step - 1], along(way))

    def im_copy(way, step, owner):
        ref = info.at[chip_at(way, step) * 2 + owner]
        return same(ref, imsend.at[way, step], imrecv.at[way, step], mate)

    for way in (0, 1):
        i_copy(way, 1).start()
    im_copy(0, 0, core).start()
    for way, sub in ((0, 0), (1, 1), (0, 1), (1, 0)):
        z_copy(way, 1, sub).start()
    for sub in (0, 1):
        m_copy(0, 0, sub, core).start()

    qw = qw_ref[...].astype(F32)
    for head in (0, 1):
        q = norm_wide(qw[:, head * wide : (head + 1) * wide], gain_qw[...])
        qws[head * tok : (head + 1) * tok] = rotate(q, cos_w, sin_w, wide // 4).astype(BF16)
    qn = rotate(norm_halves(qn_ref[...].astype(F32), beside_itself(gain_qn)), cos_n, sin_n, wide // 8)
    low = lane_ids(qn.shape) < wide // 2
    qns[0:tok] = jnp.where(low, qn, 0.0).astype(BF16)
    qns[tok : 2 * tok] = jnp.where(low, pltpu.roll(qn, wide // 2, 1), 0.0).astype(BF16)
    m_buf[...] = jnp.full(m_buf.shape, NEG_BIG, F32)
    l_buf[...] = jnp.zeros(l_buf.shape, F32)
    acc_buf[...] = jnp.zeros(acc_buf.shape, F32)

    def attend_chip(chip):
        keys = pl.ds(pl.multiple_of(chip * 2 * tok, 2 * tok), 2 * tok)
        k_w, v_w = kv_buf[keys, 0:wide], kv_buf[keys, wide : 2 * wide]
        kv_n = kv_buf[keys, 2 * wide : 3 * wide]
        work = []
        for kind in (0, 1):
            for head in (0, 1):
                work.append((kind, head))

        def scores(kind, head):
            q = (qws if kind == 0 else qns)[head * tok : (head + 1) * tok]
            return lax.dot_general(
                q,
                k_w if kind == 0 else kv_n,
                (((1,), (1,)), ((), ())),
                preferred_element_type=F32,
            )

        upcoming = scores(*work[0])
        for at, (kind, head) in enumerate(work):
            s = upcoming
            if at + 1 < len(work):
                upcoming = scores(*work[at + 1])
            factor = LOG2E * (wide if kind == 0 else wide // 2) ** (-0.5)
            m_old = m_buf[at]
            m_new = jnp.maximum(m_old, jnp.max(s, axis=-1, keepdims=True))
            alpha = jnp.exp2((m_old - m_new) * factor)
            parts = [
                jnp.exp2((s[:, i * wide : (i + 1) * wide] - m_new) * factor)
                for i in range(s.shape[1] // wide)
            ]
            total = parts[0]
            for p in parts[1:]:
                total = total + p
            weights = jnp.concatenate([p.astype(BF16) for p in parts], axis=1)
            mixed = jnp.dot(
                weights, v_w if kind == 0 else kv_n, preferred_element_type=F32
            )
            m_buf[at] = m_new
            l_buf[at] = l_buf[at] * alpha + total
            acc_buf[at] = acc_buf[at] * alpha + mixed

    def ring_step(step, nothing):
        def pass_on(way):
            i_arrival(way, step).wait_recv()
            if way == 0:
                pl.when(step < far)(lambda: i_copy(way, step + 1).start())
            else:
                pl.when(step < far - 1)(lambda: i_copy(way, step + 1).start())
            im_copy(way, step, core).start()

        @pl.when(step <= far)
        def _():
            pass_on(0)
            pl.when(step < far)(functools.partial(pass_on, 1))
            for turn in (0, 1):
                for way in (0, 1):
                    sub = turn if way == 0 else 1 - turn

                    def arrived(way=way, sub=sub, turn=turn):
                        z_arrival(way, step, sub).wait_recv()
                        if turn == 0:

                            @pl.when(step < far)
                            def _():
                                z_copy(way, step + 1, sub).start()
                        else:

                            @pl.when(step < far - 1)
                            def _():
                                z_copy(way, step + 1, sub).start()

                        m_copy(way, step, sub, core).start()

                    if turn == 0:
                        arrived()
                    else:
                        pl.when(step < far)(arrived)

        before = step - 1

        @pl.when(before == 0)
        def _():
            im_copy(0, 0, 1 - core).wait_recv()
            for sub in (0, 1):
                m_copy(0, 0, sub, 1 - core).wait_recv()

        @pl.when(before > 0)
        def _():
            im_copy(0, before, 1 - core).wait_recv()
            m_copy(0, before, 0, 1 - core).wait_recv()
            m_copy(1, before, 1, 1 - core).wait_recv()

        @pl.when(jnp.logical_and(before > 0, before < far))
        def _():
            im_copy(1, before, 1 - core).wait_recv()
            m_copy(0, before, 1, 1 - core).wait_recv()
            m_copy(1, before, 0, 1 - core).wait_recv()

        def one(side, nothing):
            attend_chip((z + chips + before * (2 * side - 1)) % chips)
            return nothing

        single = jnp.logical_or(before == 0, before == far)
        return lax.fori_loop(0, jnp.where(single, 1, 2), one, nothing)

    lax.fori_loop(1, far + 2, ring_step, 0)

    outs = []
    for at in range(4):
        outs.append(acc_buf[at] / jnp.sum(l_buf[at], axis=-1, keepdims=True))
    heads[:, 0:wide] = outs[0].astype(BF16)
    heads[:, wide : 2 * wide] = outs[1].astype(BF16)
    heads[:, 2 * wide : 3 * wide] = jnp.where(
        low, pltpu.roll(outs[2], wide // 2, 1), outs[3]
    ).astype(BF16)
    for copy in w_copies[:2]:
        copy.wait()

    rows = res_ref.shape[0]
    cols = res_ref.shape[1] // 2

    def x_copy(way, number):
        dest = (tp + 1) % peers if way == 0 else (tp + peers - 1) % peers
        with_far = way * cols
        alone = (1 - way) * cols
        if number == 0:
            src = part.at[(tp + 2) % peers, :, pl.ds(with_far, cols)]
            dst = first_in.at[way]
        else:
            at = pl.ds(alone if number == 1 else with_far, cols)
            src = part.at[dest, :, at]
            dst = last_in.at[way, :, at]
        return pltpu.make_async_remote_copy(
            src_ref=src,
            dst_ref=dst,
            send_sem=xsend.at[way, number],
            recv_sem=xrecv.at[way, number],
            device_id=xright if way == 0 else xleft,
            device_id_type=MESH,
        )

    def project(peer):
        h = heads[pl.ds(pl.multiple_of(peer * rows, rows), rows)]
        product = jnp.dot(h[:, 0 : 2 * wide], ow_buf[...], preferred_element_type=F32)
        product = product + jnp.dot(
            h[:, 2 * wide : 3 * wide], on_buf[...], preferred_element_type=F32
        )
        part[peer] = product.astype(BF16)

    project((tp + 2) % peers)
    x_copy(0, 0).start()
    x_copy(1, 0).start()
    project((tp + 1) % peers)
    x_copy(0, 1).start()
    project((tp + peers - 1) % peers)
    x_copy(1, 1).start()
    project(tp)
    for way in (0, 1):
        dest = (tp + 1) % peers if way == 0 else (tp + peers - 1) % peers
        x_copy(way, 0).wait_recv()
        at = slice(way * cols, (way + 1) * cols)
        part[dest, :, at] = (
            part[dest, :, at].astype(F32) + first_in[way].astype(F32)
        ).astype(BF16)
        x_copy(way, 2).start()
    for way in (0, 1):
        x_copy(way, 1).wait_recv()
        x_copy(way, 2).wait_recv()
    total = res_ref[...].astype(F32) + part[tp].astype(F32)
    total = total + last_in[0].astype(F32) + last_in[1].astype(F32)
    attended = total.astype(BF16)
    att_buf[...] = attended
    state = attended.astype(F32)
    mean = jnp.mean(state * state, axis=-1, keepdims=True)
    normed = (state * lax.rsqrt(mean + EPS) * norm_gain_ref[...]).astype(BF16)
    rows_buf[pl.ds(pl.multiple_of(sp * rows, rows), rows)] = normed

    def block_of(chip, owner, sub):
        at = pl.multiple_of((chip * 2 + owner) * rows + sub * (rows // 2), rows // 2)
        return rows_buf.at[pl.ds(at, rows // 2)]

    def z2_copy(way, step, sub):
        ref = block_of(chip_at(way, step - 1), core, sub)
        return same(ref, z2send.at[way, step - 1, sub], z2recv.at[way, step - 1, sub], along(way))

    def z2_arrival(way, step, sub):
        ref = block_of(chip_at(way, step), core, sub)
        return same(ref, z2send.at[way, step - 1, sub], z2recv.at[way, step - 1, sub], along(way))

    def m2_copy(way, step, sub, owner):
        ref = block_of(chip_at(way, step), owner, sub)
        return same(ref, p2send.at[way, step, sub], p2recv.at[way, step, sub], mate)

    for way, sub in ((0, 0), (1, 1), (0, 1), (1, 0)):
        z2_copy(way, 1, sub).start()
    for sub in (0, 1):
        m2_copy(0, 0, sub, core).start()
    for copy in w_copies[2:]:
        copy.wait()

    def beside(way):
        return xright if way == 0 else xleft

    def peer_at(way):
        return (tp + 1) % peers if way == 0 else (tp + peers - 1) % peers

    opposite = (tp + 2) % peers

    def a_near(way, pair, owner):
        return same(x_buf.at[pair, owner], asend.at[way, pair, 0], arecv.at[way, pair, 0], beside(way))

    def a_far(way, pair, owner):
        ref = x_buf.at[pair, owner, :, pl.ds(way * cols, cols)]
        return same(ref, asend.at[way, pair, 1], arecv.at[way, pair, 1], beside(way))

    def y_copy(way, pair, number):
        with_far = way * cols
        alone = (1 - way) * cols
        if number == 0:
            src = y_buf.at[pair, opposite, :, pl.ds(with_far, cols)]
            dst = y_first.at[pair, way]
        else:
            at = pl.ds(alone if number == 1 else with_far, cols)
            src = y_buf.at[pair, peer_at(way), :, at]
            dst = y_last.at[pair, way, :, at]
        return hop(src, dst, ysend.at[way, pair, number], yrecv.at[way, pair, number], beside(way))

    def e_copy(pair):
        return hop(
            e_buf.at[pair, 1 - core], e_mate.at[pair], esend.at[pair], erecv.at[pair], mate
        )

    tile = 2 * slots
    near = far - FAR_STEPS

    def c_copy(way, number, piece):
        last = FAR_STEPS - 1
        if piece == 0:
            at = (pl.ds(number * tile, (last - number) * tile),)
        else:
            at = (pl.ds(last * tile, tile), pl.ds(way * cols, cols))
        src = c_out.at[way] if number == 0 else c_in.at[way, number - 1]
        return hop(
            src.at[at],
            c_in.at[(way, number) + at],
            csend.at[way, number, piece],
            crecv.at[way, number, piece],
            along(way),
        )

    def cm_copy(way, number):
        at = (pl.ds(number * tile, tile),)
        to = ()
        if number == FAR_STEPS - 1:
            at = at + (pl.ds(way * cols, cols),)
            to = (slice(None), pl.ds(way * cols, cols))
        return hop(
            c_in.at[(way, number) + at],
            c_mate.at[(way, number) + to],
            cmsend.at[way, number],
            cmrecv.at[way, number],
            mate,
        )

    def pieces_of(number):
        return (0, 1) if number < FAR_STEPS - 1 else (1,)

    def picks(table, want):
        hit = jnp.logical_or(table[0:1, 0:rows] == want, table[1:2, 0:rows] == want)
        return jnp.where(hit, 1.0, 0.0).astype(BF16)

    def rows_at(device):
        return rows_buf[pl.ds(pl.multiple_of(device * rows, rows), rows)]

    def near_arrivals(step):
        for turn in (0, 1):
            for way in (0, 1):
                sub = turn if way == 0 else 1 - turn
                z2_arrival(way, step, sub).wait_recv()
                pl.when(step < near)(lambda: z2_copy(way, step + 1, sub).start())
                m2_copy(way, step, sub, core).start()

        @pl.when(step == near)
        def _():
            for way in (0, 1):
                device = chip_at(way, near) * 2 + core
                slot = lax.broadcasted_iota(jnp.int32, (FAR_STEPS * tile, rows), 0)
                onward = slot // tile + 1
                chip = (z + onward) % chips if way == 0 else (z + chips - onward) % chips
                want = ((chip * 2 + slot % tile // slots) * slots + slot % slots).astype(F32)
                c_out[way] = jnp.dot(
                    picks(info[device], want), rows_at(device), preferred_element_type=F32
                ).astype(BF16)
                for piece in (0, 1):
                    c_copy(way, 0, piece).start()

    def far_arrivals(number):
        for way in (0, 1):
            for piece in pieces_of(number):
                c_copy(way, number, piece).wait_recv()
            if number + 1 < FAR_STEPS:
                for piece in pieces_of(number + 1):
                    c_copy(way, number + 1, piece).start()
            cm_copy(way, number).start()

    def arrive(step):
        pl.when(step <= near)(functools.partial(near_arrivals, step))
        for number in range(FAR_STEPS):
            pl.when(step == near + 1 + number)(functools.partial(far_arrivals, number))

    def select_near(step):
        for way in (0, 1):
            for sub in (0, 1):
                m2_copy(way, step, sub, 1 - core).wait_recv()
        total = None
        for number, (way, owner) in enumerate(((0, 0), (1, 0), (0, 1), (1, 1))):
            device = chip_at(way, step) * 2 + owner
            slot = lax.broadcasted_iota(jnp.int32, (2 * tile, rows), 0)
            want = jnp.where(slot // slots == number, sp * slots + slot % slots, -2).astype(F32)
            picked = jnp.dot(
                picks(info[device], want), rows_at(device), preferred_element_type=F32
            )
            total = picked if total is None else total + picked
        x_buf[step, tp] = total.astype(BF16)
        for way in (0, 1):
            a_near(way, step, tp).start()

    def my_half(ref, at):
        both = ref[at].astype(F32)
        return jnp.where(core == 0, both[0:slots], both[slots:tile])

    def select_far(step):
        pair = step % far
        for number in range(FAR_STEPS):

            @pl.when(step == near + 1 + number)
            def _(number=number):
                for way in (0, 1):
                    cm_copy(way, number).wait_recv()
                for owner in (0, 1):
                    if owner == 0:
                        at_row = core * tile
                        source, at = c_in, slice(number * tile, (number + 1) * tile)
                    else:
                        at_row = (1 - core) * tile
                        source, at = c_mate, slice(None)
                    if number < FAR_STEPS - 1:
                        low = my_half(source, (0, number, at))
                        high = my_half(source, (1, number, at))
                    else:
                        low = own_rows[owner]
                        high = jnp.concatenate(
                            [
                                my_half(source, (0, number, at, slice(0, cols))),
                                my_half(source, (1, number, at, slice(cols, 2 * cols))),
                            ],
                            axis=1,
                        )
                    x_buf[pair, tp, pl.ds(pl.multiple_of(at_row, tile), tile)] = jnp.concatenate(
                        [low, high], axis=0
                    ).astype(BF16)

        for way in (0, 1):
            a_near(way, pair, tp).start()

    slot8 = lax.broadcasted_iota(jnp.int32, (slots, rows), 0)
    own_want = (sp * slots + slot8).astype(F32)
    own_rows[0] = jnp.dot(picks(info[sp], own_want), normed, preferred_element_type=F32)
    for sub in (0, 1):
        m2_copy(0, 0, sub, 1 - core).wait_recv()
    other = z * 2 + (1 - core)
    own_rows[1] = jnp.dot(picks(info[other], own_want), rows_at(other), preferred_element_type=F32)

    def forward(step):
        pair = step % far
        for way in (0, 1):
            source = peer_at(1 - way)
            a_near(way, pair, source).wait_recv()
            a_far(way, pair, source).start()

    def run_expert(step):
        pair = step % far
        for way in (0, 1):
            a_far(way, pair, opposite).wait_recv()
        x = x_buf[pair].reshape(peers * 4 * slots, 2 * cols)
        gate = jnp.dot(x, gate_buf[...], preferred_element_type=F32)
        up = jnp.dot(x, up_buf[...], preferred_element_type=F32)
        hidden = (gate / (1.0 + jnp.exp(-gate)) * up).astype(BF16)
        y = jnp.dot(hidden, down_buf[...], preferred_element_type=F32)
        y_buf[pair] = y.astype(BF16).reshape(peers, 4 * slots, 2 * cols)
        pl.when(step >= far - 1)(lambda: begin_sum(step))

    def begin_sum(step):
        pair = step % far
        for number in (0, 1):
            for way in (0, 1):
                y_copy(way, pair, number).start()

    def add_far(step):
        pair = step % far
        for way in (0, 1):
            y_copy(way, pair, 0).wait_recv()
            at = slice(way * cols, (way + 1) * cols)
            y_buf[pair, peer_at(way), :, at] = (
                y_buf[pair, peer_at(way), :, at].astype(F32) + y_first[pair, way].astype(F32)
            ).astype(BF16)
            y_copy(way, pair, 2).start()

    def finish(step):
        pair = step % far
        for way in (0, 1):
            y_copy(way, pair, 1).wait_recv()
            y_copy(way, pair, 2).wait_recv()
        total = y_buf[pair, tp].astype(F32)
        total = total + y_last[pair, 0].astype(F32) + y_last[pair, 1].astype(F32)
        e_buf[pair] = total.astype(BF16).reshape(2, 2 * slots, 2 * cols)
        e_copy(pair).start()

    stages = (
        (0, arrive, 1, far),
        (3, run_expert, 1, far),
        (0, select_near, 1, near),
        (0, select_far, near + 1, far),
        (1, forward, 1, far),
    )

    def tick(at, nothing):
        for lag, stage, first, last in stages:
            step = at - lag
            pl.when(jnp.logical_and(step >= first, step <= last))(functools.partial(stage, step))
        return nothing

    lax.fori_loop(1, far + 4, tick, 0)

    def weighted(chip, want, stack):
        table = info[chip * 2 + core]
        weight = jnp.where(table[0:1, 0:rows] == want, table[2:3, 0:rows], 0.0)
        weight = weight + jnp.where(table[1:2, 0:rows] == want, table[3:4, 0:rows], 0.0)
        coarse = weight.astype(BF16)
        fine = (weight - coarse.astype(F32)).astype(BF16)
        return lax.dot_general(
            jnp.concatenate([coarse, fine], axis=0),
            jnp.concatenate([stack, stack], axis=0),
            (((0,), (0,)), ((), ())),
            preferred_element_type=F32,
        )

    def contribution(chip, pair, which, sub):
        slot = lax.broadcasted_iota(jnp.int32, (2 * tile, rows), 0)
        expert = jnp.where(slot < tile, sp, z * 2 + (1 - core))
        ours = (slot % tile) // slots == which
        want = jnp.where(ours, expert * slots + slot % slots, -2).astype(F32)
        at = slice(sub * cols, (sub + 1) * cols)
        return weighted(
            chip, want, jnp.concatenate([e_buf[pair, core, :, at], e_mate[pair, :, at]], axis=0)
        )

    def passed_on(way, sub):
        chip = chip_at(1 - way, near)
        slot = lax.broadcasted_iota(jnp.int32, (FAR_STEPS * tile, rows), 0)
        giver = chip_at(way, FAR_STEPS - slot // tile)
        want = ((giver * 2 + slot % tile // slots) * slots + slot % slots).astype(F32)
        at = slice(sub * cols, (sub + 1) * cols)
        return weighted(chip, want, g_in[way, FAR_STEPS - 1, :, at])

    def g_copy(way, number, piece):
        at = (pl.ds(piece * tile, tile),)
        to = ()
        if piece == 0:
            at = at + (pl.ds(way * cols, cols),)
            to = (slice(None), pl.ds(way * cols, cols))
        if piece == number:
            src = g_out.at[(way, number) + to]
        else:
            src = g_in.at[(way, number - 1) + at]
        return hop(
            src,
            g_in.at[(way, number) + at],
            gsend.at[way, number, piece],
            grecv.at[way, number, piece],
            along(way),
        )

    def r_copy(way, step, sub):
        at = pl.ds(sub * cols, cols)
        return hop(
            ret_out.at[way, step, :, at],
            ret_in.at[way, step, :, at],
            rsend.at[way, step, sub],
            rrecv.at[way, step, sub],
            along(way),
        )

    for way in (0, 1):
        rest = slice((1 - way) * cols, (2 - way) * cols)
        g_in[way, FAR_STEPS - 1, 0:tile, rest] = jnp.zeros((tile, cols), BF16)

    def far_back(number):
        pair = (far - number) % far
        for way in (0, 1):
            for piece in range(number):
                g_copy(way, number - 1, piece).wait_recv()
                g_copy(way, number, piece).start()
        e_copy(pair).wait_recv()
        for way in (0, 1):
            which = 1 if number == 0 else 1 - way
            at = slice(which * slots, (which + 1) * slots)
            mine = e_buf[pair, core].astype(F32)[at]
            other = e_mate[pair].astype(F32)[at]
            g_out[way, number] = jnp.concatenate(
                [jnp.where(core == 0, mine, other), jnp.where(core == 0, other, mine)], axis=0
            ).astype(BF16)
            g_copy(way, number, number).start()

    def near_back(distance):
        step = far - distance
        e_copy(distance).wait_recv()

        @pl.when(distance == near)
        def _():
            for way in (0, 1):
                for piece in range(FAR_STEPS):
                    g_copy(way, FAR_STEPS - 1, piece).wait_recv()
                for sub in (0, 1):
                    at = slice(sub * cols, (sub + 1) * cols)
                    ret_in[way, FAR_STEPS - 1, :, at] = passed_on(way, sub).astype(BF16)

        for turn in (0, 1):
            for way in (0, 1):
                sub = turn if way == 0 else 1 - turn
                added = contribution(chip_at(1 - way, distance), distance, 1 - way, sub)
                pl.when(distance < near)(lambda: r_copy(way, step - 1, sub).wait_recv())
                at = slice(sub * cols, (sub + 1) * cols)
                ret_out[way, step, :, at] = (
                    added + ret_in[way, step - 1, :, at].astype(F32)
                ).astype(BF16)
                r_copy(way, step, sub).start()

    def back(distance):
        for number in range(FAR_STEPS):
            pl.when(distance == far - number)(functools.partial(far_back, number))
        pl.when(distance <= near)(functools.partial(near_back, distance))

    back_stages = ((3, back), (2, finish), (0, add_far), (-2, begin_sum))

    def back_tick(at, nothing):
        for lag, stage in back_stages:
            step = far - at + lag
            last = far - 2 if stage is begin_sum else far
            pl.when(jnp.logical_and(step >= 1, step <= last))(functools.partial(stage, step))
        return nothing

    lax.fori_loop(0, far + 3, back_tick, 0)
    for sub in (0, 1):
        at = slice(sub * cols, (sub + 1) * cols)
        total = att_buf[:, at].astype(F32) + contribution(z, 0, 0, sub)
        for way in (0, 1):
            r_copy(way, far - 1, sub).wait_recv()
            total = total + ret_in[way, far - 1, :, at].astype(F32)
        out_ref[:, at] = total.astype(BF16)

    for way in (0, 1):
        for number in (0, 1, 2):
            x_copy(way, number).wait_send()
    for sub in (0, 1):
        m_copy(0, 0, sub, core).wait_send()
        m2_copy(0, 0, sub, core).wait_send()
    im_copy(0, 0, core).wait_send()

    def drain(step, nothing):
        for way in (0, 1):
            i_copy(way, step).wait_send()
            im_copy(way, step, core).wait_send()
            for sub in (0, 1):
                z_copy(way, step, sub).wait_send()
                m_copy(way, step, sub, core).wait_send()
        return nothing

    def drain_near(step, nothing):
        for way in (0, 1):
            for sub in (0, 1):
                z2_copy(way, step, sub).wait_send()
                m2_copy(way, step, sub, core).wait_send()
                r_copy(way, far - step, sub).wait_send()
        return nothing

    lax.fori_loop(1, far, drain, 0)
    lax.fori_loop(1, near + 1, drain_near, 0)
    i_copy(0, far).wait_send()
    im_copy(0, far, core).wait_send()
    for way in (0, 1):
        z_copy(way, far, way).wait_send()
        m_copy(way, far, way, core).wait_send()
        for number in range(FAR_STEPS):
            for piece in pieces_of(number):
                c_copy(way, number, piece).wait_send()
            cm_copy(way, number).wait_send()
            for piece in range(number + 1):
                g_copy(way, number, piece).wait_send()

    def drain_pairs(pair, nothing):
        e_copy(pair).wait_send()
        for way in (0, 1):
            a_near(way, pair, tp).wait_send()
            a_far(way, pair, peer_at(1 - way)).wait_send()
            for number in (0, 1, 2):
                y_copy(way, pair, number).wait_send()
        return nothing

    lax.fori_loop(0, far, drain_pairs, 0)


def layer(
    residual,
    queries_wide,
    keys_wide,
    values_wide,
    queries_narrow,
    keys_narrow,
    values_narrow,
    gains,
    tables,
    norm_gain,
    route,
    output_wide,
    output_narrow,
    gate_weight,
    up_weight,
    down_weight,
):
    chips = lax.axis_size("sp") // 2
    peers = lax.axis_size("tp")
    tok, wide = keys_wide.shape
    rows, width = residual.shape
    far = chips // 2
    picked = 4 * (2 * 2 * rows // (2 * chips))
    vmem = pl.BlockSpec(memory_space=pltpu.VMEM)
    hbm = pl.BlockSpec(memory_space=pl.ANY)
    dma = pltpu.SemaphoreType.DMA
    return pl.pallas_call(
        functools.partial(layer_kernel, chips, peers),
        out_shape=jax.ShapeDtypeStruct((rows, width), BF16),
        in_specs=[vmem] * 17 + [hbm] * 5,
        out_specs=vmem,
        scratch_shapes=[
            pltpu.VMEM((2 * chips * tok, 3 * wide), BF16),
            pltpu.VMEM((2 * tok, wide), BF16),
            pltpu.VMEM((2 * tok, wide), BF16),
            pltpu.VMEM((4, tok, wide), F32),
            pltpu.VMEM((4, tok, wide), F32),
            pltpu.VMEM((4, tok, wide), F32),
            pltpu.VMEM((tok, 3 * wide), BF16),
            pltpu.VMEM(output_wide.shape, BF16),
            pltpu.VMEM(output_narrow.shape, BF16),
            pltpu.VMEM((peers, rows, width), BF16),
            pltpu.VMEM((2, rows, width // 2), BF16),
            pltpu.VMEM((2, rows, width), BF16),
            pltpu.VMEM((2 * chips,) + route.shape, F32),
            pltpu.VMEM(gate_weight.shape[1:], BF16),
            pltpu.VMEM(up_weight.shape[1:], BF16),
            pltpu.VMEM(down_weight.shape[1:], BF16),
            pltpu.VMEM((rows, width), BF16),
            pltpu.VMEM((2 * chips * rows, width), BF16),
            pltpu.VMEM((far, peers, picked, width), BF16),
            pltpu.VMEM((far, peers, picked, width), BF16),
            pltpu.VMEM((far, 2, picked, width // 2), BF16),
            pltpu.VMEM((far, 2, picked, width), BF16),
            pltpu.VMEM((far, 2, picked // 2, width), BF16),
            pltpu.VMEM((far, picked // 2, width), BF16),
            pltpu.VMEM((2, far, rows, width), BF16),
            pltpu.VMEM((2, far, rows, width), BF16),
            pltpu.VMEM((2, FAR_STEPS * picked // 2, width), BF16),
            pltpu.VMEM((2, FAR_STEPS, FAR_STEPS * picked // 2, width), BF16),
            pltpu.VMEM((2, FAR_STEPS, picked // 2, width), BF16),
            pltpu.VMEM((2, picked // 4, width), F32),
            pltpu.VMEM((2, FAR_STEPS, picked // 2, width), BF16),
            pltpu.VMEM((2, FAR_STEPS, FAR_STEPS * picked // 2, width), BF16),
            dma((5,)),
            dma((2, far, 2)),
            dma((2, far, 2)),
            dma((2, far + 1, 2)),
            dma((2, far + 1, 2)),
            dma((2, far)),
            dma((2, far)),
            dma((2, far + 1)),
            dma((2, far + 1)),
            dma((2, 3)),
            dma((2, 3)),
            dma((2, far, 2)),
            dma((2, far, 2)),
            dma((2, far + 1, 2)),
            dma((2, far + 1, 2)),
            dma((2, far, 2)),
            dma((2, far, 2)),
            dma((2, far, 3)),
            dma((2, far, 3)),
            dma((far,)),
            dma((far,)),
            dma((2, far, 2)),
            dma((2, far, 2)),
            dma((2, FAR_STEPS, 2)),
            dma((2, FAR_STEPS, 2)),
            dma((2, FAR_STEPS)),
            dma((2, FAR_STEPS)),
            dma((2, FAR_STEPS, FAR_STEPS)),
            dma((2, FAR_STEPS, FAR_STEPS)),
        ],
        compiler_params=pltpu.CompilerParams(
            collective_id=0, has_side_effects=True, vmem_limit_bytes=64 * 1024 * 1024 - 65536
        ),
        name="layer",
    )(
        queries_wide,
        keys_wide,
        values_wide,
        queries_narrow,
        keys_narrow,
        values_narrow,
        *gains,
        *tables,
        residual,
        norm_gain.reshape(1, width),
        route,
        output_wide,
        output_narrow,
        gate_weight,
        up_weight,
        down_weight,
    )


def body(
    residual,
    queries_wide,
    keys_wide,
    values_wide,
    queries_narrow,
    keys_narrow,
    values_narrow,
    query_gain_wide,
    key_gain_wide,
    query_gain_narrow,
    key_gain_narrow,
    output_wide,
    output_narrow,
    norm_gain,
    gate_weight,
    up_weight,
    down_weight,
    route_ids,
    route_weights,
):
    tok_count = queries_wide.shape[0]
    places = lax.axis_index("sp") * tok_count + jnp.arange(tok_count, dtype=jnp.int32)
    wide_width = query_gain_wide.shape[0]
    narrow_width = query_gain_narrow.shape[0]
    wide_angles = angles_of(places, wide_width)
    narrow_angles = angles_of(places, narrow_width)
    narrow_angles = jnp.concatenate([narrow_angles, narrow_angles], axis=1)
    lanes = jnp.arange(wide_width, dtype=jnp.int32)
    wide_sign = jnp.where(lanes % (wide_width // 2) < wide_width // 4, -1.0, 1.0)
    narrow_sign = jnp.where(lanes % (narrow_width // 2) < narrow_width // 4, -1.0, 1.0)
    tables = (
        jnp.cos(wide_angles),
        jnp.sin(wide_angles) * wide_sign,
        jnp.cos(narrow_angles),
        jnp.sin(narrow_angles) * narrow_sign,
    )
    gains = tuple(
        gain.reshape(1, -1)
        for gain in (query_gain_wide, key_gain_wide, query_gain_narrow, key_gain_narrow)
    )
    own_rows = residual.shape[0]
    route = jnp.concatenate([route_ids.astype(F32), route_weights], axis=1).T
    route = jnp.pad(route, ((0, 4), (0, 128 - own_rows)), constant_values=-1.0)
    return layer(
        residual,
        queries_wide,
        keys_wide,
        values_wide,
        queries_narrow,
        keys_narrow,
        values_narrow,
        gains,
        tables,
        norm_gain,
        route,
        output_wide,
        output_narrow,
        gate_weight,
        up_weight,
        down_weight,
    )


def solution(mesh):
    return jax.shard_map(
        body,
        mesh=mesh,
        in_specs=(
            P(("grp", "sp", "tp"), None),
            P(("grp", "sp"), "tp"),
            P(("grp", "sp"), "tp"),
            P(("grp", "sp"), "tp"),
            P(("grp", "sp"), "tp"),
            P(("grp", "sp"), "tp"),
            P(("grp", "sp"), "tp"),
            P(),
            P(),
            P(),
            P(),
            P("tp", None),
            P("tp", None),
            P(),
            P("sp", None, "tp"),
            P("sp", None, "tp"),
            P("sp", "tp", None),
            P(("grp", "sp", "tp"), None),
            P(("grp", "sp", "tp"), None),
        ),
        out_specs=P(("grp", "sp", "tp"), None),
        check_vma=False,
    )
```

```python
import functools
import math

import jax
import jax.numpy as jnp
from jax import lax
from jax.experimental import pallas as pl
from jax.experimental.pallas import tpu as pltpu
from jax.sharding import PartitionSpec as P

GRID = 64
FAR_STEPS = 3
THETA = 10000.0
EPS = 1e-06
NEG_BIG = -1e30
LOG2E = math.log2(math.e)
MESH = pl.DeviceIdType.MESH
F32 = jnp.float32
BF16 = jnp.bfloat16


def angles_of(places, head_width):
    quarter = head_width // 4
    inv_freq = THETA ** (-jnp.arange(quarter, dtype=jnp.float32) / quarter)
    grid_rows = (places // GRID).astype(jnp.float32)
    grid_cols = (places % GRID).astype(jnp.float32)
    row_angle = grid_rows[:, None] * inv_freq[None, :]
    col_angle = grid_cols[:, None] * inv_freq[None, :]
    return jnp.concatenate([row_angle, row_angle, col_angle, col_angle], axis=-1)


def lane_ids(shape):
    return lax.broadcasted_iota(jnp.int32, shape, 1)


def turned_lanes(values, quarter):
    lanes = lane_ids(values.shape)
    width = values.shape[1]
    return jnp.where(
        lanes % (2 * quarter) < quarter,
        pltpu.roll(values, width - quarter, 1),
        pltpu.roll(values, quarter, 1),
    )


def rotate(values, cos_table, sin_table, quarter):
    return values * cos_table + turned_lanes(values, quarter) * sin_table


def norm_wide(values, gain):
    mean = jnp.mean(values * values, axis=-1, keepdims=True)
    return values * lax.rsqrt(mean + EPS) * gain


def norm_halves(values, gain):
    lanes = lane_ids(values.shape)
    half = values.shape[1] // 2
    squares = values * values
    low = jnp.sum(jnp.where(lanes < half, squares, 0.0), axis=-1, keepdims=True) / half
    high = jnp.sum(jnp.where(lanes < half, 0.0, squares), axis=-1, keepdims=True) / half
    scale = jnp.where(lanes < half, lax.rsqrt(low + EPS), lax.rsqrt(high + EPS))
    return values * scale * gain


def layer_kernel(
    chips,
    peers,
    qw_ref,
    kw_ref,
    vw_ref,
    qn_ref,
    kn_ref,
    vn_ref,
    gain_qw,
    gain_kw,
    gain_qn,
    gain_kn,
    cos_w_ref,
    sin_w_ref,
    cos_n_ref,
    sin_n_ref,
    res_ref,
    norm_gain_ref,
    route_ref,
    ow_hbm,
    on_hbm,
    gate_hbm,
    up_hbm,
    down_hbm,
    out_ref,
    kv_buf,
    qws,
    qns,
    m_buf,
    l_buf,
    acc_buf,
    heads,
    ow_buf,
    on_buf,
    part,
    first_in,
    last_in,
    info,
    gate_buf,
    up_buf,
    down_buf,
    att_buf,
    rows_buf,
    x_buf,
    y_buf,
    y_first,
    y_last,
    e_buf,
    e_mate,
    ret_out,
    ret_in,
    c_out,
    c_in,
    c_mate,
    own_rows,
    g_out,
    g_in,
    w_sem,
    zsend,
    zrecv,
    psend,
    precv,
    isend,
    irecv,
    imsend,
    imrecv,
    xsend,
    xrecv,
    z2send,
    z2recv,
    p2send,
    p2recv,
    asend,
    arecv,
    ysend,
    yrecv,
    esend,
    erecv,
    rsend,
    rrecv,
    csend,
    crecv,
    cmsend,
    cmrecv,
    gsend,
    grecv,
):
    tok = qw_ref.shape[0]
    half = tok // 2
    wide = kw_ref.shape[1]
    sp = lax.axis_index("sp")
    tp = lax.axis_index("tp")
    z, core = sp // 2, sp % 2
    far = chips // 2
    right = {"sp": ((z + 1) % chips) * 2 + core}
    left = {"sp": ((z + chips - 1) % chips) * 2 + core}
    mate = {"sp": z * 2 + (1 - core)}
    xright = {"tp": (tp + 1) % peers}
    xleft = {"tp": (tp + peers - 1) % peers}

    w_copies = [
        pltpu.make_async_copy(ow_hbm, ow_buf, w_sem.at[0]),
        pltpu.make_async_copy(on_hbm, on_buf, w_sem.at[1]),
        pltpu.make_async_copy(gate_hbm.at[0], gate_buf, w_sem.at[2]),
        pltpu.make_async_copy(up_hbm.at[0], up_buf, w_sem.at[3]),
        pltpu.make_async_copy(down_hbm.at[0], down_buf, w_sem.at[4]),
    ]
    for copy in w_copies:
        copy.start()

    barrier = pltpu.get_barrier_semaphore()
    for other in (right, left, mate, xright, xleft):
        pl.semaphore_signal(barrier, inc=1, device_id=other, device_id_type=MESH)

    def rows_of(chip, owner, sub):
        at = pl.multiple_of((chip * 2 + owner) * tok + sub * half, half)
        return kv_buf.at[pl.ds(at, half)]

    cos_w, sin_w = cos_w_ref[...], sin_w_ref[...]
    cos_n, sin_n = cos_n_ref[...], sin_n_ref[...]

    def beside_itself(ref):
        return jnp.concatenate([ref[...], ref[...]], axis=1)

    own = pl.ds(pl.multiple_of(sp * tok, tok), tok)
    k_wide = rotate(norm_wide(kw_ref[...].astype(F32), gain_kw[...]), cos_w, sin_w, wide // 4)
    kvn = jnp.concatenate([kn_ref[...].astype(F32), vn_ref[...].astype(F32)], axis=1)
    k_narrow = rotate(norm_halves(kvn, beside_itself(gain_kn)), cos_n, sin_n, wide // 8)
    kv_buf[own, 0:wide] = k_wide.astype(BF16)
    kv_buf[own, wide : 2 * wide] = vw_ref[...]
    kv_buf[own, 2 * wide : 3 * wide] = jnp.where(
        lane_ids(kvn.shape) < wide // 2, k_narrow, kvn
    ).astype(BF16)

    slots = 2 * 2 * res_ref.shape[0] // (2 * chips)
    route = route_ref[...]
    lanes = route.shape[1]
    experts = lax.broadcasted_iota(jnp.int32, (2 * chips, lanes), 0).astype(F32)
    hits = [(route[k : k + 1] == experts).astype(F32) for k in (0, 1)]
    earlier = (
        lax.broadcasted_iota(jnp.int32, (lanes, lanes), 0)
        < lax.broadcasted_iota(jnp.int32, (lanes, lanes), 1)
    ).astype(BF16)
    places = jnp.dot((hits[0] + hits[1]).astype(BF16), earlier, preferred_element_type=F32)
    targets = [
        jnp.sum(hit * (places + experts * slots), axis=0, keepdims=True) for hit in hits
    ]
    row = lax.broadcasted_iota(jnp.int32, route.shape, 0)
    info[sp] = jnp.where(row == 0, targets[0], jnp.where(row == 1, targets[1], route))

    pl.semaphore_wait(barrier, 5)

    def hop(src, dst, send, recv, device):
        return pltpu.make_async_remote_copy(
            src_ref=src,
            dst_ref=dst,
            send_sem=send,
            recv_sem=recv,
            device_id=device,
            device_id_type=MESH,
        )

    def same(ref, send, recv, device):
        return hop(ref, ref, send, recv, device)

    def chip_at(way, distance):
        return (z + chips - distance) % chips if way == 0 else (z + distance) % chips

    def along(way):
        return right if way == 0 else left

    def z_copy(way, step, sub):
        ref = rows_of(chip_at(way, step - 1), core, sub)
        return same(ref, zsend.at[way, step - 1, sub], zrecv.at[way, step - 1, sub], along(way))

    def z_arrival(way, step, sub):
        ref = rows_of(chip_at(way, step), core, sub)
        return same(ref, zsend.at[way, step - 1, sub], zrecv.at[way, step - 1, sub], along(way))

    def m_copy(way, step, sub, owner):
        ref = rows_of(chip_at(way, step), owner, sub)
        return same(ref, psend.at[way, step, sub], precv.at[way, step, sub], mate)

    def i_copy(way, step):
        ref = info.at[chip_at(way, step - 1) * 2 + core]
        return same(ref, isend.at[way, step - 1], irecv.at[way, step - 1], along(way))

    def i_arrival(way, step):
        ref = info.at[chip_at(way, step) * 2 + core]
        return same(ref, isend.at[way, step - 1], irecv.at[way, step - 1], along(way))

    def im_copy(way, step, owner):
        ref = info.at[chip_at(way, step) * 2 + owner]
        return same(ref, imsend.at[way, step], imrecv.at[way, step], mate)

    for way in (0, 1):
        i_copy(way, 1).start()
    im_copy(0, 0, core).start()
    for way, sub in ((0, 0), (1, 1), (0, 1), (1, 0)):
        z_copy(way, 1, sub).start()
    for sub in (0, 1):
        m_copy(0, 0, sub, core).start()

    qw = qw_ref[...].astype(F32)
    for head in (0, 1):
        q = norm_wide(qw[:, head * wide : (head + 1) * wide], gain_qw[...])
        qws[head * tok : (head + 1) * tok] = rotate(q, cos_w, sin_w, wide // 4).astype(BF16)
    qn = rotate(norm_halves(qn_ref[...].astype(F32), beside_itself(gain_qn)), cos_n, sin_n, wide // 8)
    low = lane_ids(qn.shape) < wide // 2
    qns[0:tok] = jnp.where(low, qn, 0.0).astype(BF16)
    qns[tok : 2 * tok] = jnp.where(low, pltpu.roll(qn, wide // 2, 1), 0.0).astype(BF16)
    m_buf[...] = jnp.full(m_buf.shape, NEG_BIG, F32)
    l_buf[...] = jnp.zeros(l_buf.shape, F32)
    acc_buf[...] = jnp.zeros(acc_buf.shape, F32)

    def attend_chip(chip):
        keys = pl.ds(pl.multiple_of(chip * 2 * tok, 2 * tok), 2 * tok)
        k_w, v_w = kv_buf[keys, 0:wide], kv_buf[keys, wide : 2 * wide]
        kv_n = kv_buf[keys, 2 * wide : 3 * wide]
        work = []
        for kind in (0, 1):
            for head in (0, 1):
                work.append((kind, head))

        def scores(kind, head):
            q = (qws if kind == 0 else qns)[head * tok : (head + 1) * tok]
            return lax.dot_general(
                q,
                k_w if kind == 0 else kv_n,
                (((1,), (1,)), ((), ())),
                preferred_element_type=F32,
            )

        upcoming = scores(*work[0])
        for at, (kind, head) in enumerate(work):
            s = upcoming
            if at + 1 < len(work):
                upcoming = scores(*work[at + 1])
            factor = LOG2E * (wide if kind == 0 else wide // 2) ** (-0.5)
            m_old = m_buf[at]
            m_new = jnp.maximum(m_old, jnp.max(s, axis=-1, keepdims=True))
            alpha = jnp.exp2((m_old - m_new) * factor)
            parts = [
                jnp.exp2((s[:, i * wide : (i + 1) * wide] - m_new) * factor)
                for i in range(s.shape[1] // wide)
            ]
            total = parts[0]
            for p in parts[1:]:
                total = total + p
            weights = jnp.concatenate([p.astype(BF16) for p in parts], axis=1)
            mixed = jnp.dot(
                weights, v_w if kind == 0 else kv_n, preferred_element_type=F32
            )
            m_buf[at] = m_new
            l_buf[at] = l_buf[at] * alpha + total
            acc_buf[at] = acc_buf[at] * alpha + mixed

    def ring_step(step, nothing):
        def pass_on(way):
            i_arrival(way, step).wait_recv()
            if way == 0:
                pl.when(step < far)(lambda: i_copy(way, step + 1).start())
            else:
                pl.when(step < far - 1)(lambda: i_copy(way, step + 1).start())
            im_copy(way, step, core).start()

        @pl.when(step <= far)
        def _():
            pass_on(0)
            pl.when(step < far)(functools.partial(pass_on, 1))
            for turn in (0, 1):
                for way in (0, 1):
                    sub = turn if way == 0 else 1 - turn

                    def arrived(way=way, sub=sub, turn=turn):
                        z_arrival(way, step, sub).wait_recv()
                        if turn == 0:

                            @pl.when(step < far)
                            def _():
                                z_copy(way, step + 1, sub).start()
                        else:

                            @pl.when(step < far - 1)
                            def _():
                                z_copy(way, step + 1, sub).start()

                        m_copy(way, step, sub, core).start()

                    if turn == 0:
                        arrived()
                    else:
                        pl.when(step < far)(arrived)

        before = step - 1

        @pl.when(before == 0)
        def _():
            im_copy(0, 0, 1 - core).wait_recv()
            for sub in (0, 1):
                m_copy(0, 0, sub, 1 - core).wait_recv()

        @pl.when(before > 0)
        def _():
            im_copy(0, before, 1 - core).wait_recv()
            m_copy(0, before, 0, 1 - core).wait_recv()
            m_copy(1, before, 1, 1 - core).wait_recv()

        @pl.when(jnp.logical_and(before > 0, before < far))
        def _():
            im_copy(1, before, 1 - core).wait_recv()
            m_copy(0, before, 1, 1 - core).wait_recv()
            m_copy(1, before, 0, 1 - core).wait_recv()

        def one(side, nothing):
            attend_chip((z + chips + before * (2 * side - 1)) % chips)
            return nothing

        single = jnp.logical_or(before == 0, before == far)
        return lax.fori_loop(0, jnp.where(single, 1, 2), one, nothing)

    lax.fori_loop(1, far + 2, ring_step, 0)

    outs = []
    for at in range(4):
        outs.append(acc_buf[at] / jnp.sum(l_buf[at], axis=-1, keepdims=True))
    heads[:, 0:wide] = outs[0].astype(BF16)
    heads[:, wide : 2 * wide] = outs[1].astype(BF16)
    heads[:, 2 * wide : 3 * wide] = jnp.where(
        low, pltpu.roll(outs[2], wide // 2, 1), outs[3]
    ).astype(BF16)
    for copy in w_copies[:2]:
        copy.wait()

    rows = res_ref.shape[0]
    cols = res_ref.shape[1] // 2

    def x_copy(way, number, part_of):
        dest = (tp + 1) % peers if way == 0 else (tp + peers - 1) % peers
        with_far = way * cols
        alone = (1 - way) * cols
        these = pl.ds(part_of * (rows // 2), rows // 2)
        if number == 0:
            src = part.at[(tp + 2) % peers, these, pl.ds(with_far, cols)]
            dst = first_in.at[way, these]
        else:
            at = pl.ds(alone if number == 1 else with_far, cols)
            src = part.at[dest, these, at]
            dst = last_in.at[way, these, at]
        return pltpu.make_async_remote_copy(
            src_ref=src,
            dst_ref=dst,
            send_sem=xsend.at[way, number, part_of],
            recv_sem=xrecv.at[way, number, part_of],
            device_id=xright if way == 0 else xleft,
            device_id_type=MESH,
        )

    def project(peer):
        h = heads[pl.ds(pl.multiple_of(peer * rows, rows), rows)]
        product = jnp.dot(h[:, 0 : 2 * wide], ow_buf[...], preferred_element_type=F32)
        product = product + jnp.dot(
            h[:, 2 * wide : 3 * wide], on_buf[...], preferred_element_type=F32
        )
        part[peer] = product.astype(BF16)

    def add_and_send(part_of):
        these = slice(part_of * (rows // 2), (part_of + 1) * (rows // 2))
        for way in (0, 1):
            dest = (tp + 1) % peers if way == 0 else (tp + peers - 1) % peers
            x_copy(way, 0, part_of).wait_recv()
            at = slice(way * cols, (way + 1) * cols)
            part[dest, these, at] = (
                part[dest, these, at].astype(F32) + first_in[way, these].astype(F32)
            ).astype(BF16)
            x_copy(way, 2, part_of).start()

    def attend_rows(part_of):
        these = slice(part_of * (rows // 2), (part_of + 1) * (rows // 2))
        for way in (0, 1):
            x_copy(way, 1, part_of).wait_recv()
            x_copy(way, 2, part_of).wait_recv()
        total = res_ref[these].astype(F32) + part[tp, these].astype(F32)
        total = total + last_in[0, these].astype(F32) + last_in[1, these].astype(F32)
        attended = total.astype(BF16)
        att_buf[these] = attended
        state = attended.astype(F32)
        mean = jnp.mean(state * state, axis=-1, keepdims=True)
        at = pl.multiple_of(sp * rows + part_of * (rows // 2), rows // 2)
        rows_buf[pl.ds(at, rows // 2)] = (
            state * lax.rsqrt(mean + EPS) * norm_gain_ref[...]
        ).astype(BF16)

    project((tp + 2) % peers)
    for way in (0, 1):
        x_copy(way, 0, 0).start()
    project((tp + 1) % peers)
    x_copy(0, 1, 0).start()
    project((tp + peers - 1) % peers)
    x_copy(1, 1, 0).start()
    for way in (0, 1):
        x_copy(way, 0, 1).start()
    project(tp)
    add_and_send(0)
    for way in (0, 1):
        x_copy(way, 1, 1).start()

    def block_of(chip, owner, sub):
        at = pl.multiple_of((chip * 2 + owner) * rows + sub * (rows // 2), rows // 2)
        return rows_buf.at[pl.ds(at, rows // 2)]

    def z2_copy(way, step, sub):
        ref = block_of(chip_at(way, step - 1), core, sub)
        return same(ref, z2send.at[way, step - 1, sub], z2recv.at[way, step - 1, sub], along(way))

    def z2_arrival(way, step, sub):
        ref = block_of(chip_at(way, step), core, sub)
        return same(ref, z2send.at[way, step - 1, sub], z2recv.at[way, step - 1, sub], along(way))

    def m2_copy(way, step, sub, owner):
        ref = block_of(chip_at(way, step), owner, sub)
        return same(ref, p2send.at[way, step, sub], p2recv.at[way, step, sub], mate)

    add_and_send(1)
    for sub in (0, 1):
        attend_rows(sub)
        for way in (0, 1):
            z2_copy(way, 1, sub).start()
        m2_copy(0, 0, sub, core).start()
    for copy in w_copies[2:]:
        copy.wait()

    def beside(way):
        return xright if way == 0 else xleft

    def peer_at(way):
        return (tp + 1) % peers if way == 0 else (tp + peers - 1) % peers

    opposite = (tp + 2) % peers

    def a_near(way, pair, owner):
        return same(x_buf.at[pair, owner], asend.at[way, pair, 0], arecv.at[way, pair, 0], beside(way))

    def a_far(way, pair, owner):
        ref = x_buf.at[pair, owner, :, pl.ds(way * cols, cols)]
        return same(ref, asend.at[way, pair, 1], arecv.at[way, pair, 1], beside(way))

    def y_copy(way, pair, number):
        with_far = way * cols
        alone = (1 - way) * cols
        if number == 0:
            src = y_buf.at[pair, opposite, :, pl.ds(with_far, cols)]
            dst = y_first.at[pair, way]
        else:
            at = pl.ds(alone if number == 1 else with_far, cols)
            src = y_buf.at[pair, peer_at(way), :, at]
            dst = y_last.at[pair, way, :, at]
        return hop(src, dst, ysend.at[way, pair, number], yrecv.at[way, pair, number], beside(way))

    def e_copy(pair):
        return hop(
            e_buf.at[pair, 1 - core], e_mate.at[pair], esend.at[pair], erecv.at[pair], mate
        )

    tile = 2 * slots
    near = far - FAR_STEPS

    def c_copy(way, number, piece):
        last = FAR_STEPS - 1
        if piece == 0:
            at = (pl.ds(number * tile, (last - number) * tile),)
        else:
            at = (pl.ds(last * tile, tile), pl.ds(way * cols, cols))
        src = c_out.at[way] if number == 0 else c_in.at[way, number - 1]
        return hop(
            src.at[at],
            c_in.at[(way, number) + at],
            csend.at[way, number, piece],
            crecv.at[way, number, piece],
            along(way),
        )

    def cm_copy(way, number):
        at = (pl.ds(number * tile, tile),)
        to = ()
        if number == FAR_STEPS - 1:
            at = at + (pl.ds(way * cols, cols),)
            to = (slice(None), pl.ds(way * cols, cols))
        return hop(
            c_in.at[(way, number) + at],
            c_mate.at[(way, number) + to],
            cmsend.at[way, number],
            cmrecv.at[way, number],
            mate,
        )

    def pieces_of(number):
        return (0, 1) if number < FAR_STEPS - 1 else (1,)

    def picks(table, want):
        hit = jnp.logical_or(table[0:1, 0:rows] == want, table[1:2, 0:rows] == want)
        return jnp.where(hit, 1.0, 0.0).astype(BF16)

    def rows_at(device):
        return rows_buf[pl.ds(pl.multiple_of(device * rows, rows), rows)]

    def near_arrivals(step):
        for turn in (0, 1):
            for way in (0, 1):
                sub = turn
                z2_arrival(way, step, sub).wait_recv()
                pl.when(step < near)(lambda: z2_copy(way, step + 1, sub).start())
                m2_copy(way, step, sub, core).start()

        @pl.when(step == near)
        def _():
            for way in (0, 1):
                device = chip_at(way, near) * 2 + core
                slot = lax.broadcasted_iota(jnp.int32, (FAR_STEPS * tile, rows), 0)
                onward = slot // tile + 1
                chip = (z + onward) % chips if way == 0 else (z + chips - onward) % chips
                want = ((chip * 2 + slot % tile // slots) * slots + slot % slots).astype(F32)
                c_out[way] = jnp.dot(
                    picks(info[device], want), rows_at(device), preferred_element_type=F32
                ).astype(BF16)
                for piece in (0, 1):
                    c_copy(way, 0, piece).start()

    def far_arrivals(number):
        for way in (0, 1):
            for piece in pieces_of(number):
                c_copy(way, number, piece).wait_recv()
            if number + 1 < FAR_STEPS:
                for piece in pieces_of(number + 1):
                    c_copy(way, number + 1, piece).start()
            cm_copy(way, number).start()

    def arrive(step):
        pl.when(step <= near)(functools.partial(near_arrivals, step))
        for number in range(FAR_STEPS):
            pl.when(step == near + 1 + number)(functools.partial(far_arrivals, number))

    def select_near(step):
        for way in (0, 1):
            for sub in (0, 1):
                m2_copy(way, step, sub, 1 - core).wait_recv()
        total = None
        for number, (way, owner) in enumerate(((0, 0), (1, 0), (0, 1), (1, 1))):
            device = chip_at(way, step) * 2 + owner
            slot = lax.broadcasted_iota(jnp.int32, (2 * tile, rows), 0)
            want = jnp.where(slot // slots == number, sp * slots + slot % slots, -2).astype(F32)
            picked = jnp.dot(
                picks(info[device], want), rows_at(device), preferred_element_type=F32
            )
            total = picked if total is None else total + picked
        x_buf[step, tp] = total.astype(BF16)
        for way in (0, 1):
            a_near(way, step, tp).start()

    def my_half(ref, at):
        both = ref[at].astype(F32)
        return jnp.where(core == 0, both[0:slots], both[slots:tile])

    def select_far(step):
        pair = step % far
        for number in range(FAR_STEPS):

            @pl.when(step == near + 1 + number)
            def _(number=number):
                for way in (0, 1):
                    cm_copy(way, number).wait_recv()
                for owner in (0, 1):
                    if owner == 0:
                        at_row = core * tile
                        source, at = c_in, slice(number * tile, (number + 1) * tile)
                    else:
                        at_row = (1 - core) * tile
                        source, at = c_mate, slice(None)
                    if number < FAR_STEPS - 1:
                        low = my_half(source, (0, number, at))
                        high = my_half(source, (1, number, at))
                    else:
                        low = own_rows[owner]
                        high = jnp.concatenate(
                            [
                                my_half(source, (0, number, at, slice(0, cols))),
                                my_half(source, (1, number, at, slice(cols, 2 * cols))),
                            ],
                            axis=1,
                        )
                    x_buf[pair, tp, pl.ds(pl.multiple_of(at_row, tile), tile)] = jnp.concatenate(
                        [low, high], axis=0
                    ).astype(BF16)

        for way in (0, 1):
            a_near(way, pair, tp).start()

    slot8 = lax.broadcasted_iota(jnp.int32, (slots, rows), 0)
    own_want = (sp * slots + slot8).astype(F32)
    own_rows[0] = jnp.dot(picks(info[sp], own_want), rows_at(sp), preferred_element_type=F32)
    for sub in (0, 1):
        m2_copy(0, 0, sub, 1 - core).wait_recv()
    other = z * 2 + (1 - core)
    own_rows[1] = jnp.dot(picks(info[other], own_want), rows_at(other), preferred_element_type=F32)

    def forward(step):
        pair = step % far
        for way in (0, 1):
            source = peer_at(1 - way)
            a_near(way, pair, source).wait_recv()
            a_far(way, pair, source).start()

    def run_expert(step):
        pair = step % far
        for way in (0, 1):
            a_far(way, pair, opposite).wait_recv()
        x = x_buf[pair].reshape(peers * 4 * slots, 2 * cols)
        gate = jnp.dot(x, gate_buf[...], preferred_element_type=F32)
        up = jnp.dot(x, up_buf[...], preferred_element_type=F32)
        hidden = (gate / (1.0 + jnp.exp(-gate)) * up).astype(BF16)
        y = jnp.dot(hidden, down_buf[...], preferred_element_type=F32)
        y_buf[pair] = y.astype(BF16).reshape(peers, 4 * slots, 2 * cols)
        pl.when(step >= far - 1)(lambda: begin_sum(step))

    def begin_sum(step):
        pair = step % far
        for number in (0, 1):
            for way in (0, 1):
                y_copy(way, pair, number).start()

    def add_far(step):
        pair = step % far
        for way in (0, 1):
            y_copy(way, pair, 0).wait_recv()
            at = slice(way * cols, (way + 1) * cols)
            y_buf[pair, peer_at(way), :, at] = (
                y_buf[pair, peer_at(way), :, at].astype(F32) + y_first[pair, way].astype(F32)
            ).astype(BF16)
            y_copy(way, pair, 2).start()

    def finish(step):
        pair = step % far
        for way in (0, 1):
            y_copy(way, pair, 1).wait_recv()
            y_copy(way, pair, 2).wait_recv()
        total = y_buf[pair, tp].astype(F32)
        total = total + y_last[pair, 0].astype(F32) + y_last[pair, 1].astype(F32)
        e_buf[pair] = total.astype(BF16).reshape(2, 2 * slots, 2 * cols)
        e_copy(pair).start()

    stages = (
        (0, arrive, 1, far),
        (3, run_expert, 1, far),
        (0, select_near, 1, near),
        (0, select_far, near + 1, far),
        (1, forward, 1, far),
    )

    def tick(at, nothing):
        for lag, stage, first, last in stages:
            step = at - lag
            pl.when(jnp.logical_and(step >= first, step <= last))(functools.partial(stage, step))
        return nothing

    lax.fori_loop(1, far + 4, tick, 0)

    def weighted(chip, want, stack):
        table = info[chip * 2 + core]
        weight = jnp.where(table[0:1, 0:rows] == want, table[2:3, 0:rows], 0.0)
        weight = weight + jnp.where(table[1:2, 0:rows] == want, table[3:4, 0:rows], 0.0)
        coarse = weight.astype(BF16)
        fine = (weight - coarse.astype(F32)).astype(BF16)
        return lax.dot_general(
            jnp.concatenate([coarse, fine], axis=0),
            jnp.concatenate([stack, stack], axis=0),
            (((0,), (0,)), ((), ())),
            preferred_element_type=F32,
        )

    def contribution(chip, pair, which, sub):
        slot = lax.broadcasted_iota(jnp.int32, (2 * tile, rows), 0)
        expert = jnp.where(slot < tile, sp, z * 2 + (1 - core))
        ours = (slot % tile) // slots == which
        want = jnp.where(ours, expert * slots + slot % slots, -2).astype(F32)
        at = slice(sub * cols, (sub + 1) * cols)
        return weighted(
            chip, want, jnp.concatenate([e_buf[pair, core, :, at], e_mate[pair, :, at]], axis=0)
        )

    def passed_on(way, sub):
        chip = chip_at(1 - way, near)
        slot = lax.broadcasted_iota(jnp.int32, (FAR_STEPS * tile, rows), 0)
        giver = chip_at(way, FAR_STEPS - slot // tile)
        want = ((giver * 2 + slot % tile // slots) * slots + slot % slots).astype(F32)
        at = slice(sub * cols, (sub + 1) * cols)
        return weighted(chip, want, g_in[way, FAR_STEPS - 1, :, at])

    def g_copy(way, number, piece):
        at = (pl.ds(piece * tile, tile),)
        to = ()
        if piece == 0:
            at = at + (pl.ds(way * cols, cols),)
            to = (slice(None), pl.ds(way * cols, cols))
        if piece == number:
            src = g_out.at[(way, number) + to]
        else:
            src = g_in.at[(way, number - 1) + at]
        return hop(
            src,
            g_in.at[(way, number) + at],
            gsend.at[way, number, piece],
            grecv.at[way, number, piece],
            along(way),
        )

    def r_copy(way, step, sub):
        at = pl.ds(sub * cols, cols)
        return hop(
            ret_out.at[way, step, :, at],
            ret_in.at[way, step, :, at],
            rsend.at[way, step, sub],
            rrecv.at[way, step, sub],
            along(way),
        )

    for way in (0, 1):
        rest = slice((1 - way) * cols, (2 - way) * cols)
        g_in[way, FAR_STEPS - 1, 0:tile, rest] = jnp.zeros((tile, cols), BF16)

    def far_back(number):
        pair = (far - number) % far
        for way in (0, 1):
            for piece in range(number):
                g_copy(way, number - 1, piece).wait_recv()
                g_copy(way, number, piece).start()
        e_copy(pair).wait_recv()
        for way in (0, 1):
            which = 1 if number == 0 else 1 - way
            at = slice(which * slots, (which + 1) * slots)
            mine = e_buf[pair, core].astype(F32)[at]
            other = e_mate[pair].astype(F32)[at]
            g_out[way, number] = jnp.concatenate(
                [jnp.where(core == 0, mine, other), jnp.where(core == 0, other, mine)], axis=0
            ).astype(BF16)
            g_copy(way, number, number).start()

    def near_back(distance):
        step = far - distance
        e_copy(distance).wait_recv()

        @pl.when(distance == near)
        def _():
            for way in (0, 1):
                for piece in range(FAR_STEPS):
                    g_copy(way, FAR_STEPS - 1, piece).wait_recv()
                for sub in (0, 1):
                    at = slice(sub * cols, (sub + 1) * cols)
                    ret_in[way, FAR_STEPS - 1, :, at] = passed_on(way, sub).astype(BF16)

        for turn in (0, 1):
            for way in (0, 1):
                sub = turn if way == 0 else 1 - turn
                added = contribution(chip_at(1 - way, distance), distance, 1 - way, sub)
                pl.when(distance < near)(lambda: r_copy(way, step - 1, sub).wait_recv())
                at = slice(sub * cols, (sub + 1) * cols)
                ret_out[way, step, :, at] = (
                    added + ret_in[way, step - 1, :, at].astype(F32)
                ).astype(BF16)
                r_copy(way, step, sub).start()

    def back(distance):
        for number in range(FAR_STEPS):
            pl.when(distance == far - number)(functools.partial(far_back, number))
        pl.when(distance <= near)(functools.partial(near_back, distance))

    back_stages = ((3, back), (2, finish), (0, add_far), (-2, begin_sum))

    def back_tick(at, nothing):
        for lag, stage in back_stages:
            step = far - at + lag
            last = far - 2 if stage is begin_sum else far
            pl.when(jnp.logical_and(step >= 1, step <= last))(functools.partial(stage, step))
        return nothing

    lax.fori_loop(0, far + 3, back_tick, 0)
    for sub in (0, 1):
        at = slice(sub * cols, (sub + 1) * cols)
        total = att_buf[:, at].astype(F32) + contribution(z, 0, 0, sub)
        for way in (0, 1):
            r_copy(way, far - 1, sub).wait_recv()
            total = total + ret_in[way, far - 1, :, at].astype(F32)
        out_ref[:, at] = total.astype(BF16)

    for way in (0, 1):
        for number in (0, 1, 2):
            for part_of in (0, 1):
                x_copy(way, number, part_of).wait_send()
    for sub in (0, 1):
        m_copy(0, 0, sub, core).wait_send()
        m2_copy(0, 0, sub, core).wait_send()
    im_copy(0, 0, core).wait_send()

    def drain(step, nothing):
        for way in (0, 1):
            i_copy(way, step).wait_send()
            im_copy(way, step, core).wait_send()
            for sub in (0, 1):
                z_copy(way, step, sub).wait_send()
                m_copy(way, step, sub, core).wait_send()
        return nothing

    def drain_near(step, nothing):
        for way in (0, 1):
            for sub in (0, 1):
                z2_copy(way, step, sub).wait_send()
                m2_copy(way, step, sub, core).wait_send()
                r_copy(way, far - step, sub).wait_send()
        return nothing

    lax.fori_loop(1, far, drain, 0)
    lax.fori_loop(1, near + 1, drain_near, 0)
    i_copy(0, far).wait_send()
    im_copy(0, far, core).wait_send()
    for way in (0, 1):
        z_copy(way, far, way).wait_send()
        m_copy(way, far, way, core).wait_send()
        for number in range(FAR_STEPS):
            for piece in pieces_of(number):
                c_copy(way, number, piece).wait_send()
            cm_copy(way, number).wait_send()
            for piece in range(number + 1):
                g_copy(way, number, piece).wait_send()

    def drain_pairs(pair, nothing):
        e_copy(pair).wait_send()
        for way in (0, 1):
            a_near(way, pair, tp).wait_send()
            a_far(way, pair, peer_at(1 - way)).wait_send()
            for number in (0, 1, 2):
                y_copy(way, pair, number).wait_send()
        return nothing

    lax.fori_loop(0, far, drain_pairs, 0)


def layer(
    residual,
    queries_wide,
    keys_wide,
    values_wide,
    queries_narrow,
    keys_narrow,
    values_narrow,
    gains,
    tables,
    norm_gain,
    route,
    output_wide,
    output_narrow,
    gate_weight,
    up_weight,
    down_weight,
):
    chips = lax.axis_size("sp") // 2
    peers = lax.axis_size("tp")
    tok, wide = keys_wide.shape
    rows, width = residual.shape
    far = chips // 2
    picked = 4 * (2 * 2 * rows // (2 * chips))
    vmem = pl.BlockSpec(memory_space=pltpu.VMEM)
    hbm = pl.BlockSpec(memory_space=pl.ANY)
    dma = pltpu.SemaphoreType.DMA
    return pl.pallas_call(
        functools.partial(layer_kernel, chips, peers),
        out_shape=jax.ShapeDtypeStruct((rows, width), BF16),
        in_specs=[vmem] * 17 + [hbm] * 5,
        out_specs=vmem,
        scratch_shapes=[
            pltpu.VMEM((2 * chips * tok, 3 * wide), BF16),
            pltpu.VMEM((2 * tok, wide), BF16),
            pltpu.VMEM((2 * tok, wide), BF16),
            pltpu.VMEM((4, tok, wide), F32),
            pltpu.VMEM((4, tok, wide), F32),
            pltpu.VMEM((4, tok, wide), F32),
            pltpu.VMEM((tok, 3 * wide), BF16),
            pltpu.VMEM(output_wide.shape, BF16),
            pltpu.VMEM(output_narrow.shape, BF16),
            pltpu.VMEM((peers, rows, width), BF16),
            pltpu.VMEM((2, rows, width // 2), BF16),
            pltpu.VMEM((2, rows, width), BF16),
            pltpu.VMEM((2 * chips,) + route.shape, F32),
            pltpu.VMEM(gate_weight.shape[1:], BF16),
            pltpu.VMEM(up_weight.shape[1:], BF16),
            pltpu.VMEM(down_weight.shape[1:], BF16),
            pltpu.VMEM((rows, width), BF16),
            pltpu.VMEM((2 * chips * rows, width), BF16),
            pltpu.VMEM((far, peers, picked, width), BF16),
            pltpu.VMEM((far, peers, picked, width), BF16),
            pltpu.VMEM((far, 2, picked, width // 2), BF16),
            pltpu.VMEM((far, 2, picked, width), BF16),
            pltpu.VMEM((far, 2, picked // 2, width), BF16),
            pltpu.VMEM((far, picked // 2, width), BF16),
            pltpu.VMEM((2, far, rows, width), BF16),
            pltpu.VMEM((2, far, rows, width), BF16),
            pltpu.VMEM((2, FAR_STEPS * picked // 2, width), BF16),
            pltpu.VMEM((2, FAR_STEPS, FAR_STEPS * picked // 2, width), BF16),
            pltpu.VMEM((2, FAR_STEPS, picked // 2, width), BF16),
            pltpu.VMEM((2, picked // 4, width), F32),
            pltpu.VMEM((2, FAR_STEPS, picked // 2, width), BF16),
            pltpu.VMEM((2, FAR_STEPS, FAR_STEPS * picked // 2, width), BF16),
            dma((5,)),
            dma((2, far, 2)),
            dma((2, far, 2)),
            dma((2, far + 1, 2)),
            dma((2, far + 1, 2)),
            dma((2, far)),
            dma((2, far)),
            dma((2, far + 1)),
            dma((2, far + 1)),
            dma((2, 3, 2)),
            dma((2, 3, 2)),
            dma((2, far, 2)),
            dma((2, far, 2)),
            dma((2, far + 1, 2)),
            dma((2, far + 1, 2)),
            dma((2, far, 2)),
            dma((2, far, 2)),
            dma((2, far, 3)),
            dma((2, far, 3)),
            dma((far,)),
            dma((far,)),
            dma((2, far, 2)),
            dma((2, far, 2)),
            dma((2, FAR_STEPS, 2)),
            dma((2, FAR_STEPS, 2)),
            dma((2, FAR_STEPS)),
            dma((2, FAR_STEPS)),
            dma((2, FAR_STEPS, FAR_STEPS)),
            dma((2, FAR_STEPS, FAR_STEPS)),
        ],
        compiler_params=pltpu.CompilerParams(
            collective_id=0, has_side_effects=True, vmem_limit_bytes=64 * 1024 * 1024 - 65536
        ),
        name="layer",
    )(
        queries_wide,
        keys_wide,
        values_wide,
        queries_narrow,
        keys_narrow,
        values_narrow,
        *gains,
        *tables,
        residual,
        norm_gain.reshape(1, width),
        route,
        output_wide,
        output_narrow,
        gate_weight,
        up_weight,
        down_weight,
    )


def body(
    residual,
    queries_wide,
    keys_wide,
    values_wide,
    queries_narrow,
    keys_narrow,
    values_narrow,
    query_gain_wide,
    key_gain_wide,
    query_gain_narrow,
    key_gain_narrow,
    output_wide,
    output_narrow,
    norm_gain,
    gate_weight,
    up_weight,
    down_weight,
    route_ids,
    route_weights,
):
    tok_count = queries_wide.shape[0]
    places = lax.axis_index("sp") * tok_count + jnp.arange(tok_count, dtype=jnp.int32)
    wide_width = query_gain_wide.shape[0]
    narrow_width = query_gain_narrow.shape[0]
    wide_angles = angles_of(places, wide_width)
    narrow_angles = angles_of(places, narrow_width)
    narrow_angles = jnp.concatenate([narrow_angles, narrow_angles], axis=1)
    lanes = jnp.arange(wide_width, dtype=jnp.int32)
    wide_sign = jnp.where(lanes % (wide_width // 2) < wide_width // 4, -1.0, 1.0)
    narrow_sign = jnp.where(lanes % (narrow_width // 2) < narrow_width // 4, -1.0, 1.0)
    tables = (
        jnp.cos(wide_angles),
        jnp.sin(wide_angles) * wide_sign,
        jnp.cos(narrow_angles),
        jnp.sin(narrow_angles) * narrow_sign,
    )
    gains = tuple(
        gain.reshape(1, -1)
        for gain in (query_gain_wide, key_gain_wide, query_gain_narrow, key_gain_narrow)
    )
    own_rows = residual.shape[0]
    route = jnp.concatenate([route_ids.astype(F32), route_weights], axis=1).T
    route = jnp.pad(route, ((0, 4), (0, 128 - own_rows)), constant_values=-1.0)
    return layer(
        residual,
        queries_wide,
        keys_wide,
        values_wide,
        queries_narrow,
        keys_narrow,
        values_narrow,
        gains,
        tables,
        norm_gain,
        route,
        output_wide,
        output_narrow,
        gate_weight,
        up_weight,
        down_weight,
    )


def solution(mesh):
    return jax.shard_map(
        body,
        mesh=mesh,
        in_specs=(
            P(("grp", "sp", "tp"), None),
            P(("grp", "sp"), "tp"),
            P(("grp", "sp"), "tp"),
            P(("grp", "sp"), "tp"),
            P(("grp", "sp"), "tp"),
            P(("grp", "sp"), "tp"),
            P(("grp", "sp"), "tp"),
            P(),
            P(),
            P(),
            P(),
            P("tp", None),
            P("tp", None),
            P(),
            P("sp", None, "tp"),
            P("sp", None, "tp"),
            P("sp", "tp", None),
            P(("grp", "sp", "tp"), None),
            P(("grp", "sp", "tp"), None),
        ),
        out_specs=P(("grp", "sp", "tp"), None),
        check_vma=False,
    )
```
